32 devices in a mesh: fs: 16 (over z, y, x), tp: 2 (over core).
Axes of the slice: x: 2, y: 2, z: 4, core: 2. Of those that a mesh axis runs over, the one named last changes fastest.
Arguments:
- residual_in: bfloat16 [4096, 2048], P(('fs', 'tp')), may hold values from -6 to 6
- gain_first: float32 [2048], replicated, may hold values from 0.1 to 1.9
- gain_mixer: float32 [2048], replicated, may hold values from 0.1 to 1.9
- gain_second: float32 [2048], replicated, may hold values from 0.1 to 1.9
- gate_weight: float32 [2048, 6144], P('fs', 'tp'), may hold values from -0.125 to 0.125
- gate_scale: float32 [6144], P('tp'), may hold values from 0.3 to 3
- up_weight: float32 [2048, 6144], P('fs', 'tp'), may hold values from -0.125 to 0.125
- up_scale: float32 [6144], P('tp'), may hold values from 0.3 to 3
- down_weight: float32 [6144, 2048], P('tp', 'fs'), may hold values from -0.078125 to 0.078125
- down_scale: float32 [2048], P('fs'), may hold values from 0.3 to 3
- query_weight: float32 [2048, 2048], P('fs', 'tp'), may hold values from -0.125 to 0.125
- query_scale: float32 [2048], P('tp'), may hold values from 0.3 to 3
- key_weight: float32 [2048, 2048], P('fs', 'tp'), may hold values from -0.125 to 0.125
- key_scale: float32 [2048], P('tp'), may hold values from 0.3 to 3
- value_weight: float32 [2048, 2048], P('fs', 'tp'), may hold values from -0.125 to 0.125
- value_scale: float32 [2048], P('tp'), may hold values from 0.3 to 3
- output_weight: float32 [2048, 2048], P('tp', 'fs'), may hold values from -0.125 to 0.125
- output_scale: float32 [2048], P('fs'), may hold values from 0.3 to 3
Outputs:
- residual_out: bfloat16 [4096, 2048], P(('fs', 'tp'))
The draws below stay inside these ranges and needn't reach their ends.
All inputs are finite; a program needn't handle non-finite values.
Results may differ from the reference program's by a relative error of at most 0.028.
Values may be sent and summed in bfloat16 or wider, within the bound.
A program may use at most 128 MiB of HBM per device.

```python
import math
import jax
import jax.numpy as jnp
from jax import lax

D = 2048
FF = 6144
HEADS = 8
HEAD_DIM = 256
MIX_WIDTH = 2048
TOK = 256
BLOCK = 64
TOKENS = 4096
N_FS = 16
N_TP = 2


def steps_of(stream_key, dims, shards, low, top_value):
    loudness, own = 1.0, jax.random.fold_in(stream_key, 6)
    for axis_at, parts in shards:
        draws = jnp.exp(jax.random.uniform(jax.random.fold_in(own, axis_at), (parts,), jnp.float32, low / len(shards), top_value / len(shards)))
        loudness = loudness * jnp.repeat(draws, dims[axis_at] // parts).reshape([-1 if axis == axis_at else 1 for axis in range(len(dims))])
    return loudness


def centred(stream_key, extent, scale, reach, split=(), kind=jnp.bfloat16):
    entries = scale * jax.random.normal(stream_key, extent, jnp.float32)
    if split:
        entries = entries * steps_of(stream_key, extent, split, -0.22, 0.18)
    return jnp.clip(entries, -reach, reach).astype(kind)


def setup_inputs(seed: int = 0) -> dict:
    key_list = jax.random.split(jax.random.key(seed), 19)
    residual_in = centred(key_list[0], (TOKENS, D), 1.0, 6.0, ((0, 32),))
    gain_first = jnp.clip(1.0 + 0.18 * jax.random.normal(key_list[1], (D,), jnp.float32), 0.1, 1.9)
    gain_mixer = jnp.clip(1.0 + 0.18 * jax.random.normal(key_list[2], (D,), jnp.float32), 0.1, 1.9)
    gain_second = jnp.clip(1.0 + 0.18 * jax.random.normal(key_list[3], (D,), jnp.float32), 0.1, 1.9)
    gate_weight = centred(key_list[4], (D, FF), D ** -0.5, 0.125, ((0, 16), (1, 2)), jnp.float32)
    gate_scale = jnp.clip(jnp.exp(math.log(3.0) - 2.3025851 * jax.random.uniform(key_list[5], (FF,), jnp.float32) ** steps_of(key_list[5], (FF,), ((0, 2),), -0.2, 0.2)), 0.3, 3.0)
    up_weight = centred(key_list[6], (D, FF), D ** -0.5, 0.125, ((0, 16), (1, 2)), jnp.float32)
    up_scale = jnp.clip(jnp.exp(math.log(3.0) - 2.3025851 * jax.random.uniform(key_list[7], (FF,), jnp.float32) ** steps_of(key_list[7], (FF,), ((0, 2),), -0.2, 0.2)), 0.3, 3.0)
    down_weight = centred(key_list[8], (FF, D), FF ** -0.5, 0.078125, ((0, 2), (1, 16)), jnp.float32)
    down_scale = jnp.clip(jnp.exp(math.log(3.0) - 2.3025851 * jax.random.uniform(key_list[9], (D,), jnp.float32) ** steps_of(key_list[9], (D,), ((0, 16),), -0.2, 0.2)), 0.3, 3.0)
    query_weight = centred(key_list[10], (D, MIX_WIDTH), D ** -0.5, 0.125, ((0, 16), (1, 2)), jnp.float32)
    query_scale = jnp.clip(jnp.exp(math.log(3.0) - 2.3025851 * jax.random.uniform(key_list[11], (MIX_WIDTH,), jnp.float32) ** steps_of(key_list[11], (MIX_WIDTH,), ((0, 2),), -0.2, 0.2)), 0.3, 3.0)
    key_weight = centred(key_list[12], (D, MIX_WIDTH), D ** -0.5, 0.125, ((0, 16), (1, 2)), jnp.float32)
    key_scale = jnp.clip(jnp.exp(math.log(3.0) - 2.3025851 * jax.random.uniform(key_list[13], (MIX_WIDTH,), jnp.float32) ** steps_of(key_list[13], (MIX_WIDTH,), ((0, 2),), -0.2, 0.2)), 0.3, 3.0)
    value_weight = centred(key_list[14], (D, MIX_WIDTH), D ** -0.5, 0.125, ((0, 16), (1, 2)), jnp.float32)
    value_scale = jnp.clip(jnp.exp(math.log(3.0) - 2.3025851 * jax.random.uniform(key_list[15], (MIX_WIDTH,), jnp.float32) ** steps_of(key_list[15], (MIX_WIDTH,), ((0, 2),), -0.2, 0.2)), 0.3, 3.0)
    output_weight = centred(key_list[16], (MIX_WIDTH, D), MIX_WIDTH ** -0.5, 0.125, ((0, 2), (1, 16)), jnp.float32)
    output_scale = jnp.clip(jnp.exp(math.log(3.0) - 2.3025851 * jax.random.uniform(key_list[17], (D,), jnp.float32) ** steps_of(key_list[17], (D,), ((0, 16),), -0.2, 0.2)), 0.3, 3.0)
    return dict(residual_in=residual_in, gain_first=gain_first, gain_mixer=gain_mixer, gain_second=gain_second, gate_weight=gate_weight, gate_scale=gate_scale, up_weight=up_weight, up_scale=up_scale, down_weight=down_weight, down_scale=down_scale, query_weight=query_weight, query_scale=query_scale, key_weight=key_weight, key_scale=key_scale, value_weight=value_weight, value_scale=value_scale, output_weight=output_weight, output_scale=output_scale)


EPSILON = 1e-06
HEAD_FLOOR = 0.25
ROTARY_BASE = 10000.0
HIGHEST = lax.Precision.HIGHEST

def normalize(sequence_rows, gain_vector):
    values = sequence_rows.astype(jnp.float32)
    scaled = values * lax.rsqrt(lax.optimization_barrier(jnp.mean(values * values, axis=-1, keepdims=True)) + EPSILON)
    return (scaled * gain_vector).astype(jnp.bfloat16)

def head_rates(first_head, head_count, length):
    head_number = (first_head + jnp.arange(head_count)).astype(jnp.float32)
    return jnp.exp(jnp.log(1.0 / 16.0) + head_number / (HEADS - 1) * jnp.log(4.0 / length))

def rotate(values, positions):
    half_width = values.shape[-1] // 2
    frequency = ROTARY_BASE ** (-jnp.arange(half_width, dtype=jnp.float32) * 2.0 / values.shape[-1])
    angles = positions[:, None] * frequency[None, :]
    cosine = jnp.cos(angles)[:, None, :]
    sine_value = jnp.sin(angles)[:, None, :]
    front_half = values[..., :half_width]
    back_half = values[..., half_width:]
    return jnp.concatenate([front_half * cosine - back_half * sine_value, back_half * cosine + front_half * sine_value], axis=-1)

def retention(query_pre, key_pre, value_pre, decay_rates):
    length, head_count, head_width = query_pre.shape
    positions = jnp.arange(length, dtype=jnp.float32)
    query_rot = rotate(query_pre, positions).astype(jnp.bfloat16)
    key_rot = rotate(key_pre, positions).astype(jnp.bfloat16)
    value_low = value_pre.astype(jnp.bfloat16)
    blocks = length // BLOCK
    inside = jnp.arange(BLOCK, dtype=jnp.float32)
    distance = inside[:, None] - inside[None, :]
    within = jnp.where(distance >= 0, jnp.exp(-decay_rates[:, None, None] * jnp.maximum(distance, 0.0)), 0.0) * head_width ** (-0.5)
    query_blocks = query_rot.reshape(blocks, BLOCK, head_count, head_width)
    key_blocks = key_rot.reshape(blocks, BLOCK, head_count, head_width)
    value_blocks = value_low.reshape(blocks, BLOCK, head_count, head_width)
    scores = jnp.einsum('nihe,njhe->nhij', query_blocks.astype(jnp.float32), key_blocks.astype(jnp.float32), precision=HIGHEST)
    weights = (scores * within[None]).astype(jnp.bfloat16)
    inner_part = jnp.einsum('nhij,njhe->nihe', weights.astype(jnp.float32), value_blocks.astype(jnp.float32), precision=HIGHEST)
    fading = jnp.exp(-decay_rates[None, :] * (BLOCK - 1.0 - inside[:, None])) * head_width ** (-0.5)
    key_faded = key_blocks.astype(jnp.float32) * fading[None, :, :, None]
    updates = jnp.einsum('njhd,njhe->nhde', key_faded, value_blocks.astype(jnp.float32), precision=HIGHEST)
    block_decay = jnp.exp(-decay_rates * BLOCK)

    def advance(memory_state, update):
        return (memory_state * block_decay[:, None, None] + update, memory_state)
    _, before = lax.scan(advance, jnp.zeros((head_count, head_width, head_width), jnp.float32), updates)
    rising = jnp.exp(-decay_rates[None, :] * (inside[:, None] + 1.0))
    queried = query_blocks.astype(jnp.float32) * rising[None, :, :, None]
    carried_part = jnp.einsum('nihd,nhde->nihe', queried, before, precision=HIGHEST)
    combined = (inner_part + carried_part).reshape(length, head_count, head_width)
    normed = combined * lax.rsqrt(jnp.maximum(lax.optimization_barrier(jnp.mean(combined * combined, axis=-1, keepdims=True)), HEAD_FLOOR))
    return normed.astype(jnp.bfloat16).reshape(length, head_count * head_width)

def partial_sums(inputs, weight, factor, range_width):
    combined = jnp.zeros((inputs.shape[0], weight.shape[1]), jnp.float32)
    for member in range(N_TP):
        partial_piece = jnp.dot(inputs[:, member * range_width:(member + 1) * range_width], weight[member * range_width:(member + 1) * range_width], preferred_element_type=jnp.float32) * factor
        combined = combined + lax.optimization_barrier(partial_piece.astype(jnp.bfloat16)).astype(jnp.float32)
    return combined

def reference(residual_in, gain_first, gain_mixer, gain_second, gate_weight, gate_scale, up_weight, up_scale, down_weight, down_scale, query_weight, query_scale, key_weight, key_scale, value_weight, value_scale, output_weight, output_scale):
    gate_low = gate_weight.astype(jnp.bfloat16)
    up_low = up_weight.astype(jnp.bfloat16)
    down_low = down_weight.astype(jnp.bfloat16)
    query_low = query_weight.astype(jnp.bfloat16)
    key_low = key_weight.astype(jnp.bfloat16)
    value_low = value_weight.astype(jnp.bfloat16)
    output_low = output_weight.astype(jnp.bfloat16)
    decay_rates = head_rates(0, HEADS, TOK)

    def feed_forward(sequence_rows, gain_vector):
        normed = normalize(sequence_rows, gain_vector)
        gate_pre = jnp.dot(normed, gate_low, preferred_element_type=jnp.float32) * gate_scale
        up_pre = jnp.dot(normed, up_low, preferred_element_type=jnp.float32) * up_scale
        hidden = (jax.nn.silu(gate_pre) * up_pre).astype(jnp.bfloat16)
        return partial_sums(hidden, down_low, down_scale, FF // N_TP)

    def one_sequence(sequence_rows):
        middle = (sequence_rows.astype(jnp.float32) + 0.5 * feed_forward(sequence_rows, gain_first)).astype(jnp.bfloat16)
        mixer_input = normalize(middle, gain_mixer)
        query_pre = (jnp.dot(mixer_input, query_low, preferred_element_type=jnp.float32) * query_scale).reshape(TOK, HEADS, HEAD_DIM)
        key_pre = (jnp.dot(mixer_input, key_low, preferred_element_type=jnp.float32) * key_scale).reshape(TOK, HEADS, HEAD_DIM)
        value_pre = (jnp.dot(mixer_input, value_low, preferred_element_type=jnp.float32) * value_scale).reshape(TOK, HEADS, HEAD_DIM)
        mixed = retention(query_pre, key_pre, value_pre, decay_rates)
        mixer_out = partial_sums(mixed, output_low, output_scale, HEADS * HEAD_DIM // N_TP)
        second = (middle.astype(jnp.float32) + mixer_out).astype(jnp.bfloat16)
        return (second.astype(jnp.float32) + 0.5 * feed_forward(second, gain_second)).astype(jnp.bfloat16)
    sequences = residual_in.reshape(N_FS, TOK, D)
    return lax.map(one_sequence, sequences).reshape(N_FS * TOK, D)
```

```python
import functools
import math

import jax
import jax.numpy as jnp
import numpy as np
from jax import lax
from jax.experimental import pallas as pl
from jax.experimental.pallas import tpu as pltpu
from jax.sharding import PartitionSpec as P

HEADS = 8
HEAD_DIM = 256
BLOCK = 64


EPSILON = 1e-06
HEAD_FLOOR = 0.25
ROTARY_BASE = 10000.0
HIGHEST = lax.Precision.HIGHEST


def normalize(sequence_rows, gain_vector):
    values = sequence_rows.astype(jnp.float32)
    scaled = values * lax.rsqrt(jnp.mean(values * values, axis=-1, keepdims=True) + EPSILON)
    return (scaled * gain_vector).astype(jnp.bfloat16)


def head_rates(first_head, head_count, length):
    head_number = (first_head + jnp.arange(head_count)).astype(jnp.float32)
    return jnp.exp(jnp.log(1.0 / 16.0) + head_number / (HEADS - 1) * jnp.log(4.0 / length))


def rotate(values, positions):
    half_width = values.shape[-1] // 2
    frequency = ROTARY_BASE ** (-jnp.arange(half_width, dtype=jnp.float32) * 2.0 / values.shape[-1])
    angles = positions[:, None] * frequency[None, :]
    cosine = jnp.cos(angles)[:, None, :]
    sine_value = jnp.sin(angles)[:, None, :]
    front_half = values[..., :half_width]
    back_half = values[..., half_width:]
    return jnp.concatenate(
        [
            front_half * cosine - back_half * sine_value,
            back_half * cosine + front_half * sine_value,
        ],
        axis=-1,
    )


def retention(query_pre, key_pre, value_pre, decay_rates):
    length, head_count, head_width = query_pre.shape
    positions = jnp.arange(length, dtype=jnp.float32)
    query_rot = rotate(query_pre, positions).astype(jnp.bfloat16)
    key_rot = rotate(key_pre, positions).astype(jnp.bfloat16)
    value_low = value_pre.astype(jnp.bfloat16)
    blocks = length // BLOCK
    inside = jnp.arange(BLOCK, dtype=jnp.float32)
    distance = inside[:, None] - inside[None, :]
    within = jnp.where(
        distance >= 0, jnp.exp(-decay_rates[:, None, None] * jnp.maximum(distance, 0.0)), 0.0
    ) * head_width ** (-0.5)
    query_blocks = query_rot.reshape(blocks, BLOCK, head_count, head_width)
    key_blocks = key_rot.reshape(blocks, BLOCK, head_count, head_width)
    value_blocks = value_low.reshape(blocks, BLOCK, head_count, head_width)
    scores = jnp.einsum(
        "nihe,njhe->nhij", query_blocks, key_blocks, preferred_element_type=jnp.float32
    )
    weights = (scores * within[None]).astype(jnp.bfloat16)
    inner_part = jnp.einsum(
        "nhij,njhe->nihe", weights, value_blocks, preferred_element_type=jnp.float32
    )
    fading = jnp.exp(-decay_rates[None, :] * (BLOCK - 1.0 - inside[:, None])) * head_width ** (-0.5)
    key_faded = key_blocks.astype(jnp.float32) * fading[None, :, :, None]
    updates = jnp.einsum(
        "njhd,njhe->nhde", key_faded, value_blocks.astype(jnp.float32), precision=HIGHEST
    )
    block_decay = jnp.exp(-decay_rates * BLOCK)

    def advance(memory_state, update):
        return (memory_state * block_decay[:, None, None] + update, memory_state)

    _, before = lax.scan(
        advance, jnp.zeros((head_count, head_width, head_width), jnp.float32), updates
    )
    rising = jnp.exp(-decay_rates[None, :] * (inside[:, None] + 1.0))
    queried = query_blocks.astype(jnp.float32) * rising[None, :, :, None]
    carried_part = jnp.einsum("nihd,nhde->nihe", queried, before, precision=HIGHEST)
    combined = (inner_part + carried_part).reshape(length, head_count, head_width)
    normed = combined * lax.rsqrt(
        jnp.maximum(jnp.mean(combined * combined, axis=-1, keepdims=True), HEAD_FLOOR)
    )
    return normed.astype(jnp.bfloat16).reshape(length, head_count * head_width)


def split_three(values):
    high = values.astype(jnp.bfloat16)
    rest = values - high.astype(jnp.float32)
    middle_part = rest.astype(jnp.bfloat16)
    low = (rest - middle_part.astype(jnp.float32)).astype(jnp.bfloat16)
    return [high, middle_part, low]


def make_body(n_fs, n_tp, share):
    spread = n_fs // share
    STRIDED = False
    if STRIDED:
        teams = [[m * spread + r for m in range(share)] for r in range(spread)]
    else:
        teams = [[r * share + m for m in range(share)] for r in range(spread)]
    twins = [[team[m] for team in teams] for m in range(share)]
    row_teams = [[f * n_tp + t for f in team for t in range(n_tp)] for team in teams]

    def my_rank():
        position = lax.axis_index("fs")
        return position // spread if STRIDED else position % share

    def fetch(pieces):
        swapped = lax.all_to_all(
            pieces, "fs", split_axis=0, concat_axis=0, axis_index_groups=teams, tiled=True
        )
        return lax.all_gather(swapped, "fs", axis=0, axis_index_groups=twins, tiled=False)

    def order_features(rows):
        if not STRIDED:
            return rows
        count = rows.shape[0]
        return rows.reshape(count, share, spread, -1).swapaxes(1, 2).reshape(count, -1)

    def collect_rows(rows, gain_vector):
        return lax.all_gather(
            order_features(normalize(rows, gain_vector)),
            ("fs", "tp"),
            axis=0,
            axis_index_groups=row_teams,
            tiled=True,
        )

    def return_rows(inputs, weight, factor):
        term = jnp.dot(inputs, weight, preferred_element_type=jnp.float32) * factor
        return lax.psum_scatter(
            term.astype(jnp.bfloat16),
            ("fs", "tp"),
            scatter_dimension=0,
            axis_index_groups=row_teams,
            tiled=True,
        ).astype(jnp.float32)

    def columns_of(weight):
        low = weight.astype(jnp.bfloat16)
        return low.reshape(low.shape[0], share, -1).swapaxes(0, 1)

    def rows_of(weight):
        low = weight.astype(jnp.bfloat16)
        return low.reshape(share, -1, low.shape[1])

    def own(vector, rank):
        width = vector.shape[0] // share
        return lax.dynamic_slice_in_dim(vector, rank * width, width)

    def body(
        residual_in,
        gain_first,
        gain_mixer,
        gain_second,
        gate_weight,
        gate_scale,
        up_weight,
        up_scale,
        down_weight,
        down_scale,
        query_weight,
        query_scale,
        key_weight,
        key_scale,
        value_weight,
        value_scale,
        output_weight,
        output_scale,
    ):
        rank = my_rank()
        hidden_width = gate_weight.shape[1] // share
        mix_width = query_weight.shape[1] // share
        entry = fetch(jnp.concatenate([columns_of(gate_weight), columns_of(up_weight)], axis=2))
        factors = split_three(down_scale) + split_three(output_scale)
        factors = jnp.stack(factors + [jnp.zeros_like(factors[0])] * 10)
        leave_piece = jnp.concatenate(
            [
                rows_of(down_weight),
                rows_of(output_weight),
                jnp.broadcast_to(factors[None], (share,) + factors.shape),
            ],
            axis=1,
        )
        first_input = collect_rows(residual_in, gain_first)
        leave_piece, entry = lax.optimization_barrier((leave_piece, entry)) if False else (leave_piece, entry)
        leave = fetch(leave_piece)
        project_piece = jnp.concatenate(
            [columns_of(query_weight), columns_of(key_weight), columns_of(value_weight)], axis=2
        )
        project_piece, leave = lax.optimization_barrier((project_piece, leave)) if False else (project_piece, leave)
        project = fetch(project_piece)

        entry = entry.reshape(-1, 2 * hidden_width)
        project = project.reshape(-1, 3 * mix_width)
        if STRIDED:
            leave = leave.swapaxes(0, 1)
        leave = leave.transpose(2, 0, 1, 3).reshape(leave.shape[2], -1)
        down_full = leave[:hidden_width]
        output_full = leave[hidden_width : hidden_width + mix_width]
        parts = leave[hidden_width + mix_width :].astype(jnp.float32)
        down_factor = parts[0] + parts[1] + parts[2]
        output_factor = parts[3] + parts[4] + parts[5]
        gate_own, up_own = own(gate_scale, rank), own(up_scale, rank)

        def half_step(inputs):
            both = jnp.dot(inputs, entry, preferred_element_type=jnp.float32)
            gate_pre = both[:, :hidden_width] * gate_own
            up_pre = both[:, hidden_width:] * up_own
            hidden = (jax.nn.silu(gate_pre) * up_pre).astype(jnp.bfloat16)
            return return_rows(hidden, down_full, down_factor)

        mlp_first = half_step(first_input)
        middle = (residual_in.astype(jnp.float32) + 0.5 * mlp_first).astype(jnp.bfloat16)
        mixer_input = collect_rows(middle, gain_mixer)
        both = jnp.dot(mixer_input, project, preferred_element_type=jnp.float32)
        scale = jnp.concatenate([own(v, rank) for v in (query_scale, key_scale, value_scale)])
        length = residual_in.shape[0] * n_tp
        heads_own = mix_width // HEAD_DIM
        both = (both * scale).reshape(share, length, 3, heads_own, HEAD_DIM)
        first_head = (lax.axis_index("tp") * share + rank) * heads_own
        decay_rates = head_rates(first_head, heads_own, length)
        mixed = jax.vmap(lambda t: retention(t[:, 0], t[:, 1], t[:, 2], decay_rates))(both)
        mixer_out = return_rows(mixed.reshape(share * length, mix_width), output_full, output_factor)
        second = (middle.astype(jnp.float32) + mixer_out).astype(jnp.bfloat16)
        mlp_second = half_step(collect_rows(second, gain_second))
        return (second.astype(jnp.float32) + 0.5 * mlp_second).astype(jnp.bfloat16)

    return body


MESH = pl.DeviceIdType.MESH
GU, DN, QKV, OUT, SC = range(5)
FAR_FIRST = ((1, 0, 0), (1, 1, 0), (1, 0, 1), (1, 1, 1), (0, 1, 0), (0, 1, 1), (0, 0, 1))
TEAM = ((1, 1), (1, 0), (0, 1))
LAG_REDUCE, LAG_FINISH, LAG_PASS = 1, 3, 5


def fused_kernel(
    res_ref, g1_ref, g2_ref, g3_ref,
    gate_ref, up_ref, down_ref, q_ref, k_ref, v_ref, o_ref,
    gs_ref, us_ref, qs_ref, ks_ref, vs_ref, scales_ref, cos_ref, sin_ref,
    out_ref,
    rows_raw, rows_normed, w_gu, w_d, w_qkv, w_o, w_sc,
    st_gu, st_d, st_qkv, st_o, acc, hidden, mixed, part, part_twin, chip_part, far_part,
    w_recv, w_send, w_fwd, ag_recv, ag_send, tw_recv, tw_send, rs_recv, rs_send,
):
    f32, bf16 = jnp.float32, jnp.bfloat16
    f, t = lax.axis_index("fs"), lax.axis_index("tp")
    x, y, z = f % 2, (f // 2) % 2, f // 4
    zl, zh = z % 2, z // 2
    me = zl * 2 + x
    own = res_ref.shape[0]
    width = res_ref.shape[1]
    seq = 2 * own
    ff = hidden.shape[1]
    hd = mixed.shape[1]
    piece = gate_ref.shape[0]
    chunk = 2 * piece
    chunks = width // chunk
    f_y = z * 4 + (1 - y) * 2 + x

    def plane_peer(dh, dl, dx):
        hh, ll, xx = (zh + dh) % 2, (zl + dl) % 2, (x + dx) % 2
        return (2 * hh + ll) * 4 + y * 2 + xx, ll * 2 + xx

    def remote(src, dst, send, recv, fs, tp):
        return pltpu.make_async_remote_copy(
            src_ref=src, dst_ref=dst, send_sem=send, recv_sem=recv, device_id=(fs, tp), device_id_type=MESH
        )

    barrier = pltpu.get_barrier_semaphore()
    for dh, dl, dx in FAR_FIRST:
        peer, _ = plane_peer(dh, dl, dx)
        pl.semaphore_signal(barrier, inc=1, device_id=(peer, t), device_id_type=MESH)
    pl.semaphore_signal(barrier, inc=1, device_id=(f_y, t), device_id_type=MESH)
    pl.semaphore_signal(barrier, inc=1, device_id=(f, 1 - t), device_id_type=MESH)
    pl.semaphore_wait(barrier, 9)

    def slot(kind, s):
        if kind == GU:
            return w_gu.at[pl.ds(pl.multiple_of(s * piece, piece), piece), :]
        if kind == DN:
            return w_d.at[:, pl.ds(pl.multiple_of(s * piece, piece), piece)]
        if kind == QKV:
            return w_qkv.at[pl.ds(pl.multiple_of(s * piece, piece), piece), :]
        if kind == OUT:
            return w_o.at[:, pl.ds(pl.multiple_of(s * piece, piece), piece)]
        return w_sc.at[pl.ds(pl.multiple_of(s * 8, 8), 8), :]

    def staged(kind, m):
        if kind == SC:
            return scales_ref
        return {GU: st_gu, DN: st_d, QKV: st_qkv, OUT: st_o}[kind].at[m]

    def send_pieces(kind):
        remote(staged(kind, me), slot(kind, f), w_fwd.at[kind, me], w_recv.at[kind, f], f_y, t).start()
        for i, (dh, dl, dx) in enumerate(FAR_FIRST):
            peer, m = plane_peer(dh, dl, dx)
            remote(staged(kind, m), slot(kind, f), w_send.at[kind, i], w_recv.at[kind, f], peer, t).start()
        slot(kind, f)[...] = staged(kind, me)[...]

    def pair_base(j):
        zz = 2 * ((zh + (j // 2) % 2) % 2) + j % 2
        return zz * 4 + ((y + j // 4) % 2) * 2

    def take_pair(kind, j):
        base = pair_base(j)
        for xx in (0, 1):
            s = base + xx

            @pl.when(s != f)
            def _():
                remote(slot(kind, s), slot(kind, s), w_fwd.at[kind, 0], w_recv.at[kind, s], f_y, t).wait_recv()

            @pl.when((s != f) & (j < 4))
            def _():
                remote(
                    slot(kind, s), slot(kind, s), w_fwd.at[kind, (j % 4) * 2 + xx], w_recv.at[kind, s], f_y, t
                ).start()

    def take_all(kind):
        def step(j, _):
            take_pair(kind, j)
            return 0

        lax.fori_loop(0, 8, step, 0)

    def finish_sends(kind):
        for i, (dh, dl, dx) in enumerate(FAR_FIRST):
            peer, m = plane_peer(dh, dl, dx)
            remote(staged(kind, m), slot(kind, f), w_send.at[kind, i], w_recv.at[kind, f], peer, t).wait_send()
        for i in range(8):
            remote(slot(kind, f), slot(kind, f), w_fwd.at[kind, i], w_recv.at[kind, f], f_y, t).wait_send()

    def block_rows(m, core):
        return pl.ds(pl.multiple_of((m * 2 + core) * own, own), own)

    def column(j):
        return pl.multiple_of(pair_base(j) * piece, chunk)

    def ag_copy(j, i, src, m, core, fs, tp):
        dst = rows_raw.at[block_rows(m, core), pl.ds(column(j), chunk)]
        return remote(dst if src is None else src, dst, ag_send.at[j, i], ag_recv.at[j, m * 2 + core], fs, tp)

    def ag_start(j, src):
        for i, (dl, dx) in enumerate(TEAM):
            peer, _ = plane_peer(0, dl, dx)
            ag_copy(j, i, src, me, t, peer, t).start()
        ag_copy(j, 3, src, me, t, f, 1 - t).start()

    def ag_pass(j):
        for i, (dl, dx) in enumerate(TEAM):
            _, m = plane_peer(0, dl, dx)
            ag_copy(j, 4 + i, None, m, t, f, 1 - t).wait_recv()
            ag_copy(j, 4 + i, None, m, t, f, 1 - t).start()

    def ag_finish():
        def step(j, _):
            for m in range(4):
                ag_copy(j, 0, None, m, 1 - t, f, 1 - t).wait_recv()
            for i in range(7):
                ag_copy(j, i, None, me, t, f, 1 - t).wait_send()
            return 0

        lax.fori_loop(0, chunks, step, 0)

    def norm_rows(gain_ref):
        def step(i, _):
            at = pl.ds(pl.multiple_of(i * 32, 32), 32)
            v = rows_raw[at, :].astype(f32)
            r = lax.rsqrt(jnp.mean(v * v, axis=-1, keepdims=True) + EPSILON)
            rows_normed[at, :] = (v * r * gain_ref[...]).astype(bf16)
            return 0

        lax.fori_loop(0, rows_raw.shape[0] // 32, step, 0)

    def row_tiles(size, body):
        def step(i, _):
            body(pl.ds(pl.multiple_of(i * size, size), size))
            return 0

        lax.fori_loop(0, rows_raw.shape[0] // size, step, 0)

    def accumulate(kind, weights, columns):
        def step(j, _):
            take_pair(kind, j)
            at = pl.ds(column(j), chunk)

            def tile(r):
                acc[r, :columns] += jnp.dot(rows_normed[r, at], weights[at, :], preferred_element_type=f32)

            row_tiles(seq, tile)
            return 0

        def clear(r):
            acc[r, :columns] = jnp.zeros((seq, columns), f32)

        row_tiles(seq, clear)
        lax.fori_loop(0, 8, step, 0)

    def silu_mul(gate, up):
        gate = gate * gs_ref[...]
        return (gate / (1.0 + jnp.exp(-gate)) * (up * us_ref[...])).astype(bf16)

    def leave(inputs, weights, scale_row, factor, arriving, last):
        def product(j):
            if arriving is not None:
                take_pair(arriving, j)
            base = pair_base(j)
            at = pl.ds(column(j), chunk)
            factors = jnp.concatenate(
                [w_sc[pl.ds((base + h) * 8 + scale_row, 1), :] for h in (0, 1)], axis=1
            )

            def step(m, _):
                r = pl.ds(pl.multiple_of(m * seq, seq), seq)
                term = jnp.dot(inputs[r, :], weights[:, at], preferred_element_type=f32) * factors
                term = term.astype(bf16)
                part[0, m, :, at] = term[:own]
                part[1, m, :, at] = term[own:]
                return 0

            lax.fori_loop(0, 4, step, 0)
            to_twin(j).start()

        def to_twin(j):
            at = pl.ds(column(j), chunk)
            return remote(part.at[1 - t, :, :, at], part_twin.at[:, :, at], tw_send.at[j], tw_recv.at[j], f, 1 - t)

        def to_team(j, i):
            dl, dx = TEAM[i]
            at = pl.ds(column(j), chunk)
            peer, _ = plane_peer(0, dl, dx)
            return remote(chip_part.at[i, :, at], far_part.at[i, :, at], rs_send.at[j, i], rs_recv.at[j, i], peer, t)

        def reduce(j):
            at = pl.ds(column(j), chunk)
            to_twin(j).wait_recv()
            for i, (dl, dx) in enumerate(TEAM):
                _, m = plane_peer(0, dl, dx)
                chip_part[i, :, at] = (part[t, m, :, at].astype(f32) + part_twin[m, :, at].astype(f32)).astype(bf16)
                to_team(j, i).start()

        def finish(j):
            at = pl.ds(column(j), chunk)
            total = part[t, me, :, at].astype(f32) + part_twin[me, :, at].astype(f32)
            for i in range(3):
                to_team(j, i).wait_recv()
                total = total + far_part[i, :, at].astype(f32)
            mine = block_rows(me, t)
            fresh = (rows_raw[mine, at].astype(f32) + factor * total).astype(bf16)
            if last:
                out_ref[:, at] = fresh
            else:
                rows_raw[mine, at] = fresh
                ag_start(j, None)

        def step(i, _):
            pl.when(i < chunks)(lambda: product(i))
            j_reduce, j_finish, j_pass = i - LAG_REDUCE, i - LAG_FINISH, i - LAG_PASS
            pl.when((j_reduce >= 0) & (j_reduce < chunks))(lambda: reduce(j_reduce))
            pl.when((j_finish >= 0) & (j_finish < chunks))(lambda: finish(j_finish))
            if not last:
                pl.when(j_pass >= 0)(lambda: ag_pass(j_pass))
            return 0

        lax.fori_loop(0, chunks + (LAG_FINISH if last else LAG_PASS), step, 0)

        def drain(j, _):
            to_twin(j).wait_send()
            for i in range(3):
                to_team(j, i).wait_send()
            return 0

        lax.fori_loop(0, chunks, drain, 0)
        if not last:
            ag_finish()

    def first_rows(j, _):
        ag_start(j, res_ref.at[:, pl.ds(column(j), chunk)])
        return 0

    lax.fori_loop(0, chunks, first_rows, 0)
    rows_raw[block_rows(me, t), :] = res_ref[...]

    send_pieces(SC)
    for m in range(4):
        at = slice(m * ff, (m + 1) * ff)
        st_gu[m, :, :ff] = gate_ref[:, at].astype(bf16)
        st_gu[m, :, ff:] = up_ref[:, at].astype(bf16)
    send_pieces(GU)
    for m in range(4):
        st_d[m] = down_ref[m * ff : (m + 1) * ff, :].astype(bf16)
    send_pieces(DN)
    for m in range(4):
        at = slice(m * hd, (m + 1) * hd)
        st_qkv[m, :, :hd] = q_ref[:, at].astype(bf16)
        st_qkv[m, :, hd : 2 * hd] = k_ref[:, at].astype(bf16)
        st_qkv[m, :, 2 * hd :] = v_ref[:, at].astype(bf16)
        st_o[m] = o_ref[at, :].astype(bf16)
    send_pieces(QKV)
    send_pieces(OUT)

    def first_pass(j, _):
        ag_pass(j)
        return 0

    lax.fori_loop(0, chunks, first_pass, 0)
    ag_finish()
    norm_rows(g1_ref)
    take_all(SC)

    accumulate(GU, w_gu, 2 * ff)

    def first_hidden(r):
        hidden[r, :] = silu_mul(acc[r, :ff], acc[r, ff:])

    row_tiles(own, first_hidden)
    leave(hidden, w_d, 0, 0.5, DN, False)

    norm_rows(g2_ref)
    accumulate(QKV, w_qkv, 3 * hd)
    take_all(OUT)
    head = (t * 4 + me).astype(f32)
    ri = lax.broadcasted_iota(jnp.int32, (seq, seq), 0)
    ci = lax.broadcasted_iota(jnp.int32, (seq, seq), 1)
    rate = jnp.exp(math.log(1.0 / 16.0) + jnp.full((seq, seq), head, f32) / (HEADS - 1) * math.log(4.0 / seq))
    distance = jnp.maximum(ri - ci, 0).astype(f32)
    decay = jnp.where(ri >= ci, jnp.exp(-rate * distance), 0.0) * hd ** (-0.5)

    def turn(values):
        a, b = values[:, : hd // 2], values[:, hd // 2 :]
        c, s = cos_ref[...], sin_ref[...]
        return jnp.concatenate([a * c - b * s, b * c + a * s], axis=1).astype(bf16)

    def sequence(r):
        q = turn(acc[r, :hd] * qs_ref[...])
        k = turn(acc[r, hd : 2 * hd] * ks_ref[...])
        v = (acc[r, 2 * hd : 3 * hd] * vs_ref[...]).astype(bf16)
        scores = lax.dot_general(q, k, (((1,), (1,)), ((), ())), preferred_element_type=f32)
        both = jnp.dot((scores * decay).astype(bf16), v, preferred_element_type=f32)
        level = jnp.maximum(jnp.mean(both * both, axis=-1, keepdims=True), HEAD_FLOOR)
        mixed[r, :] = (both * lax.rsqrt(level)).astype(bf16)

    row_tiles(seq, sequence)
    leave(mixed, w_o, 1, 1.0, None, False)

    norm_rows(g3_ref)

    def second_hidden(r):
        gate = jnp.dot(rows_normed[r, :], w_gu[:, :ff], preferred_element_type=f32)
        up = jnp.dot(rows_normed[r, :], w_gu[:, ff:], preferred_element_type=f32)
        hidden[r, :] = silu_mul(gate, up)

    row_tiles(seq, second_hidden)
    leave(hidden, w_d, 0, 0.5, None, True)
    for kind in (SC, GU, DN, QKV, OUT):
        finish_sends(kind)


def fused_body(
    residual_in, gain_first, gain_mixer, gain_second,
    gate_weight, gate_scale, up_weight, up_scale, down_weight, down_scale,
    query_weight, query_scale, key_weight, key_scale, value_weight, value_scale,
    output_weight, output_scale,
):
    f32, bf16 = jnp.float32, jnp.bfloat16
    own, width = residual_in.shape
    rows, piece = 8 * own, gate_weight.shape[0]
    ff, hd = gate_weight.shape[1] // 4, query_weight.shape[1] // 4
    chunks = width // (2 * piece)
    x, z = lax.axis_index("fs") % 2, lax.axis_index("fs") // 4
    me = (z % 2) * 2 + x

    def part_of(vector, size):
        return lax.dynamic_slice_in_dim(vector, me * size, size).reshape(1, -1)

    scales = jnp.concatenate([down_scale[None], output_scale[None], jnp.zeros((6, piece), f32)])
    half = hd // 2
    frequency = np.float32(ROTARY_BASE) ** (-np.arange(half, dtype=np.float32) * np.float32(2.0) / np.float32(hd))
    angles = np.arange(2 * own, dtype=np.float32)[:, None] * frequency.astype(np.float32)[None]
    cosine, sine_value = np.cos(angles).astype(np.float32), np.sin(angles).astype(np.float32)
    operands = (
        residual_in, gain_first.reshape(1, -1), gain_mixer.reshape(1, -1), gain_second.reshape(1, -1),
        gate_weight, up_weight, down_weight, query_weight, key_weight, value_weight, output_weight,
        part_of(gate_scale, ff), part_of(up_scale, ff),
        part_of(query_scale, hd), part_of(key_scale, hd), part_of(value_scale, hd),
        scales, jnp.asarray(cosine), jnp.asarray(sine_value),
    )
    dma = pltpu.SemaphoreType.DMA
    return pl.pallas_call(
        fused_kernel,
        out_shape=jax.ShapeDtypeStruct((own, width), bf16),
        in_specs=[pl.BlockSpec(memory_space=pltpu.VMEM)] * len(operands),
        out_specs=pl.BlockSpec(memory_space=pltpu.VMEM),
        scratch_shapes=[
            pltpu.VMEM((rows, width), bf16),
            pltpu.VMEM((rows, width), bf16),
            pltpu.VMEM((width, 2 * ff), bf16),
            pltpu.VMEM((ff, width), bf16),
            pltpu.VMEM((width, 3 * hd), bf16),
            pltpu.VMEM((hd, width), bf16),
            pltpu.VMEM((8 * (width // piece), piece), f32),
            pltpu.VMEM((4, piece, 2 * ff), bf16),
            pltpu.VMEM((4, ff, piece), bf16),
            pltpu.VMEM((4, piece, 3 * hd), bf16),
            pltpu.VMEM((4, hd, piece), bf16),
            pltpu.VMEM((rows, 2 * ff), f32),
            pltpu.VMEM((rows, ff), bf16),
            pltpu.VMEM((rows, hd), bf16),
            pltpu.VMEM((2, 4, own, width), bf16),
            pltpu.VMEM((4, own, width), bf16),
            pltpu.VMEM((3, own, width), bf16),
            pltpu.VMEM((3, own, width), bf16),
            dma((5, 16)), dma((5, 7)), dma((5, 8)),
            dma((chunks, 8)), dma((chunks, 7)),
            dma((chunks,)), dma((chunks,)), dma((chunks, 3)), dma((chunks, 3)),
        ],
        compiler_params=pltpu.CompilerParams(
            collective_id=0, has_side_effects=True, vmem_limit_bytes=63 * 2**20
        ),
    )(*operands)


def solution(mesh):
    n_fs, n_tp = mesh.shape["fs"], mesh.shape["tp"]
    share = math.gcd(math.gcd(HEADS // n_tp, n_fs), 4)
    if (n_fs, n_tp, share) == (16, 2, 4):
        body = fused_body
    else:
        body = make_body(n_fs, n_tp, share)
    in_specs = (
        P(("fs", "tp"), None),
        P(),
        P(),
        P(),
        P("fs", "tp"),
        P("tp"),
        P("fs", "tp"),
        P("tp"),
        P("tp", "fs"),
        P("fs"),
        P("fs", "tp"),
        P("tp"),
        P("fs", "tp"),
        P("tp"),
        P("fs", "tp"),
        P("tp"),
        P("tp", "fs"),
        P("fs"),
    )
    out_specs = P(("fs", "tp"), None)
    return jax.shard_map(body, mesh=mesh, in_specs=in_specs, out_specs=out_specs, check_vma=False)
```

```python
import functools
import math

import jax
import jax.numpy as jnp
import numpy as np
from jax import lax
from jax.experimental import pallas as pl
from jax.experimental.pallas import tpu as pltpu
from jax.sharding import PartitionSpec as P

HEADS = 8
HEAD_DIM = 256
BLOCK = 64


EPSILON = 1e-06
HEAD_FLOOR = 0.25
ROTARY_BASE = 10000.0
HIGHEST = lax.Precision.HIGHEST


def normalize(sequence_rows, gain_vector):
    values = sequence_rows.astype(jnp.float32)
    scaled = values * lax.rsqrt(jnp.mean(values * values, axis=-1, keepdims=True) + EPSILON)
    return (scaled * gain_vector).astype(jnp.bfloat16)


def head_rates(first_head, head_count, length):
    head_number = (first_head + jnp.arange(head_count)).astype(jnp.float32)
    return jnp.exp(jnp.log(1.0 / 16.0) + head_number / (HEADS - 1) * jnp.log(4.0 / length))


def rotate(values, positions):
    half_width = values.shape[-1] // 2
    frequency = ROTARY_BASE ** (-jnp.arange(half_width, dtype=jnp.float32) * 2.0 / values.shape[-1])
    angles = positions[:, None] * frequency[None, :]
    cosine = jnp.cos(angles)[:, None, :]
    sine_value = jnp.sin(angles)[:, None, :]
    front_half = values[..., :half_width]
    back_half = values[..., half_width:]
    return jnp.concatenate(
        [
            front_half * cosine - back_half * sine_value,
            back_half * cosine + front_half * sine_value,
        ],
        axis=-1,
    )


def retention(query_pre, key_pre, value_pre, decay_rates):
    length, head_count, head_width = query_pre.shape
    positions = jnp.arange(length, dtype=jnp.float32)
    query_rot = rotate(query_pre, positions).astype(jnp.bfloat16)
    key_rot = rotate(key_pre, positions).astype(jnp.bfloat16)
    value_low = value_pre.astype(jnp.bfloat16)
    blocks = length // BLOCK
    inside = jnp.arange(BLOCK, dtype=jnp.float32)
    distance = inside[:, None] - inside[None, :]
    within = jnp.where(
        distance >= 0, jnp.exp(-decay_rates[:, None, None] * jnp.maximum(distance, 0.0)), 0.0
    ) * head_width ** (-0.5)
    query_blocks = query_rot.reshape(blocks, BLOCK, head_count, head_width)
    key_blocks = key_rot.reshape(blocks, BLOCK, head_count, head_width)
    value_blocks = value_low.reshape(blocks, BLOCK, head_count, head_width)
    scores = jnp.einsum(
        "nihe,njhe->nhij", query_blocks, key_blocks, preferred_element_type=jnp.float32
    )
    weights = (scores * within[None]).astype(jnp.bfloat16)
    inner_part = jnp.einsum(
        "nhij,njhe->nihe", weights, value_blocks, preferred_element_type=jnp.float32
    )
    fading = jnp.exp(-decay_rates[None, :] * (BLOCK - 1.0 - inside[:, None])) * head_width ** (-0.5)
    key_faded = key_blocks.astype(jnp.float32) * fading[None, :, :, None]
    updates = jnp.einsum(
        "njhd,njhe->nhde", key_faded, value_blocks.astype(jnp.float32), precision=HIGHEST
    )
    block_decay = jnp.exp(-decay_rates * BLOCK)

    def advance(memory_state, update):
        return (memory_state * block_decay[:, None, None] + update, memory_state)

    _, before = lax.scan(
        advance, jnp.zeros((head_count, head_width, head_width), jnp.float32), updates
    )
    rising = jnp.exp(-decay_rates[None, :] * (inside[:, None] + 1.0))
    queried = query_blocks.astype(jnp.float32) * rising[None, :, :, None]
    carried_part = jnp.einsum("nihd,nhde->nihe", queried, before, precision=HIGHEST)
    combined = (inner_part + carried_part).reshape(length, head_count, head_width)
    normed = combined * lax.rsqrt(
        jnp.maximum(jnp.mean(combined * combined, axis=-1, keepdims=True), HEAD_FLOOR)
    )
    return normed.astype(jnp.bfloat16).reshape(length, head_count * head_width)


def split_three(values):
    high = values.astype(jnp.bfloat16)
    rest = values - high.astype(jnp.float32)
    middle_part = rest.astype(jnp.bfloat16)
    low = (rest - middle_part.astype(jnp.float32)).astype(jnp.bfloat16)
    return [high, middle_part, low]


def make_body(n_fs, n_tp, share):
    spread = n_fs // share
    STRIDED = False
    if STRIDED:
        teams = [[m * spread + r for m in range(share)] for r in range(spread)]
    else:
        teams = [[r * share + m for m in range(share)] for r in range(spread)]
    twins = [[team[m] for team in teams] for m in range(share)]
    row_teams = [[f * n_tp + t for f in team for t in range(n_tp)] for team in teams]

    def my_rank():
        position = lax.axis_index("fs")
        return position // spread if STRIDED else position % share

    def fetch(pieces):
        swapped = lax.all_to_all(
            pieces, "fs", split_axis=0, concat_axis=0, axis_index_groups=teams, tiled=True
        )
        return lax.all_gather(swapped, "fs", axis=0, axis_index_groups=twins, tiled=False)

    def order_features(rows):
        if not STRIDED:
            return rows
        count = rows.shape[0]
        return rows.reshape(count, share, spread, -1).swapaxes(1, 2).reshape(count, -1)

    def collect_rows(rows, gain_vector):
        return lax.all_gather(
            order_features(normalize(rows, gain_vector)),
            ("fs", "tp"),
            axis=0,
            axis_index_groups=row_teams,
            tiled=True,
        )

    def return_rows(inputs, weight, factor):
        term = jnp.dot(inputs, weight, preferred_element_type=jnp.float32) * factor
        return lax.psum_scatter(
            term.astype(jnp.bfloat16),
            ("fs", "tp"),
            scatter_dimension=0,
            axis_index_groups=row_teams,
            tiled=True,
        ).astype(jnp.float32)

    def columns_of(weight):
        low = weight.astype(jnp.bfloat16)
        return low.reshape(low.shape[0], share, -1).swapaxes(0, 1)

    def rows_of(weight):
        low = weight.astype(jnp.bfloat16)
        return low.reshape(share, -1, low.shape[1])

    def own(vector, rank):
        width = vector.shape[0] // share
        return lax.dynamic_slice_in_dim(vector, rank * width, width)

    def body(
        residual_in,
        gain_first,
        gain_mixer,
        gain_second,
        gate_weight,
        gate_scale,
        up_weight,
        up_scale,
        down_weight,
        down_scale,
        query_weight,
        query_scale,
        key_weight,
        key_scale,
        value_weight,
        value_scale,
        output_weight,
        output_scale,
    ):
        rank = my_rank()
        hidden_width = gate_weight.shape[1] // share
        mix_width = query_weight.shape[1] // share
        entry = fetch(jnp.concatenate([columns_of(gate_weight), columns_of(up_weight)], axis=2))
        factors = split_three(down_scale) + split_three(output_scale)
        factors = jnp.stack(factors + [jnp.zeros_like(factors[0])] * 10)
        leave_piece = jnp.concatenate(
            [
                rows_of(down_weight),
                rows_of(output_weight),
                jnp.broadcast_to(factors[None], (share,) + factors.shape),
            ],
            axis=1,
        )
        first_input = collect_rows(residual_in, gain_first)
        leave_piece, entry = lax.optimization_barrier((leave_piece, entry)) if False else (leave_piece, entry)
        leave = fetch(leave_piece)
        project_piece = jnp.concatenate(
            [columns_of(query_weight), columns_of(key_weight), columns_of(value_weight)], axis=2
        )
        project_piece, leave = lax.optimization_barrier((project_piece, leave)) if False else (project_piece, leave)
        project = fetch(project_piece)

        entry = entry.reshape(-1, 2 * hidden_width)
        project = project.reshape(-1, 3 * mix_width)
        if STRIDED:
            leave = leave.swapaxes(0, 1)
        leave = leave.transpose(2, 0, 1, 3).reshape(leave.shape[2], -1)
        down_full = leave[:hidden_width]
        output_full = leave[hidden_width : hidden_width + mix_width]
        parts = leave[hidden_width + mix_width :].astype(jnp.float32)
        down_factor = parts[0] + parts[1] + parts[2]
        output_factor = parts[3] + parts[4] + parts[5]
        gate_own, up_own = own(gate_scale, rank), own(up_scale, rank)

        def half_step(inputs):
            both = jnp.dot(inputs, entry, preferred_element_type=jnp.float32)
            gate_pre = both[:, :hidden_width] * gate_own
            up_pre = both[:, hidden_width:] * up_own
            hidden = (jax.nn.silu(gate_pre) * up_pre).astype(jnp.bfloat16)
            return return_rows(hidden, down_full, down_factor)

        mlp_first = half_step(first_input)
        middle = (residual_in.astype(jnp.float32) + 0.5 * mlp_first).astype(jnp.bfloat16)
        mixer_input = collect_rows(middle, gain_mixer)
        both = jnp.dot(mixer_input, project, preferred_element_type=jnp.float32)
        scale = jnp.concatenate([own(v, rank) for v in (query_scale, key_scale, value_scale)])
        length = residual_in.shape[0] * n_tp
        heads_own = mix_width // HEAD_DIM
        both = (both * scale).reshape(share, length, 3, heads_own, HEAD_DIM)
        first_head = (lax.axis_index("tp") * share + rank) * heads_own
        decay_rates = head_rates(first_head, heads_own, length)
        mixed = jax.vmap(lambda t: retention(t[:, 0], t[:, 1], t[:, 2], decay_rates))(both)
        mixer_out = return_rows(mixed.reshape(share * length, mix_width), output_full, output_factor)
        second = (middle.astype(jnp.float32) + mixer_out).astype(jnp.bfloat16)
        mlp_second = half_step(collect_rows(second, gain_second))
        return (second.astype(jnp.float32) + 0.5 * mlp_second).astype(jnp.bfloat16)

    return body


MESH = pl.DeviceIdType.MESH
GU, DN, QKV, OUT, SC = range(5)
PLANE = ((0, 0, 1), (0, 1, 0), (0, 1, 1), (1, 0, 0), (1, 1, 0), (1, 0, 1), (1, 1, 1))


def fused_kernel(
    res_ref, g1_ref, g2_ref, g3_ref,
    gate_ref, up_ref, down_ref, q_ref, k_ref, v_ref, o_ref,
    gs_ref, us_ref, qs_ref, ks_ref, vs_ref, ds_ref, os_ref, cos_ref, sin_ref,
    out_ref,
    rows_raw, rows_normed, w_gu, w_d, w_qkv, w_o, w_sc,
    st_gu, st_d, st_qkv, st_o, scales_ref, acc, hidden, mixed, part, part_twin, chip_part, far_part,
    w_recv, w_send, w_fwd, ag_recv, ag_send, tw_recv, tw_send, rs_recv, rs_send,
):
    f32, bf16 = jnp.float32, jnp.bfloat16
    f, t = lax.axis_index("fs"), lax.axis_index("tp")
    x, y, z = f % 2, (f // 2) % 2, f // 4
    zl, zh = z % 2, z // 2
    me = zl * 2 + x
    own = res_ref.shape[0]
    width = res_ref.shape[1]
    seq = 2 * own
    ff = hidden.shape[1]
    hd = mixed.shape[1]
    piece = gate_ref.shape[0]
    chunk = 2 * piece
    chunks = width // chunk
    f_y = z * 4 + (1 - y) * 2 + x

    def plane_peer(dh, dl, dx):
        hh, ll, xx = (zh + dh) % 2, (zl + dl) % 2, (x + dx) % 2
        return (2 * hh + ll) * 4 + y * 2 + xx, ll * 2 + xx

    def remote(src, dst, send, recv, fs, tp):
        return pltpu.make_async_remote_copy(
            src_ref=src, dst_ref=dst, send_sem=send, recv_sem=recv, device_id=(fs, tp), device_id_type=MESH
        )

    barrier = pltpu.get_barrier_semaphore()
    for dh, dl, dx in PLANE:
        peer, _ = plane_peer(dh, dl, dx)
        pl.semaphore_signal(barrier, inc=1, device_id=(peer, t), device_id_type=MESH)
    pl.semaphore_signal(barrier, inc=1, device_id=(f_y, t), device_id_type=MESH)
    pl.semaphore_signal(barrier, inc=1, device_id=(f, 1 - t), device_id_type=MESH)
    pl.semaphore_wait(barrier, 9)

    def slot(kind, s):
        if kind == GU:
            return w_gu.at[pl.ds(pl.multiple_of(s * piece, piece), piece), :]
        if kind == DN:
            return w_d.at[:, pl.ds(pl.multiple_of(s * piece, piece), piece)]
        if kind == QKV:
            return w_qkv.at[pl.ds(pl.multiple_of(s * piece, piece), piece), :]
        if kind == OUT:
            return w_o.at[:, pl.ds(pl.multiple_of(s * piece, piece), piece)]
        return w_sc.at[pl.ds(pl.multiple_of(s * 8, 8), 8), :]

    def staged(kind, m):
        if kind == SC:
            return scales_ref
        return {GU: st_gu, DN: st_d, QKV: st_qkv, OUT: st_o}[kind].at[m]

    def send_pieces(kind):
        own_place = me if kind == DN else x
        remote(staged(kind, me), slot(kind, f), w_fwd.at[kind, own_place], w_recv.at[kind, f], f_y, t).start()
        for i, (dh, dl, dx) in enumerate(PLANE):
            peer, m = plane_peer(dh, dl, dx)
            remote(staged(kind, m), slot(kind, f), w_send.at[kind, i], w_recv.at[kind, f], peer, t).start()
        slot(kind, f)[...] = staged(kind, me)[...]

    def pair_base(j):
        zz = 2 * ((zh + (j // 2) % 2) % 2) + j % 2
        return zz * 4 + ((y + j // 4) % 2) * 2

    def near_base(j):
        zz = 2 * ((zh + (j // 2) % 2) % 2) + (zl + j) % 2
        return zz * 4 + ((y + j // 4) % 2) * 2

    def take_pair(kind, j):
        base = pair_base(j) if kind == DN else near_base(j)
        for xx in (0, 1):
            s = base + xx

            @pl.when(s != f)
            def _():
                remote(slot(kind, s), slot(kind, s), w_fwd.at[kind, 0], w_recv.at[kind, s], f_y, t).wait_recv()

            @pl.when((s != f) & (j < 4))
            def _():
                remote(
                    slot(kind, s), slot(kind, s), w_fwd.at[kind, (j % 4) * 2 + xx], w_recv.at[kind, s], f_y, t
                ).start()

    def take_all(kind):
        def step(j, _):
            take_pair(kind, j)
            return 0

        lax.fori_loop(0, 8, step, 0)

    def finish_sends(kind):
        for i, (dh, dl, dx) in enumerate(PLANE):
            peer, m = plane_peer(dh, dl, dx)
            remote(staged(kind, m), slot(kind, f), w_send.at[kind, i], w_recv.at[kind, f], peer, t).wait_send()
        for i in range(8):
            remote(slot(kind, f), slot(kind, f), w_fwd.at[kind, i], w_recv.at[kind, f], f_y, t).wait_send()

    def block_rows(m, core):
        return pl.ds(pl.multiple_of((m * 2 + core) * own, own), own)

    def column(j):
        return pl.multiple_of(pair_base(j) * piece, chunk)

    def ag_copy(j, i, src, m, core, fs, tp):
        dst = rows_raw.at[block_rows(m, core), pl.ds(column(j), chunk)]
        return remote(dst if src is None else src, dst, ag_send.at[j, i], ag_recv.at[j, m * 2 + core], fs, tp)

    def way(dl, dx):
        first, m_first = plane_peer(0, dl, dx)
        second, m_second = plane_peer(0, 1 - dl, 1 - dx)
        return first, second, m_first, m_second, plane_peer(0, 1, 1)[1]

    z_then_x, x_then_z, by_core = way(1, 0), way(0, 1), way(t, 1 - t)

    def ag_start(j, src, route):
        first, second, _, _, _ = route
        ag_copy(j, 0, src, me, t, first, t).start()
        ag_copy(j, 1, src, me, t, second, t).start()
        ag_copy(j, 2, src, me, t, f, 1 - t).start()

    def ag_relay(j, route):
        _, second, m_first, _, _ = route
        ag_copy(j, 3, None, m_first, t, second, t).wait_recv()
        ag_copy(j, 3, None, m_first, t, second, t).start()
        ag_copy(j, 4, None, m_first, t, f, 1 - t).start()

    def ag_pass(j, route):
        for i, m in enumerate(route[3:]):
            ag_copy(j, 5 + i, None, m, t, f, 1 - t).wait_recv()
            ag_copy(j, 5 + i, None, m, t, f, 1 - t).start()

    def ag_finish():
        def step(j, _):
            for m in range(4):
                ag_copy(j, 0, None, m, 1 - t, f, 1 - t).wait_recv()
            for i in range(7):
                ag_copy(j, i, None, me, t, f, 1 - t).wait_send()
            return 0

        lax.fori_loop(0, chunks, step, 0)

    def norm_rows(gain_ref):
        def step(i, _):
            at = pl.ds(pl.multiple_of(i * 32, 32), 32)
            v = rows_raw[at, :].astype(f32)
            r = lax.rsqrt(jnp.mean(v * v, axis=-1, keepdims=True) + EPSILON)
            rows_normed[at, :] = (v * r * gain_ref[...]).astype(bf16)
            return 0

        lax.fori_loop(0, rows_raw.shape[0] // 32, step, 0)

    def row_tiles(size, body):
        def step(i, _):
            body(pl.ds(pl.multiple_of(i * size, size), size))
            return 0

        lax.fori_loop(0, rows_raw.shape[0] // size, step, 0)

    def clear(columns):
        def tile(r):
            acc[r, :columns] = jnp.zeros((seq, columns), f32)

        row_tiles(seq, tile)

    def accumulate(kind, weights, columns, begin, end, take):
        def step(j, _):
            if take:
                take_pair(kind, j)
            at = pl.ds(pl.multiple_of(near_base(j) * piece, chunk), chunk)

            def tile(r):
                acc[r, :columns] += jnp.dot(rows_normed[r, at], weights[at, :], preferred_element_type=f32)

            row_tiles(seq, tile)
            return 0

        lax.fori_loop(begin, end, step, 0)

    def silu_mul(gate, up):
        gate = gate * gs_ref[:, pl.ds(pl.multiple_of(me * ff, ff), ff)]
        return (gate / (1.0 + jnp.exp(-gate)) * (up * us_ref[:, pl.ds(pl.multiple_of(me * ff, ff), ff)])).astype(bf16)

    def leave(inputs, weights, scale_row, factor, arriving, last, sums, rows, lags, during=None):
        def product(j):
            if arriving is not None:
                take_pair(arriving, j)
            base = pair_base(j)
            at = pl.ds(column(j), chunk)
            factors = jnp.concatenate(
                [w_sc[pl.ds((base + h) * 8 + scale_row, 1), :] for h in (0, 1)], axis=1
            )

            def step(m, _):
                r = pl.ds(pl.multiple_of(m * seq, seq), seq)
                term = jnp.dot(inputs[r, :], weights[:, at], preferred_element_type=f32) * factors
                term = term.astype(bf16)
                part[0, m, :, at] = term[:own]
                part[1, m, :, at] = term[own:]
                return 0

            lax.fori_loop(0, 4, step, 0)
            to_twin(j).start()

        def to_twin(j):
            at = pl.ds(column(j), chunk)
            return remote(part.at[1 - t, :, :, at], part_twin.at[:, :, at], tw_send.at[j], tw_recv.at[j], f, 1 - t)

        first, second, m_first, m_second, m_third = sums

        def to_first(j):
            at = pl.ds(column(j), chunk)
            pair = pl.ds(0, 2)
            return remote(
                chip_part.at[pair, :, at], far_part.at[pair, :, at], rs_send.at[j, 0], rs_recv.at[j, 0], first, t
            )

        def to_second(j):
            at = pl.ds(column(j), chunk)
            return remote(chip_part.at[2, :, at], far_part.at[2, :, at], rs_send.at[j, 1], rs_recv.at[j, 1], second, t)

        def chip_sum(m, at):
            return part[t, m, :, at].astype(f32) + part_twin[m, :, at].astype(f32)

        def reduce(j):
            at = pl.ds(column(j), chunk)
            to_twin(j).wait_recv()
            chip_part[0, :, at] = chip_sum(m_first, at).astype(bf16)
            chip_part[1, :, at] = chip_sum(m_third, at).astype(bf16)
            to_first(j).start()

        def relay(j):
            at = pl.ds(column(j), chunk)
            to_first(j).wait_recv()
            chip_part[2, :, at] = (chip_sum(m_second, at) + far_part[1, :, at].astype(f32)).astype(bf16)
            to_second(j).start()

        def finish(j):
            at = pl.ds(column(j), chunk)
            to_second(j).wait_recv()
            total = chip_sum(me, at) + far_part[0, :, at].astype(f32) + far_part[2, :, at].astype(f32)
            mine = block_rows(me, t)
            fresh = (rows_raw[mine, at].astype(f32) + factor * total).astype(bf16)
            if last:
                out_ref[:, at] = fresh
            else:
                rows_raw[mine, at] = fresh
                ag_start(j, None, rows)

        stages = [product, reduce, relay, finish]
        if not last:
            stages += [lambda j: ag_relay(j, rows), lambda j: ag_pass(j, rows)]

        def step(i, _):
            for lag, stage in zip(lags, stages):
                pl.when((i >= lag) & (i < chunks + lag))(lambda stage=stage, lag=lag: stage(i - lag))
            if during is not None:
                during(i)
            return 0

        lax.fori_loop(0, chunks + lags[len(stages) - 1], step, 0)

        def drain(j, _):
            to_twin(j).wait_send()
            to_first(j).wait_send()
            to_second(j).wait_send()
            return 0

        lax.fori_loop(0, chunks, drain, 0)
        if not last:
            ag_finish()

    def each_chunk(body):
        def step(j, _):
            body(j)
            return 0

        lax.fori_loop(0, chunks, step, 0)

    scales_ref[...] = jnp.zeros_like(scales_ref)
    scales_ref[0:1, :] = ds_ref[...]
    scales_ref[1:2, :] = os_ref[...]
    send_pieces(SC)

    each_chunk(lambda j: ag_start(j, res_ref.at[:, pl.ds(column(j), chunk)], z_then_x))
    rows_raw[block_rows(me, t), :] = res_ref[...]

    for m in range(4):
        at = slice(m * ff, (m + 1) * ff)
        st_gu[m, :, :ff] = gate_ref[:, at].astype(bf16)
        st_gu[m, :, ff:] = up_ref[:, at].astype(bf16)
    send_pieces(GU)
    for m in range(4):
        st_d[m] = down_ref[m * ff : (m + 1) * ff, :].astype(bf16)
    send_pieces(DN)
    for m in range(4):
        at = slice(m * hd, (m + 1) * hd)
        st_qkv[m, :, :hd] = q_ref[:, at].astype(bf16)
        st_qkv[m, :, hd : 2 * hd] = k_ref[:, at].astype(bf16)
        st_qkv[m, :, 2 * hd :] = v_ref[:, at].astype(bf16)
        st_o[m] = o_ref[at, :].astype(bf16)
    send_pieces(QKV)
    send_pieces(OUT)

    clear(2 * ff)
    each_chunk(lambda j: ag_relay(j, z_then_x))
    for j in range(3):
        take_pair(GU, j)
    each_chunk(lambda j: ag_pass(j, z_then_x))
    ag_finish()
    norm_rows(g1_ref)
    take_pair(GU, 3)
    accumulate(GU, w_gu, 2 * ff, 0, 4, False)
    accumulate(GU, w_gu, 2 * ff, 4, 8, True)
    take_all(SC)

    def first_hidden(r):
        hidden[r, :] = silu_mul(acc[r, :ff], acc[r, ff:])

    row_tiles(own, first_hidden)

    def take_qkv(i):
        pl.when((i >= 7) & (i < 15) & (i % 2 == 1))(lambda: take_pair(QKV, (i - 7) // 2))

    leave(hidden, w_d, 0, 0.5, DN, False, x_then_z, z_then_x, (0, 1, 4, 6, 7, 8), take_qkv)

    norm_rows(g2_ref)
    clear(3 * hd)
    accumulate(QKV, w_qkv, 3 * hd, 0, 4, False)
    accumulate(QKV, w_qkv, 3 * hd, 4, 8, True)
    take_all(OUT)
    head = (t * 4 + me).astype(f32)
    ri = lax.broadcasted_iota(jnp.int32, (seq, seq), 0)
    ci = lax.broadcasted_iota(jnp.int32, (seq, seq), 1)
    rate = jnp.exp(math.log(1.0 / 16.0) + jnp.full((seq, seq), head, f32) / (HEADS - 1) * math.log(4.0 / seq))
    distance = jnp.maximum(ri - ci, 0).astype(f32)
    decay = jnp.where(ri >= ci, jnp.exp(-rate * distance), 0.0) * hd ** (-0.5)

    at_head = pl.ds(pl.multiple_of(me * hd, hd), hd)

    def turn(values):
        a, b = values[:, : hd // 2], values[:, hd // 2 :]
        c, s = cos_ref[...], sin_ref[...]
        return jnp.concatenate([a * c - b * s, b * c + a * s], axis=1).astype(bf16)

    def sequence(r):
        q = turn(acc[r, :hd] * qs_ref[:, at_head])
        k = turn(acc[r, hd : 2 * hd] * ks_ref[:, at_head])
        v = (acc[r, 2 * hd : 3 * hd] * vs_ref[:, at_head]).astype(bf16)
        scores = lax.dot_general(q, k, (((1,), (1,)), ((), ())), preferred_element_type=f32)
        both = jnp.dot((scores * decay).astype(bf16), v, preferred_element_type=f32)
        level = jnp.maximum(jnp.mean(both * both, axis=-1, keepdims=True), HEAD_FLOOR)
        mixed[r, :] = (both * lax.rsqrt(level)).astype(bf16)

    row_tiles(seq, sequence)
    leave(mixed, w_o, 1, 1.0, None, False, by_core, by_core, (0, 1, 3, 5, 7, 9))

    norm_rows(g3_ref)

    def second_hidden(r):
        gate = jnp.dot(rows_normed[r, :], w_gu[:, :ff], preferred_element_type=f32)
        up = jnp.dot(rows_normed[r, :], w_gu[:, ff:], preferred_element_type=f32)
        hidden[r, :] = silu_mul(gate, up)

    row_tiles(seq, second_hidden)
    leave(hidden, w_d, 0, 0.5, None, True, by_core, by_core, (0, 1, 3, 5))
    for kind in (SC, GU, DN, QKV, OUT):
        finish_sends(kind)


def fused_body(
    residual_in, gain_first, gain_mixer, gain_second,
    gate_weight, gate_scale, up_weight, up_scale, down_weight, down_scale,
    query_weight, query_scale, key_weight, key_scale, value_weight, value_scale,
    output_weight, output_scale,
):
    f32, bf16 = jnp.float32, jnp.bfloat16
    own, width = residual_in.shape
    rows, piece = 8 * own, gate_weight.shape[0]
    ff, hd = gate_weight.shape[1] // 4, query_weight.shape[1] // 4
    chunks = width // (2 * piece)

    def row(vector):
        return vector.reshape(1, -1)

    half = hd // 2
    frequency = np.float32(ROTARY_BASE) ** (-np.arange(half, dtype=np.float32) * np.float32(2.0) / np.float32(hd))
    angles = np.arange(2 * own, dtype=np.float32)[:, None] * frequency.astype(np.float32)[None]
    cosine, sine_value = np.cos(angles).astype(np.float32), np.sin(angles).astype(np.float32)
    operands = (
        residual_in, row(gain_first), row(gain_mixer), row(gain_second),
        gate_weight, up_weight, down_weight, query_weight, key_weight, value_weight, output_weight,
        row(gate_scale), row(up_scale), row(query_scale), row(key_scale), row(value_scale),
        row(down_scale), row(output_scale), jnp.asarray(cosine), jnp.asarray(sine_value),
    )
    dma = pltpu.SemaphoreType.DMA
    return pl.pallas_call(
        fused_kernel,
        out_shape=jax.ShapeDtypeStruct((own, width), bf16),
        in_specs=[pl.BlockSpec(memory_space=pltpu.VMEM)] * len(operands),
        out_specs=pl.BlockSpec(memory_space=pltpu.VMEM),
        scratch_shapes=[
            pltpu.VMEM((rows, width), bf16),
            pltpu.VMEM((rows, width), bf16),
            pltpu.VMEM((width, 2 * ff), bf16),
            pltpu.VMEM((ff, width), bf16),
            pltpu.VMEM((width, 3 * hd), bf16),
            pltpu.VMEM((hd, width), bf16),
            pltpu.VMEM((8 * (width // piece), piece), f32),
            pltpu.VMEM((4, piece, 2 * ff), bf16),
            pltpu.VMEM((4, ff, piece), bf16),
            pltpu.VMEM((4, piece, 3 * hd), bf16),
            pltpu.VMEM((4, hd, piece), bf16),
            pltpu.VMEM((8, piece), f32),
            pltpu.VMEM((rows, 2 * ff), f32),
            pltpu.VMEM((rows, ff), bf16),
            pltpu.VMEM((rows, hd), bf16),
            pltpu.VMEM((2, 4, own, width), bf16),
            pltpu.VMEM((4, own, width), bf16),
            pltpu.VMEM((3, own, width), bf16),
            pltpu.VMEM((3, own, width), bf16),
            dma((5, 16)), dma((5, 7)), dma((5, 8)),
            dma((chunks, 8)), dma((chunks, 7)),
            dma((chunks,)), dma((chunks,)), dma((chunks, 2)), dma((chunks, 2)),
        ],
        compiler_params=pltpu.CompilerParams(
            collective_id=0, has_side_effects=True, vmem_limit_bytes=63 * 2**20
        ),
    )(*operands)


def solution(mesh):
    n_fs, n_tp = mesh.shape["fs"], mesh.shape["tp"]
    share = math.gcd(math.gcd(HEADS // n_tp, n_fs), 4)
    if (n_fs, n_tp, share) == (16, 2, 4):
        body = fused_body
    else:
        body = make_body(n_fs, n_tp, share)
    in_specs = (
        P(("fs", "tp"), None),
        P(),
        P(),
        P(),
        P("fs", "tp"),
        P("tp"),
        P("fs", "tp"),
        P("tp"),
        P("tp", "fs"),
        P("fs"),
        P("fs", "tp"),
        P("tp"),
        P("fs", "tp"),
        P("tp"),
        P("fs", "tp"),
        P("tp"),
        P("tp", "fs"),
        P("fs"),
    )
    out_specs = P(("fs", "tp"), None)
    return jax.shard_map(body, mesh=mesh, in_specs=in_specs, out_specs=out_specs, check_vma=False)
```

```python
import functools
import math

import jax
import jax.numpy as jnp
import numpy as np
from jax import lax
from jax.experimental import pallas as pl
from jax.experimental.pallas import tpu as pltpu
from jax.sharding import PartitionSpec as P

HEADS = 8
HEAD_DIM = 256
BLOCK = 64


EPSILON = 1e-06
HEAD_FLOOR = 0.25
ROTARY_BASE = 10000.0
HIGHEST = lax.Precision.HIGHEST


def normalize(sequence_rows, gain_vector):
    values = sequence_rows.astype(jnp.float32)
    scaled = values * lax.rsqrt(jnp.mean(values * values, axis=-1, keepdims=True) + EPSILON)
    return (scaled * gain_vector).astype(jnp.bfloat16)


def head_rates(first_head, head_count, length):
    head_number = (first_head + jnp.arange(head_count)).astype(jnp.float32)
    return jnp.exp(jnp.log(1.0 / 16.0) + head_number / (HEADS - 1) * jnp.log(4.0 / length))


def rotate(values, positions):
    half_width = values.shape[-1] // 2
    frequency = ROTARY_BASE ** (-jnp.arange(half_width, dtype=jnp.float32) * 2.0 / values.shape[-1])
    angles = positions[:, None] * frequency[None, :]
    cosine = jnp.cos(angles)[:, None, :]
    sine_value = jnp.sin(angles)[:, None, :]
    front_half = values[..., :half_width]
    back_half = values[..., half_width:]
    return jnp.concatenate(
        [
            front_half * cosine - back_half * sine_value,
            back_half * cosine + front_half * sine_value,
        ],
        axis=-1,
    )


def retention(query_pre, key_pre, value_pre, decay_rates):
    length, head_count, head_width = query_pre.shape
    positions = jnp.arange(length, dtype=jnp.float32)
    query_rot = rotate(query_pre, positions).astype(jnp.bfloat16)
    key_rot = rotate(key_pre, positions).astype(jnp.bfloat16)
    value_low = value_pre.astype(jnp.bfloat16)
    blocks = length // BLOCK
    inside = jnp.arange(BLOCK, dtype=jnp.float32)
    distance = inside[:, None] - inside[None, :]
    within = jnp.where(
        distance >= 0, jnp.exp(-decay_rates[:, None, None] * jnp.maximum(distance, 0.0)), 0.0
    ) * head_width ** (-0.5)
    query_blocks = query_rot.reshape(blocks, BLOCK, head_count, head_width)
    key_blocks = key_rot.reshape(blocks, BLOCK, head_count, head_width)
    value_blocks = value_low.reshape(blocks, BLOCK, head_count, head_width)
    scores = jnp.einsum(
        "nihe,njhe->nhij", query_blocks, key_blocks, preferred_element_type=jnp.float32
    )
    weights = (scores * within[None]).astype(jnp.bfloat16)
    inner_part = jnp.einsum(
        "nhij,njhe->nihe", weights, value_blocks, preferred_element_type=jnp.float32
    )
    fading = jnp.exp(-decay_rates[None, :] * (BLOCK - 1.0 - inside[:, None])) * head_width ** (-0.5)
    key_faded = key_blocks.astype(jnp.float32) * fading[None, :, :, None]
    updates = jnp.einsum(
        "njhd,njhe->nhde", key_faded, value_blocks.astype(jnp.float32), precision=HIGHEST
    )
    block_decay = jnp.exp(-decay_rates * BLOCK)

    def advance(memory_state, update):
        return (memory_state * block_decay[:, None, None] + update, memory_state)

    _, before = lax.scan(
        advance, jnp.zeros((head_count, head_width, head_width), jnp.float32), updates
    )
    rising = jnp.exp(-decay_rates[None, :] * (inside[:, None] + 1.0))
    queried = query_blocks.astype(jnp.float32) * rising[None, :, :, None]
    carried_part = jnp.einsum("nihd,nhde->nihe", queried, before, precision=HIGHEST)
    combined = (inner_part + carried_part).reshape(length, head_count, head_width)
    normed = combined * lax.rsqrt(
        jnp.maximum(jnp.mean(combined * combined, axis=-1, keepdims=True), HEAD_FLOOR)
    )
    return normed.astype(jnp.bfloat16).reshape(length, head_count * head_width)


def split_three(values):
    high = values.astype(jnp.bfloat16)
    rest = values - high.astype(jnp.float32)
    middle_part = rest.astype(jnp.bfloat16)
    low = (rest - middle_part.astype(jnp.float32)).astype(jnp.bfloat16)
    return [high, middle_part, low]


def make_body(n_fs, n_tp, share):
    spread = n_fs // share
    STRIDED = False
    if STRIDED:
        teams = [[m * spread + r for m in range(share)] for r in range(spread)]
    else:
        teams = [[r * share + m for m in range(share)] for r in range(spread)]
    twins = [[team[m] for team in teams] for m in range(share)]
    row_teams = [[f * n_tp + t for f in team for t in range(n_tp)] for team in teams]

    def my_rank():
        position = lax.axis_index("fs")
        return position // spread if STRIDED else position % share

    def fetch(pieces):
        swapped = lax.all_to_all(
            pieces, "fs", split_axis=0, concat_axis=0, axis_index_groups=teams, tiled=True
        )
        return lax.all_gather(swapped, "fs", axis=0, axis_index_groups=twins, tiled=False)

    def order_features(rows):
        if not STRIDED:
            return rows
        count = rows.shape[0]
        return rows.reshape(count, share, spread, -1).swapaxes(1, 2).reshape(count, -1)

    def collect_rows(rows, gain_vector):
        return lax.all_gather(
            order_features(normalize(rows, gain_vector)),
            ("fs", "tp"),
            axis=0,
            axis_index_groups=row_teams,
            tiled=True,
        )

    def return_rows(inputs, weight, factor):
        term = jnp.dot(inputs, weight, preferred_element_type=jnp.float32) * factor
        return lax.psum_scatter(
            term.astype(jnp.bfloat16),
            ("fs", "tp"),
            scatter_dimension=0,
            axis_index_groups=row_teams,
            tiled=True,
        ).astype(jnp.float32)

    def columns_of(weight):
        low = weight.astype(jnp.bfloat16)
        return low.reshape(low.shape[0], share, -1).swapaxes(0, 1)

    def rows_of(weight):
        low = weight.astype(jnp.bfloat16)
        return low.reshape(share, -1, low.shape[1])

    def own(vector, rank):
        width = vector.shape[0] // share
        return lax.dynamic_slice_in_dim(vector, rank * width, width)

    def body(
        residual_in,
        gain_first,
        gain_mixer,
        gain_second,
        gate_weight,
        gate_scale,
        up_weight,
        up_scale,
        down_weight,
        down_scale,
        query_weight,
        query_scale,
        key_weight,
        key_scale,
        value_weight,
        value_scale,
        output_weight,
        output_scale,
    ):
        rank = my_rank()
        hidden_width = gate_weight.shape[1] // share
        mix_width = query_weight.shape[1] // share
        entry = fetch(jnp.concatenate([columns_of(gate_weight), columns_of(up_weight)], axis=2))
        factors = split_three(down_scale) + split_three(output_scale)
        factors = jnp.stack(factors + [jnp.zeros_like(factors[0])] * 10)
        leave_piece = jnp.concatenate(
            [
                rows_of(down_weight),
                rows_of(output_weight),
                jnp.broadcast_to(factors[None], (share,) + factors.shape),
            ],
            axis=1,
        )
        first_input = collect_rows(residual_in, gain_first)
        leave_piece, entry = lax.optimization_barrier((leave_piece, entry)) if False else (leave_piece, entry)
        leave = fetch(leave_piece)
        project_piece = jnp.concatenate(
            [columns_of(query_weight), columns_of(key_weight), columns_of(value_weight)], axis=2
        )
        project_piece, leave = lax.optimization_barrier((project_piece, leave)) if False else (project_piece, leave)
        project = fetch(project_piece)

        entry = entry.reshape(-1, 2 * hidden_width)
        project = project.reshape(-1, 3 * mix_width)
        if STRIDED:
            leave = leave.swapaxes(0, 1)
        leave = leave.transpose(2, 0, 1, 3).reshape(leave.shape[2], -1)
        down_full = leave[:hidden_width]
        output_full = leave[hidden_width : hidden_width + mix_width]
        parts = leave[hidden_width + mix_width :].astype(jnp.float32)
        down_factor = parts[0] + parts[1] + parts[2]
        output_factor = parts[3] + parts[4] + parts[5]
        gate_own, up_own = own(gate_scale, rank), own(up_scale, rank)

        def half_step(inputs):
            both = jnp.dot(inputs, entry, preferred_element_type=jnp.float32)
            gate_pre = both[:, :hidden_width] * gate_own
            up_pre = both[:, hidden_width:] * up_own
            hidden = (jax.nn.silu(gate_pre) * up_pre).astype(jnp.bfloat16)
            return return_rows(hidden, down_full, down_factor)

        mlp_first = half_step(first_input)
        middle = (residual_in.astype(jnp.float32) + 0.5 * mlp_first).astype(jnp.bfloat16)
        mixer_input = collect_rows(middle, gain_mixer)
        both = jnp.dot(mixer_input, project, preferred_element_type=jnp.float32)
        scale = jnp.concatenate([own(v, rank) for v in (query_scale, key_scale, value_scale)])
        length = residual_in.shape[0] * n_tp
        heads_own = mix_width // HEAD_DIM
        both = (both * scale).reshape(share, length, 3, heads_own, HEAD_DIM)
        first_head = (lax.axis_index("tp") * share + rank) * heads_own
        decay_rates = head_rates(first_head, heads_own, length)
        mixed = jax.vmap(lambda t: retention(t[:, 0], t[:, 1], t[:, 2], decay_rates))(both)
        mixer_out = return_rows(mixed.reshape(share * length, mix_width), output_full, output_factor)
        second = (middle.astype(jnp.float32) + mixer_out).astype(jnp.bfloat16)
        mlp_second = half_step(collect_rows(second, gain_second))
        return (second.astype(jnp.float32) + 0.5 * mlp_second).astype(jnp.bfloat16)

    return body


MESH = pl.DeviceIdType.MESH
GATE, UP, DN, QKV, OUT, SC = range(6)
PLANE = ((0, 0, 1), (0, 1, 0), (0, 1, 1), (1, 0, 0), (1, 1, 0), (1, 0, 1), (1, 1, 1))


def fused_kernel(
    res_ref, g1_ref, g2_ref, g3_ref,
    gate_ref, up_ref, down_ref, q_ref, k_ref, v_ref, o_ref,
    gs_ref, us_ref, qs_ref, ks_ref, vs_ref, ds_ref, os_ref, cos_ref, sin_ref,
    out_ref,
    rows_raw, rows_normed, w_gu, w_d, w_qkv, w_o, w_sc,
    st_gu, st_d, st_qkv, st_o, scales_ref, acc, hidden, mixed, part, part_twin, chip_part, far_part,
    w_recv, w_send, w_fwd, ag_recv, ag_send, tw_recv, tw_send, rs_recv, rs_send,
):
    f32, bf16 = jnp.float32, jnp.bfloat16
    f, t = lax.axis_index("fs"), lax.axis_index("tp")
    x, y, z = f % 2, (f // 2) % 2, f // 4
    zl, zh = z % 2, z // 2
    me = zl * 2 + x
    own = res_ref.shape[0]
    width = res_ref.shape[1]
    seq = 2 * own
    ff = hidden.shape[1]
    hd = mixed.shape[1]
    piece = gate_ref.shape[0]
    chunk = 2 * piece
    chunks = width // chunk
    f_y = z * 4 + (1 - y) * 2 + x

    def plane_peer(dh, dl, dx):
        hh, ll, xx = (zh + dh) % 2, (zl + dl) % 2, (x + dx) % 2
        return (2 * hh + ll) * 4 + y * 2 + xx, ll * 2 + xx

    def remote(src, dst, send, recv, fs, tp):
        return pltpu.make_async_remote_copy(
            src_ref=src, dst_ref=dst, send_sem=send, recv_sem=recv, device_id=(fs, tp), device_id_type=MESH
        )

    barrier = pltpu.get_barrier_semaphore()
    for dh, dl, dx in PLANE:
        peer, _ = plane_peer(dh, dl, dx)
        pl.semaphore_signal(barrier, inc=1, device_id=(peer, t), device_id_type=MESH)
    pl.semaphore_signal(barrier, inc=1, device_id=(f_y, t), device_id_type=MESH)
    pl.semaphore_signal(barrier, inc=1, device_id=(f, 1 - t), device_id_type=MESH)
    pl.semaphore_wait(barrier, 9)

    def slot(kind, s):
        if kind in (GATE, UP):
            return w_gu.at[pl.ds(pl.multiple_of(s * piece, piece), piece), pl.ds(kind * ff, ff)]
        if kind == DN:
            return w_d.at[:, pl.ds(pl.multiple_of(s * piece, piece), piece)]
        if kind == QKV:
            return w_qkv.at[pl.ds(pl.multiple_of(s * piece, piece), piece), :]
        if kind == OUT:
            return w_o.at[:, pl.ds(pl.multiple_of(s * piece, piece), piece)]
        return w_sc.at[pl.ds(pl.multiple_of(s * 8, 8), 8), :]

    def staged(kind, m):
        if kind == SC:
            return scales_ref
        if kind in (GATE, UP):
            return st_gu.at[m, :, pl.ds(kind * ff, ff)]
        return {DN: st_d, QKV: st_qkv, OUT: st_o}[kind].at[m]

    def send_near(kind):
        own_place = me if kind == DN else x
        remote(staged(kind, me), slot(kind, f), w_fwd.at[kind, own_place], w_recv.at[kind, f], f_y, t).start()
        send_some(kind, 0, 3)
        slot(kind, f)[...] = staged(kind, me)[...]

    def send_far(kind):
        send_some(kind, 3, 7)

    def send_some(kind, begin, end):
        for i in range(begin, end):
            peer, m = plane_peer(*PLANE[i])
            remote(staged(kind, m), slot(kind, f), w_send.at[kind, i], w_recv.at[kind, f], peer, t).start()

    def send_pieces(kind):
        send_near(kind)
        send_far(kind)

    def pair_base(j):
        zz = 2 * ((zh + (j // 2) % 2) % 2) + j % 2
        return zz * 4 + ((y + j // 4) % 2) * 2

    def near_base(j):
        zz = 2 * ((zh + (j // 2) % 2) % 2) + (zl + j) % 2
        return zz * 4 + ((y + j // 4) % 2) * 2

    def take_pair(kind, j):
        base = pair_base(j) if kind == DN else near_base(j)
        for xx in (0, 1):
            s = base + xx

            @pl.when(s != f)
            def _():
                remote(slot(kind, s), slot(kind, s), w_fwd.at[kind, 0], w_recv.at[kind, s], f_y, t).wait_recv()

            @pl.when((s != f) & (j < 4))
            def _():
                remote(
                    slot(kind, s), slot(kind, s), w_fwd.at[kind, (j % 4) * 2 + xx], w_recv.at[kind, s], f_y, t
                ).start()

    def take_some(kind, begin, end):
        def step(j, _):
            take_pair(kind, j)
            return 0

        lax.fori_loop(begin, end, step, 0)

    def finish_sends(kind):
        for i, (dh, dl, dx) in enumerate(PLANE):
            peer, m = plane_peer(dh, dl, dx)
            remote(staged(kind, m), slot(kind, f), w_send.at[kind, i], w_recv.at[kind, f], peer, t).wait_send()
        for i in range(8):
            remote(slot(kind, f), slot(kind, f), w_fwd.at[kind, i], w_recv.at[kind, f], f_y, t).wait_send()

    def block_rows(m, core):
        return pl.ds(pl.multiple_of((m * 2 + core) * own, own), own)

    def column(j):
        return pl.multiple_of(pair_base(j) * piece, chunk)

    def ag_copy(j, i, src, m, core, fs, tp):
        dst = rows_raw.at[block_rows(m, core), pl.ds(column(j), chunk)]
        return remote(dst if src is None else src, dst, ag_send.at[j, i], ag_recv.at[j, m * 2 + core], fs, tp)

    def way(dl, dx):
        first, m_first = plane_peer(0, dl, dx)
        second, m_second = plane_peer(0, 1 - dl, 1 - dx)
        return first, second, m_first, m_second, plane_peer(0, 1, 1)[1]

    z_then_x, x_then_z, by_core = way(1, 0), way(0, 1), way(t, 1 - t)

    def ag_start(j, src, route):
        first, second, _, _, _ = route
        ag_copy(j, 0, src, me, t, first, t).start()
        ag_copy(j, 1, src, me, t, second, t).start()
        ag_copy(j, 2, src, me, t, f, 1 - t).start()

    def ag_relay(j, route):
        _, second, m_first, _, _ = route
        ag_copy(j, 3, None, m_first, t, second, t).wait_recv()
        ag_copy(j, 3, None, m_first, t, second, t).start()
        ag_copy(j, 4, None, m_first, t, f, 1 - t).start()

    def ag_pass(j, route):
        for i, m in enumerate(route[3:]):
            ag_copy(j, 5 + i, None, m, t, f, 1 - t).wait_recv()
            ag_copy(j, 5 + i, None, m, t, f, 1 - t).start()

    def ag_finish():
        def step(j, _):
            for m in range(4):
                ag_copy(j, 0, None, m, 1 - t, f, 1 - t).wait_recv()
            for i in range(7):
                ag_copy(j, i, None, me, t, f, 1 - t).wait_send()
            return 0

        lax.fori_loop(0, chunks, step, 0)

    def norm_rows(gain_ref):
        def step(i, _):
            at = pl.ds(pl.multiple_of(i * 32, 32), 32)
            v = rows_raw[at, :].astype(f32)
            r = lax.rsqrt(jnp.mean(v * v, axis=-1, keepdims=True) + EPSILON)
            rows_normed[at, :] = (v * r * gain_ref[...]).astype(bf16)
            return 0

        lax.fori_loop(0, rows_raw.shape[0] // 32, step, 0)

    def row_tiles(size, body):
        def step(i, _):
            body(pl.ds(pl.multiple_of(i * size, size), size))
            return 0

        lax.fori_loop(0, rows_raw.shape[0] // size, step, 0)

    def silu_mul(gate, up):
        gate = gate * gs_ref[:, pl.ds(pl.multiple_of(me * ff, ff), ff)]
        return (gate / (1.0 + jnp.exp(-gate)) * (up * us_ref[:, pl.ds(pl.multiple_of(me * ff, ff), ff)])).astype(bf16)

    def leave(inputs, weights, scale_row, factor, arriving, last, sums, rows, lags, during=None):
        def product(j):
            if arriving is not None:
                take_pair(arriving, j)
            base = pair_base(j)
            at = pl.ds(column(j), chunk)
            factors = jnp.concatenate(
                [w_sc[pl.ds((base + h) * 8 + scale_row, 1), :] for h in (0, 1)], axis=1
            )

            def step(m, _):
                r = pl.ds(pl.multiple_of(m * seq, seq), seq)
                term = jnp.dot(inputs[r, :], weights[:, at], preferred_element_type=f32) * factors
                term = term.astype(bf16)
                part[0, m, :, at] = term[:own]
                part[1, m, :, at] = term[own:]
                return 0

            lax.fori_loop(0, 4, step, 0)
            to_twin(j).start()

        def to_twin(j):
            at = pl.ds(column(j), chunk)
            return remote(part.at[1 - t, :, :, at], part_twin.at[:, :, at], tw_send.at[j], tw_recv.at[j], f, 1 - t)

        first, second, m_first, m_second, m_third = sums

        def to_first(j):
            at = pl.ds(column(j), chunk)
            pair = pl.ds(0, 2)
            return remote(
                chip_part.at[pair, :, at], far_part.at[pair, :, at], rs_send.at[j, 0], rs_recv.at[j, 0], first, t
            )

        def to_second(j):
            at = pl.ds(column(j), chunk)
            return remote(chip_part.at[2, :, at], far_part.at[2, :, at], rs_send.at[j, 1], rs_recv.at[j, 1], second, t)

        def chip_sum(m, at):
            return part[t, m, :, at].astype(f32) + part_twin[m, :, at].astype(f32)

        def reduce(j):
            at = pl.ds(column(j), chunk)
            to_twin(j).wait_recv()
            chip_part[0, :, at] = chip_sum(m_first, at).astype(bf16)
            chip_part[1, :, at] = chip_sum(m_third, at).astype(bf16)
            to_first(j).start()

        def relay(j):
            at = pl.ds(column(j), chunk)
            to_first(j).wait_recv()
            chip_part[2, :, at] = (chip_sum(m_second, at) + far_part[1, :, at].astype(f32)).astype(bf16)
            to_second(j).start()

        def finish(j):
            at = pl.ds(column(j), chunk)
            to_second(j).wait_recv()
            total = chip_sum(me, at) + far_part[0, :, at].astype(f32) + far_part[2, :, at].astype(f32)
            mine = block_rows(me, t)
            fresh = (rows_raw[mine, at].astype(f32) + factor * total).astype(bf16)
            if last:
                out_ref[:, at] = fresh
            else:
                rows_raw[mine, at] = fresh
                ag_start(j, None, rows)

        stages = [product, reduce, relay, finish]
        if not last:
            stages += [lambda j: ag_relay(j, rows), lambda j: ag_pass(j, rows)]

        def step(i, _):
            for lag, stage in zip(lags, stages):
                pl.when((i >= lag) & (i < chunks + lag))(lambda stage=stage, lag=lag: stage(i - lag))
            if during is not None:
                during(i)
            return 0

        lax.fori_loop(0, chunks + lags[len(stages) - 1], step, 0)

        def drain(j, _):
            to_twin(j).wait_send()
            to_first(j).wait_send()
            to_second(j).wait_send()
            return 0

        lax.fori_loop(0, chunks, drain, 0)
        if not last:
            ag_finish()

    def each_chunk(body):
        def step(j, _):
            body(j)
            return 0

        lax.fori_loop(0, chunks, step, 0)

    scales_ref[...] = jnp.zeros_like(scales_ref)
    scales_ref[0:1, :] = ds_ref[...]
    scales_ref[1:2, :] = os_ref[...]
    send_pieces(SC)

    for m in range(4):
        at = slice(m * ff, (m + 1) * ff)
        st_gu[m, :, :ff] = gate_ref[:, at].astype(bf16)
    send_pieces(GATE)
    each_chunk(lambda j: ag_start(j, res_ref.at[:, pl.ds(column(j), chunk)], z_then_x))
    rows_raw[block_rows(me, t), :] = res_ref[...]

    for m in range(4):
        st_gu[m, :, ff:] = up_ref[:, m * ff : (m + 1) * ff].astype(bf16)
    send_pieces(UP)
    for m in range(4):
        at = slice(m * hd, (m + 1) * hd)
        st_d[m] = down_ref[m * ff : (m + 1) * ff, :].astype(bf16)
        st_qkv[m, :, :hd] = q_ref[:, at].astype(bf16)
        st_qkv[m, :, hd : 2 * hd] = k_ref[:, at].astype(bf16)
        st_qkv[m, :, 2 * hd :] = v_ref[:, at].astype(bf16)
        st_o[m] = o_ref[at, :].astype(bf16)

    ahead = zl != zh
    take_some(SC, 0, 4)
    take_some(GATE, 0, 4)
    each_chunk(lambda j: ag_relay(j, z_then_x))
    pl.when(ahead)(lambda: send_pieces(DN))
    pl.when(jnp.logical_not(ahead))(lambda: send_near(DN))
    send_near(QKV)
    send_near(OUT)
    take_some(UP, 0, 2)
    each_chunk(lambda j: ag_pass(j, z_then_x))
    ag_finish()
    norm_rows(g1_ref)
    take_some(UP, 2, 3)
    take_some(GATE, 4, 8)

    def first_gate(r):
        acc[r, :ff] = jnp.dot(rows_normed[r, :], w_gu[:, :ff], preferred_element_type=f32)

    row_tiles(seq, first_gate)
    take_some(UP, 3, 4)
    pl.when(ahead)(lambda: send_far(QKV))
    pl.when(jnp.logical_not(ahead))(lambda: send_far(DN))
    take_some(UP, 4, 8)
    take_some(SC, 4, 8)

    def first_hidden(r):
        up = jnp.dot(rows_normed[r, :], w_gu[:, ff:], preferred_element_type=f32)
        hidden[r, :] = silu_mul(acc[r, :ff], up)

    row_tiles(seq, first_hidden)

    def take_early(i):
        pl.when((i == 3) & ahead)(lambda: send_far(OUT))
        pl.when((i == 3) & jnp.logical_not(ahead))(lambda: send_far(QKV))
        pl.when((i == 8) & jnp.logical_not(ahead))(lambda: send_far(OUT))
        pl.when((i >= 7) & (i < 15) & (i % 2 == 1))(lambda: take_pair(QKV, (i - 7) // 2))
        pl.when(i >= 14)(lambda: take_pair(OUT, i - 14))

    leave(hidden, w_d, 0, 0.5, DN, False, x_then_z, by_core, (0, 1, 4, 6, 8, 10), take_early)

    norm_rows(g2_ref)
    take_some(QKV, 4, 8)

    def project(r):
        acc[r, : 3 * hd] = jnp.dot(rows_normed[r, :], w_qkv[...], preferred_element_type=f32)

    row_tiles(seq, project)
    take_some(OUT, 4, 8)
    head = (t * 4 + me).astype(f32)
    ri = lax.broadcasted_iota(jnp.int32, (seq, seq), 0)
    ci = lax.broadcasted_iota(jnp.int32, (seq, seq), 1)
    rate = jnp.exp(math.log(1.0 / 16.0) + jnp.full((seq, seq), head, f32) / (HEADS - 1) * math.log(4.0 / seq))
    distance = jnp.maximum(ri - ci, 0).astype(f32)
    decay = jnp.where(ri >= ci, jnp.exp(-rate * distance), 0.0) * hd ** (-0.5)

    at_head = pl.ds(pl.multiple_of(me * hd, hd), hd)

    def turn(values):
        a, b = values[:, : hd // 2], values[:, hd // 2 :]
        c, s = cos_ref[...], sin_ref[...]
        return jnp.concatenate([a * c - b * s, b * c + a * s], axis=1).astype(bf16)

    def sequence(r):
        q = turn(acc[r, :hd] * qs_ref[:, at_head])
        k = turn(acc[r, hd : 2 * hd] * ks_ref[:, at_head])
        v = (acc[r, 2 * hd : 3 * hd] * vs_ref[:, at_head]).astype(bf16)
        scores = lax.dot_general(q, k, (((1,), (1,)), ((), ())), preferred_element_type=f32)
        both = jnp.dot((scores * decay).astype(bf16), v, preferred_element_type=f32)
        level = jnp.maximum(jnp.mean(both * both, axis=-1, keepdims=True), HEAD_FLOOR)
        mixed[r, :] = (both * lax.rsqrt(level)).astype(bf16)

    row_tiles(seq, sequence)
    leave(mixed, w_o, 1, 1.0, None, False, by_core, by_core, (0, 1, 3, 5, 7, 9))

    norm_rows(g3_ref)

    def second_hidden(r):
        gate = jnp.dot(rows_normed[r, :], w_gu[:, :ff], preferred_element_type=f32)
        up = jnp.dot(rows_normed[r, :], w_gu[:, ff:], preferred_element_type=f32)
        hidden[r, :] = silu_mul(gate, up)

    row_tiles(seq, second_hidden)
    leave(hidden, w_d, 0, 0.5, None, True, by_core, by_core, (0, 1, 3, 5))
    for kind in (SC, GATE, UP, DN, QKV, OUT):
        finish_sends(kind)


def fused_body(
    residual_in, gain_first, gain_mixer, gain_second,
    gate_weight, gate_scale, up_weight, up_scale, down_weight, down_scale,
    query_weight, query_scale, key_weight, key_scale, value_weight, value_scale,
    output_weight, output_scale,
):
    f32, bf16 = jnp.float32, jnp.bfloat16
    own, width = residual_in.shape
    rows, piece = 8 * own, gate_weight.shape[0]
    ff, hd = gate_weight.shape[1] // 4, query_weight.shape[1] // 4
    chunks = width // (2 * piece)

    def row(vector):
        return vector.reshape(1, -1)

    half = hd // 2
    frequency = np.float32(ROTARY_BASE) ** (-np.arange(half, dtype=np.float32) * np.float32(2.0) / np.float32(hd))
    angles = np.arange(2 * own, dtype=np.float32)[:, None] * frequency.astype(np.float32)[None]
    cosine, sine_value = np.cos(angles).astype(np.float32), np.sin(angles).astype(np.float32)
    operands = (
        residual_in, row(gain_first), row(gain_mixer), row(gain_second),
        gate_weight, up_weight, down_weight, query_weight, key_weight, value_weight, output_weight,
        row(gate_scale), row(up_scale), row(query_scale), row(key_scale), row(value_scale),
        row(down_scale), row(output_scale), jnp.asarray(cosine), jnp.asarray(sine_value),
    )
    dma = pltpu.SemaphoreType.DMA
    return pl.pallas_call(
        fused_kernel,
        out_shape=jax.ShapeDtypeStruct((own, width), bf16),
        in_specs=[pl.BlockSpec(memory_space=pltpu.VMEM)] * len(operands),
        out_specs=pl.BlockSpec(memory_space=pltpu.VMEM),
        scratch_shapes=[
            pltpu.VMEM((rows, width), bf16),
            pltpu.VMEM((rows, width), bf16),
            pltpu.VMEM((width, 2 * ff), bf16),
            pltpu.VMEM((ff, width), bf16),
            pltpu.VMEM((width, 3 * hd), bf16),
            pltpu.VMEM((hd, width), bf16),
            pltpu.VMEM((8 * (width // piece), piece), f32),
            pltpu.VMEM((4, piece, 2 * ff), bf16),
            pltpu.VMEM((4, ff, piece), bf16),
            pltpu.VMEM((4, piece, 3 * hd), bf16),
            pltpu.VMEM((4, hd, piece), bf16),
            pltpu.VMEM((8, piece), f32),
            pltpu.VMEM((rows, max(ff, 3 * hd)), f32),
            pltpu.VMEM((rows, ff), bf16),
            pltpu.VMEM((rows, hd), bf16),
            pltpu.VMEM((2, 4, own, width), bf16),
            pltpu.VMEM((4, own, width), bf16),
            pltpu.VMEM((3, own, width), bf16),
            pltpu.VMEM((3, own, width), bf16),
            dma((6, 16)), dma((6, 7)), dma((6, 8)),
            dma((chunks, 8)), dma((chunks, 7)),
            dma((chunks,)), dma((chunks,)), dma((chunks, 2)), dma((chunks, 2)),
        ],
        compiler_params=pltpu.CompilerParams(
            collective_id=0, has_side_effects=True, vmem_limit_bytes=63 * 2**20
        ),
    )(*operands)


def solution(mesh):
    n_fs, n_tp = mesh.shape["fs"], mesh.shape["tp"]
    share = math.gcd(math.gcd(HEADS // n_tp, n_fs), 4)
    if (n_fs, n_tp, share) == (16, 2, 4):
        body = fused_body
    else:
        body = make_body(n_fs, n_tp, share)
    in_specs = (
        P(("fs", "tp"), None),
        P(),
        P(),
        P(),
        P("fs", "tp"),
        P("tp"),
        P("fs", "tp"),
        P("tp"),
        P("tp", "fs"),
        P("fs"),
        P("fs", "tp"),
        P("tp"),
        P("fs", "tp"),
        P("tp"),
        P("fs", "tp"),
        P("tp"),
        P("tp", "fs"),
        P("fs"),
    )
    out_specs = P(("fs", "tp"), None)
    return jax.shard_map(body, mesh=mesh, in_specs=in_specs, out_specs=out_specs, check_vma=False)
```

```python
import functools
import math

import jax
import jax.numpy as jnp
import numpy as np
from jax import lax
from jax.experimental import pallas as pl
from jax.experimental.pallas import tpu as pltpu
from jax.sharding import PartitionSpec as P

HEADS = 8
HEAD_DIM = 256
BLOCK = 64


EPSILON = 1e-06
HEAD_FLOOR = 0.25
ROTARY_BASE = 10000.0
HIGHEST = lax.Precision.HIGHEST


def normalize(sequence_rows, gain_vector):
    values = sequence_rows.astype(jnp.float32)
    scaled = values * lax.rsqrt(jnp.mean(values * values, axis=-1, keepdims=True) + EPSILON)
    return (scaled * gain_vector).astype(jnp.bfloat16)


def head_rates(first_head, head_count, length):
    head_number = (first_head + jnp.arange(head_count)).astype(jnp.float32)
    return jnp.exp(jnp.log(1.0 / 16.0) + head_number / (HEADS - 1) * jnp.log(4.0 / length))


def rotate(values, positions):
    half_width = values.shape[-1] // 2
    frequency = ROTARY_BASE ** (-jnp.arange(half_width, dtype=jnp.float32) * 2.0 / values.shape[-1])
    angles = positions[:, None] * frequency[None, :]
    cosine = jnp.cos(angles)[:, None, :]
    sine_value = jnp.sin(angles)[:, None, :]
    front_half = values[..., :half_width]
    back_half = values[..., half_width:]
    return jnp.concatenate(
        [
            front_half * cosine - back_half * sine_value,
            back_half * cosine + front_half * sine_value,
        ],
        axis=-1,
    )


def retention(query_pre, key_pre, value_pre, decay_rates):
    length, head_count, head_width = query_pre.shape
    positions = jnp.arange(length, dtype=jnp.float32)
    query_rot = rotate(query_pre, positions).astype(jnp.bfloat16)
    key_rot = rotate(key_pre, positions).astype(jnp.bfloat16)
    value_low = value_pre.astype(jnp.bfloat16)
    blocks = length // BLOCK
    inside = jnp.arange(BLOCK, dtype=jnp.float32)
    distance = inside[:, None] - inside[None, :]
    within = jnp.where(
        distance >= 0, jnp.exp(-decay_rates[:, None, None] * jnp.maximum(distance, 0.0)), 0.0
    ) * head_width ** (-0.5)
    query_blocks = query_rot.reshape(blocks, BLOCK, head_count, head_width)
    key_blocks = key_rot.reshape(blocks, BLOCK, head_count, head_width)
    value_blocks = value_low.reshape(blocks, BLOCK, head_count, head_width)
    scores = jnp.einsum(
        "nihe,njhe->nhij", query_blocks, key_blocks, preferred_element_type=jnp.float32
    )
    weights = (scores * within[None]).astype(jnp.bfloat16)
    inner_part = jnp.einsum(
        "nhij,njhe->nihe", weights, value_blocks, preferred_element_type=jnp.float32
    )
    fading = jnp.exp(-decay_rates[None, :] * (BLOCK - 1.0 - inside[:, None])) * head_width ** (-0.5)
    key_faded = key_blocks.astype(jnp.float32) * fading[None, :, :, None]
    updates = jnp.einsum(
        "njhd,njhe->nhde", key_faded, value_blocks.astype(jnp.float32), precision=HIGHEST
    )
    block_decay = jnp.exp(-decay_rates * BLOCK)

    def advance(memory_state, update):
        return (memory_state * block_decay[:, None, None] + update, memory_state)

    _, before = lax.scan(
        advance, jnp.zeros((head_count, head_width, head_width), jnp.float32), updates
    )
    rising = jnp.exp(-decay_rates[None, :] * (inside[:, None] + 1.0))
    queried = query_blocks.astype(jnp.float32) * rising[None, :, :, None]
    carried_part = jnp.einsum("nihd,nhde->nihe", queried, before, precision=HIGHEST)
    combined = (inner_part + carried_part).reshape(length, head_count, head_width)
    normed = combined * lax.rsqrt(
        jnp.maximum(jnp.mean(combined * combined, axis=-1, keepdims=True), HEAD_FLOOR)
    )
    return normed.astype(jnp.bfloat16).reshape(length, head_count * head_width)


def split_three(values):
    high = values.astype(jnp.bfloat16)
    rest = values - high.astype(jnp.float32)
    middle_part = rest.astype(jnp.bfloat16)
    low = (rest - middle_part.astype(jnp.float32)).astype(jnp.bfloat16)
    return [high, middle_part, low]


def make_body(n_fs, n_tp, share):
    spread = n_fs // share
    STRIDED = False
    if STRIDED:
        teams = [[m * spread + r for m in range(share)] for r in range(spread)]
    else:
        teams = [[r * share + m for m in range(share)] for r in range(spread)]
    twins = [[team[m] for team in teams] for m in range(share)]
    row_teams = [[f * n_tp + t for f in team for t in range(n_tp)] for team in teams]

    def my_rank():
        position = lax.axis_index("fs")
        return position // spread if STRIDED else position % share

    def fetch(pieces):
        swapped = lax.all_to_all(
            pieces, "fs", split_axis=0, concat_axis=0, axis_index_groups=teams, tiled=True
        )
        return lax.all_gather(swapped, "fs", axis=0, axis_index_groups=twins, tiled=False)

    def order_features(rows):
        if not STRIDED:
            return rows
        count = rows.shape[0]
        return rows.reshape(count, share, spread, -1).swapaxes(1, 2).reshape(count, -1)

    def collect_rows(rows, gain_vector):
        return lax.all_gather(
            order_features(normalize(rows, gain_vector)),
            ("fs", "tp"),
            axis=0,
            axis_index_groups=row_teams,
            tiled=True,
        )

    def return_rows(inputs, weight, factor):
        term = jnp.dot(inputs, weight, preferred_element_type=jnp.float32) * factor
        return lax.psum_scatter(
            term.astype(jnp.bfloat16),
            ("fs", "tp"),
            scatter_dimension=0,
            axis_index_groups=row_teams,
            tiled=True,
        ).astype(jnp.float32)

    def columns_of(weight):
        low = weight.astype(jnp.bfloat16)
        return low.reshape(low.shape[0], share, -1).swapaxes(0, 1)

    def rows_of(weight):
        low = weight.astype(jnp.bfloat16)
        return low.reshape(share, -1, low.shape[1])

    def own(vector, rank):
        width = vector.shape[0] // share
        return lax.dynamic_slice_in_dim(vector, rank * width, width)

    def body(
        residual_in,
        gain_first,
        gain_mixer,
        gain_second,
        gate_weight,
        gate_scale,
        up_weight,
        up_scale,
        down_weight,
        down_scale,
        query_weight,
        query_scale,
        key_weight,
        key_scale,
        value_weight,
        value_scale,
        output_weight,
        output_scale,
    ):
        rank = my_rank()
        hidden_width = gate_weight.shape[1] // share
        mix_width = query_weight.shape[1] // share
        entry = fetch(jnp.concatenate([columns_of(gate_weight), columns_of(up_weight)], axis=2))
        factors = split_three(down_scale) + split_three(output_scale)
        factors = jnp.stack(factors + [jnp.zeros_like(factors[0])] * 10)
        leave_piece = jnp.concatenate(
            [
                rows_of(down_weight),
                rows_of(output_weight),
                jnp.broadcast_to(factors[None], (share,) + factors.shape),
            ],
            axis=1,
        )
        first_input = collect_rows(residual_in, gain_first)
        leave_piece, entry = lax.optimization_barrier((leave_piece, entry)) if False else (leave_piece, entry)
        leave = fetch(leave_piece)
        project_piece = jnp.concatenate(
            [columns_of(query_weight), columns_of(key_weight), columns_of(value_weight)], axis=2
        )
        project_piece, leave = lax.optimization_barrier((project_piece, leave)) if False else (project_piece, leave)
        project = fetch(project_piece)

        entry = entry.reshape(-1, 2 * hidden_width)
        project = project.reshape(-1, 3 * mix_width)
        if STRIDED:
            leave = leave.swapaxes(0, 1)
        leave = leave.transpose(2, 0, 1, 3).reshape(leave.shape[2], -1)
        down_full = leave[:hidden_width]
        output_full = leave[hidden_width : hidden_width + mix_width]
        parts = leave[hidden_width + mix_width :].astype(jnp.float32)
        down_factor = parts[0] + parts[1] + parts[2]
        output_factor = parts[3] + parts[4] + parts[5]
        gate_own, up_own = own(gate_scale, rank), own(up_scale, rank)

        def half_step(inputs):
            both = jnp.dot(inputs, entry, preferred_element_type=jnp.float32)
            gate_pre = both[:, :hidden_width] * gate_own
            up_pre = both[:, hidden_width:] * up_own
            hidden = (jax.nn.silu(gate_pre) * up_pre).astype(jnp.bfloat16)
            return return_rows(hidden, down_full, down_factor)

        mlp_first = half_step(first_input)
        middle = (residual_in.astype(jnp.float32) + 0.5 * mlp_first).astype(jnp.bfloat16)
        mixer_input = collect_rows(middle, gain_mixer)
        both = jnp.dot(mixer_input, project, preferred_element_type=jnp.float32)
        scale = jnp.concatenate([own(v, rank) for v in (query_scale, key_scale, value_scale)])
        length = residual_in.shape[0] * n_tp
        heads_own = mix_width // HEAD_DIM
        both = (both * scale).reshape(share, length, 3, heads_own, HEAD_DIM)
        first_head = (lax.axis_index("tp") * share + rank) * heads_own
        decay_rates = head_rates(first_head, heads_own, length)
        mixed = jax.vmap(lambda t: retention(t[:, 0], t[:, 1], t[:, 2], decay_rates))(both)
        mixer_out = return_rows(mixed.reshape(share * length, mix_width), output_full, output_factor)
        second = (middle.astype(jnp.float32) + mixer_out).astype(jnp.bfloat16)
        mlp_second = half_step(collect_rows(second, gain_second))
        return (second.astype(jnp.float32) + 0.5 * mlp_second).astype(jnp.bfloat16)

    return body


MESH = pl.DeviceIdType.MESH
GATE, UP, DN, QKV, OUT, SC = range(6)
PLANE = ((0, 0, 1), (0, 1, 0), (0, 1, 1), (1, 0, 0), (1, 1, 0), (1, 0, 1), (1, 1, 1))


EARLY = (
    (4, QKV, 0), (5, QKV, 1), (9, QKV, 2), (11, QKV, 3), (12, OUT, 0), (12, OUT, 1), (13, OUT, 2), (13, OUT, 3),
    (15, QKV, 4), (15, QKV, 5), (17, QKV, 6), (17, QKV, 7)
)


def fused_kernel(
    res_ref, g1_ref, g2_ref, g3_ref,
    gate_hbm, up_hbm, down_hbm, q_hbm, k_hbm, v_hbm, o_hbm,
    gs_ref, us_ref, qs_ref, ks_ref, vs_ref, ds_ref, os_ref, cos_ref, sin_ref,
    out_ref,
    rows_raw, rows_normed, w_gu, w_d, w_qkv, w_o, w_sc,
    st_gu, st_d, st_qkv, st_o, scales_ref, acc, power, hidden, mixed, part, part_twin, chip_part, far_part,
    gate_ref, up_ref, down_ref, q_ref, k_ref, v_ref, o_ref, in_sems,
    w_recv, w_send, w_fwd, ag_recv, ag_send, tw_recv, tw_send, rs_recv, rs_send,
):
    f32, bf16 = jnp.float32, jnp.bfloat16
    f, t = lax.axis_index("fs"), lax.axis_index("tp")
    x, y, z = f % 2, (f // 2) % 2, f // 4
    zl, zh = z % 2, z // 2
    me = zl * 2 + x
    own = res_ref.shape[0]
    width = res_ref.shape[1]
    seq = 2 * own
    ff = hidden.shape[1]
    hd = mixed.shape[1]
    piece = gate_ref.shape[0]
    chunk = 2 * piece
    chunks = width // chunk
    f_y = z * 4 + (1 - y) * 2 + x

    def plane_peer(dh, dl, dx):
        hh, ll, xx = (zh + dh) % 2, (zl + dl) % 2, (x + dx) % 2
        return (2 * hh + ll) * 4 + y * 2 + xx, ll * 2 + xx

    def remote(src, dst, send, recv, fs, tp):
        return pltpu.make_async_remote_copy(
            src_ref=src, dst_ref=dst, send_sem=send, recv_sem=recv, device_id=(fs, tp), device_id_type=MESH
        )

    sources = (gate_hbm, up_hbm, down_hbm, q_hbm, k_hbm, v_hbm, o_hbm)
    landed = (gate_ref, up_ref, down_ref, q_ref, k_ref, v_ref, o_ref)
    loads = [pltpu.make_async_copy(a, b, in_sems.at[i]) for i, (a, b) in enumerate(zip(sources, landed))]
    for load in loads:
        load.start()

    barrier = pltpu.get_barrier_semaphore()
    for dh, dl, dx in PLANE:
        peer, _ = plane_peer(dh, dl, dx)
        pl.semaphore_signal(barrier, inc=1, device_id=(peer, t), device_id_type=MESH)
    pl.semaphore_signal(barrier, inc=1, device_id=(f_y, t), device_id_type=MESH)
    pl.semaphore_signal(barrier, inc=1, device_id=(f, 1 - t), device_id_type=MESH)
    pl.semaphore_wait(barrier, 9)

    def slot(kind, s):
        if kind in (GATE, UP):
            return w_gu.at[pl.ds(pl.multiple_of(s * piece, piece), piece), pl.ds(kind * ff, ff)]
        if kind == DN:
            return w_d.at[:, pl.ds(pl.multiple_of(s * piece, piece), piece)]
        if kind == QKV:
            return w_qkv.at[pl.ds(pl.multiple_of(s * piece, piece), piece), :]
        if kind == OUT:
            return w_o.at[:, pl.ds(pl.multiple_of(s * piece, piece), piece)]
        return w_sc.at[pl.ds(pl.multiple_of(s * 8, 8), 8), :]

    def staged(kind, m):
        if kind == SC:
            return scales_ref
        if kind in (GATE, UP):
            return st_gu.at[m, :, pl.ds(kind * ff, ff)]
        return {DN: st_d, QKV: st_qkv, OUT: st_o}[kind].at[m]

    def send_across(kind):
        own_place = me if kind == DN else x
        remote(staged(kind, me), slot(kind, f), w_fwd.at[kind, own_place], w_recv.at[kind, f], f_y, t).start()

    def send_near(kind):
        send_some(kind, 0, 3)
        slot(kind, f)[...] = staged(kind, me)[...]

    def send_far(kind):
        send_some(kind, 3, 7)

    def send_some(kind, begin, end):
        for i in range(begin, end):
            peer, m = plane_peer(*PLANE[i])
            remote(staged(kind, m), slot(kind, f), w_send.at[kind, i], w_recv.at[kind, f], peer, t).start()

    def send_pieces(kind):
        send_across(kind)
        send_near(kind)
        send_far(kind)

    def pair_base(j):
        zz = 2 * ((zh + (j // 2) % 2) % 2) + j % 2
        return zz * 4 + ((y + j // 4) % 2) * 2

    def near_base(j):
        zz = 2 * ((zh + (j // 2) % 2) % 2) + (zl + j) % 2
        return zz * 4 + ((y + j // 4) % 2) * 2

    def take_pair(kind, j):
        base = pair_base(j) if kind == DN else near_base(j)
        for xx in (0, 1):
            s = base + xx

            @pl.when(s != f)
            def _():
                remote(slot(kind, s), slot(kind, s), w_fwd.at[kind, 0], w_recv.at[kind, s], f_y, t).wait_recv()

            @pl.when((s != f) & (j < 4))
            def _():
                remote(
                    slot(kind, s), slot(kind, s), w_fwd.at[kind, (j % 4) * 2 + xx], w_recv.at[kind, s], f_y, t
                ).start()

    def take_some(kind, begin, end):
        def step(j, _):
            take_pair(kind, j)
            return 0

        lax.fori_loop(begin, end, step, 0)

    def finish_sends(kind):
        for i, (dh, dl, dx) in enumerate(PLANE):
            peer, m = plane_peer(dh, dl, dx)
            remote(staged(kind, m), slot(kind, f), w_send.at[kind, i], w_recv.at[kind, f], peer, t).wait_send()
        for i in range(8):
            remote(slot(kind, f), slot(kind, f), w_fwd.at[kind, i], w_recv.at[kind, f], f_y, t).wait_send()

    def block_rows(m, core):
        return pl.ds(pl.multiple_of((m * 2 + core) * own, own), own)

    def column(j):
        return pl.multiple_of(pair_base(j) * piece, chunk)

    def ag_copy(j, i, src, m, core, fs, tp):
        dst = rows_raw.at[block_rows(m, core), pl.ds(column(j), chunk)]
        return remote(dst if src is None else src, dst, ag_send.at[j, i], ag_recv.at[j, m * 2 + core], fs, tp)

    def way(dl, dx):
        first, m_first = plane_peer(0, dl, dx)
        second, m_second = plane_peer(0, 1 - dl, 1 - dx)
        return first, second, m_first, m_second, plane_peer(0, 1, 1)[1]

    z_then_x, x_then_z, by_core = way(1, 0), way(0, 1), way(t, 1 - t)

    def ag_start(j, src, route):
        first, second, _, _, _ = route
        ag_copy(j, 0, src, me, t, first, t).start()
        ag_copy(j, 1, src, me, t, second, t).start()
        ag_copy(j, 2, src, me, t, f, 1 - t).start()

    def ag_relay(j, route):
        _, second, m_first, _, _ = route
        ag_copy(j, 3, None, m_first, t, second, t).wait_recv()
        ag_copy(j, 3, None, m_first, t, second, t).start()
        ag_copy(j, 4, None, m_first, t, f, 1 - t).start()

    def ag_pass(j, route):
        for i, m in enumerate(route[3:]):
            ag_copy(j, 5 + i, None, m, t, f, 1 - t).wait_recv()
            ag_copy(j, 5 + i, None, m, t, f, 1 - t).start()

    def ag_arrive(j):
        for m in range(4):
            ag_copy(j, 0, None, m, 1 - t, f, 1 - t).wait_recv()

    def ag_settle(j):
        for i in range(7):
            ag_copy(j, i, None, me, t, f, 1 - t).wait_send()

    def each_chunk(body):
        def step(j, _):
            body(j)
            return 0

        lax.fori_loop(0, chunks, step, 0)

    def norm_rows(gain_ref):
        def step(i, _):
            at = pl.ds(pl.multiple_of(i * 32, 32), 32)
            v = rows_raw[at, :].astype(f32)
            r = lax.rsqrt(jnp.mean(v * v, axis=-1, keepdims=True) + EPSILON)
            rows_normed[at, :] = (v * r * gain_ref[...]).astype(bf16)
            return 0

        lax.fori_loop(0, rows_raw.shape[0] // 32, step, 0)

    def row_tiles(size, body):
        def step(i, _):
            body(pl.ds(pl.multiple_of(i * size, size), size))
            return 0

        lax.fori_loop(0, rows_raw.shape[0] // size, step, 0)

    def absorber(gain_ref, weights):
        columns = weights.shape[1]

        def stage(j):
            at = pl.ds(column(j), chunk)

            @pl.when(j == 0)
            def _():
                def clear(r):
                    acc[r, :columns] = jnp.zeros((seq, columns), f32)
                    power[r, :] = jnp.zeros((seq, piece), f32)

                row_tiles(seq, clear)

            ag_arrive(j)

            def tile(r):
                v = rows_raw[r, at].astype(f32)
                square = v * v
                power[r, :] += square[:, :piece] + square[:, piece:]
                v = (v * gain_ref[:, at]).astype(bf16)
                acc[r, :columns] += jnp.dot(v, weights[at, :], preferred_element_type=f32)

            row_tiles(seq, tile)

        return stage

    def row_factor(r):
        return lax.rsqrt(jnp.sum(power[r, :], axis=-1, keepdims=True) / width + EPSILON)

    def silu_mul(gate, up):
        gate = gate * gs_ref[:, pl.ds(pl.multiple_of(me * ff, ff), ff)]
        return (gate / (1.0 + jnp.exp(-gate)) * (up * us_ref[:, pl.ds(pl.multiple_of(me * ff, ff), ff)])).astype(bf16)

    def leave(inputs, weights, scale_row, factor, arriving, last, sums, rows, lags, absorb=None, during=None):
        def product(j):
            if arriving is not None:
                take_pair(arriving, j)
            base = pair_base(j)
            at = pl.ds(column(j), chunk)
            factors = jnp.concatenate(
                [w_sc[pl.ds((base + h) * 8 + scale_row, 1), :] for h in (0, 1)], axis=1
            )

            def step(i, _):
                r = pl.ds(pl.multiple_of(i * 2 * seq, 2 * seq), 2 * seq)
                term = jnp.dot(inputs[r, :], weights[:, at], preferred_element_type=f32) * factors
                term = term.astype(bf16)
                for m in range(2):
                    for core in range(2):
                        part[core, i * 2 + m, :, at] = term[(m * 2 + core) * own : (m * 2 + core + 1) * own]
                return 0

            lax.fori_loop(0, 2, step, 0)
            to_twin(j).start()

        def to_twin(j):
            at = pl.ds(column(j), chunk)
            return remote(part.at[1 - t, :, :, at], part_twin.at[:, :, at], tw_send.at[j], tw_recv.at[j], f, 1 - t)

        first, second, m_first, m_second, m_third = sums

        def to_first(j):
            at = pl.ds(column(j), chunk)
            pair = pl.ds(0, 2)
            return remote(
                chip_part.at[pair, :, at], far_part.at[pair, :, at], rs_send.at[j, 0], rs_recv.at[j, 0], first, t
            )

        def to_second(j):
            at = pl.ds(column(j), chunk)
            return remote(chip_part.at[2, :, at], far_part.at[2, :, at], rs_send.at[j, 1], rs_recv.at[j, 1], second, t)

        def chip_sum(m, at):
            return part[t, m, :, at].astype(f32) + part_twin[m, :, at].astype(f32)

        def reduce(j):
            at = pl.ds(column(j), chunk)
            to_twin(j).wait_recv()
            chip_part[0, :, at] = chip_sum(m_first, at).astype(bf16)
            chip_part[1, :, at] = chip_sum(m_third, at).astype(bf16)
            to_first(j).start()

        def relay(j):
            at = pl.ds(column(j), chunk)
            to_first(j).wait_recv()
            chip_part[2, :, at] = (chip_sum(m_second, at) + far_part[1, :, at].astype(f32)).astype(bf16)
            to_second(j).start()

        def finish(j):
            at = pl.ds(column(j), chunk)
            to_second(j).wait_recv()
            total = chip_sum(me, at) + far_part[0, :, at].astype(f32) + far_part[2, :, at].astype(f32)
            mine = block_rows(me, t)
            fresh = (rows_raw[mine, at].astype(f32) + factor * total).astype(bf16)
            if last:
                out_ref[:, at] = fresh
            else:
                rows_raw[mine, at] = fresh
                ag_start(j, None, rows)

        stages = [product, reduce, relay, finish]
        if not last:
            stages += [lambda j: ag_relay(j, rows), lambda j: ag_pass(j, rows), absorb]

        def step(i, _):
            for lag, stage in zip(lags, stages):
                pl.when((i >= lag) & (i < chunks + lag))(lambda stage=stage, lag=lag: stage(i - lag))
            if during is not None:
                during(i)
            return 0

        lax.fori_loop(0, chunks + lags[len(stages) - 1], step, 0)

        def drain(j, _):
            to_twin(j).wait_send()
            to_first(j).wait_send()
            to_second(j).wait_send()
            return 0

        lax.fori_loop(0, chunks, drain, 0)
        if not last:
            each_chunk(ag_settle)

    scales_ref[...] = jnp.zeros_like(scales_ref)
    scales_ref[0:1, :] = ds_ref[...]
    scales_ref[1:2, :] = os_ref[...]
    send_pieces(SC)

    loads[0].wait()
    for m in range(4):
        at = slice(m * ff, (m + 1) * ff)
        st_gu[m, :, :ff] = gate_ref[:, at].astype(bf16)
    send_pieces(GATE)
    each_chunk(lambda j: ag_start(j, res_ref.at[:, pl.ds(column(j), chunk)], z_then_x))
    rows_raw[block_rows(me, t), :] = res_ref[...]

    loads[1].wait()
    for m in range(4):
        st_gu[m, :, ff:] = up_ref[:, m * ff : (m + 1) * ff].astype(bf16)
    send_pieces(UP)
    for load in loads[2:]:
        load.wait()
    for m in range(4):
        at = slice(m * hd, (m + 1) * hd)
        st_d[m] = down_ref[m * ff : (m + 1) * ff, :].astype(bf16)
        st_qkv[m, :, :hd] = q_ref[:, at].astype(bf16)
        st_qkv[m, :, hd : 2 * hd] = k_ref[:, at].astype(bf16)
        st_qkv[m, :, 2 * hd :] = v_ref[:, at].astype(bf16)
        st_o[m] = o_ref[at, :].astype(bf16)

    for kind in (DN, QKV, OUT):
        send_across(kind)

    ahead = zl != zh
    take_some(SC, 0, 4)
    take_some(GATE, 0, 4)
    each_chunk(lambda j: ag_relay(j, z_then_x))
    send_near(DN)
    pl.when(ahead)(lambda: send_far(DN))
    send_near(QKV)
    send_near(OUT)
    take_some(UP, 0, 2)
    each_chunk(lambda j: ag_pass(j, z_then_x))
    each_chunk(ag_arrive)
    each_chunk(ag_settle)
    norm_rows(g1_ref)
    take_some(UP, 2, 3)
    take_some(GATE, 4, 8)

    def first_gate(r):
        acc[r, :ff] = jnp.dot(rows_normed[r, :], w_gu[:, :ff], preferred_element_type=f32)

    row_tiles(seq, first_gate)
    take_some(UP, 3, 4)
    pl.when(ahead)(lambda: send_far(QKV))
    pl.when(jnp.logical_not(ahead))(lambda: send_far(DN))
    take_some(UP, 4, 8)
    take_some(SC, 4, 8)

    def first_hidden(r):
        up = jnp.dot(rows_normed[r, :], w_gu[:, ff:], preferred_element_type=f32)
        hidden[r, :] = silu_mul(acc[r, :ff], up)

    row_tiles(seq, first_hidden)

    def take_early(i):
        pl.when((i == 3) & ahead)(lambda: send_far(OUT))
        pl.when((i == 3) & jnp.logical_not(ahead))(lambda: send_far(QKV))
        pl.when((i == 8) & jnp.logical_not(ahead))(lambda: send_far(OUT))
        for at, kind, j in EARLY:
            pl.when(i == at)(lambda kind=kind, j=j: take_pair(kind, j))

    leave(hidden, w_d, 0, 0.5, DN, False, x_then_z, by_core, (0, 1, 4, 7, 9, 11, 12), absorber(g2_ref, w_qkv), take_early)

    take_some(OUT, 4, 8)
    head = (t * 4 + me).astype(f32)
    ri = lax.broadcasted_iota(jnp.int32, (seq, seq), 0)
    ci = lax.broadcasted_iota(jnp.int32, (seq, seq), 1)
    rate = jnp.exp(math.log(1.0 / 16.0) + jnp.full((seq, seq), head, f32) / (HEADS - 1) * math.log(4.0 / seq))
    distance = jnp.maximum(ri - ci, 0).astype(f32)
    decay = jnp.where(ri >= ci, jnp.exp(-rate * distance), 0.0) * hd ** (-0.5)

    at_head = pl.ds(pl.multiple_of(me * hd, hd), hd)

    def turn(values):
        a, b = values[:, : hd // 2], values[:, hd // 2 :]
        c, s = cos_ref[...], sin_ref[...]
        return jnp.concatenate([a * c - b * s, b * c + a * s], axis=1).astype(bf16)

    def sequence(r):
        factor = row_factor(r)
        q = turn(acc[r, :hd] * factor * qs_ref[:, at_head])
        k = turn(acc[r, hd : 2 * hd] * factor * ks_ref[:, at_head])
        v = (acc[r, 2 * hd : 3 * hd] * factor * vs_ref[:, at_head]).astype(bf16)
        scores = lax.dot_general(q, k, (((1,), (1,)), ((), ())), preferred_element_type=f32)
        both = jnp.dot((scores * decay).astype(bf16), v, preferred_element_type=f32)
        level = jnp.maximum(jnp.mean(both * both, axis=-1, keepdims=True), HEAD_FLOOR)
        mixed[r, :] = (both * lax.rsqrt(level)).astype(bf16)

    row_tiles(seq, sequence)
    leave(mixed, w_o, 1, 1.0, None, False, by_core, by_core, (0, 1, 3, 6, 9, 12, 13), absorber(g3_ref, w_gu))

    def second_hidden(r):
        factor = row_factor(r)
        hidden[r, :] = silu_mul(acc[r, :ff] * factor, acc[r, ff : 2 * ff] * factor)

    row_tiles(own, second_hidden)
    leave(hidden, w_d, 0, 0.5, None, True, by_core, by_core, (0, 1, 4, 8))
    for kind in (SC, GATE, UP, DN, QKV, OUT):
        finish_sends(kind)


def fused_body(
    residual_in, gain_first, gain_mixer, gain_second,
    gate_weight, gate_scale, up_weight, up_scale, down_weight, down_scale,
    query_weight, query_scale, key_weight, key_scale, value_weight, value_scale,
    output_weight, output_scale,
):
    f32, bf16 = jnp.float32, jnp.bfloat16
    own, width = residual_in.shape
    rows, piece = 8 * own, gate_weight.shape[0]
    ff, hd = gate_weight.shape[1] // 4, query_weight.shape[1] // 4
    chunks = width // (2 * piece)

    def row(vector):
        return vector.reshape(1, -1)

    half = hd // 2
    frequency = np.float32(ROTARY_BASE) ** (-np.arange(half, dtype=np.float32) * np.float32(2.0) / np.float32(hd))
    angles = np.arange(2 * own, dtype=np.float32)[:, None] * frequency.astype(np.float32)[None]
    cosine, sine_value = np.cos(angles).astype(np.float32), np.sin(angles).astype(np.float32)
    operands = (
        residual_in, row(gain_first), row(gain_mixer), row(gain_second),
        gate_weight, up_weight, down_weight, query_weight, key_weight, value_weight, output_weight,
        row(gate_scale), row(up_scale), row(query_scale), row(key_scale), row(value_scale),
        row(down_scale), row(output_scale), jnp.asarray(cosine), jnp.asarray(sine_value),
    )
    dma = pltpu.SemaphoreType.DMA
    return pl.pallas_call(
        fused_kernel,
        out_shape=jax.ShapeDtypeStruct((own, width), bf16),
        in_specs=[pl.BlockSpec(memory_space=pl.ANY if 4 <= i < 11 else pltpu.VMEM) for i in range(len(operands))],
        out_specs=pl.BlockSpec(memory_space=pltpu.VMEM),
        scratch_shapes=[
            pltpu.VMEM((rows, width), bf16),
            pltpu.VMEM((rows, width), bf16),
            pltpu.VMEM((width, 2 * ff), bf16),
            pltpu.VMEM((ff, width), bf16),
            pltpu.VMEM((width, 3 * hd), bf16),
            pltpu.VMEM((hd, width), bf16),
            pltpu.VMEM((8 * (width // piece), piece), f32),
            pltpu.VMEM((4, piece, 2 * ff), bf16),
            pltpu.VMEM((4, ff, piece), bf16),
            pltpu.VMEM((4, piece, 3 * hd), bf16),
            pltpu.VMEM((4, hd, piece), bf16),
            pltpu.VMEM((8, piece), f32),
            pltpu.VMEM((rows, max(2 * ff, 3 * hd)), f32),
            pltpu.VMEM((rows, piece), f32),
            pltpu.VMEM((rows, ff), bf16),
            pltpu.VMEM((rows, hd), bf16),
            pltpu.VMEM((2, 4, own, width), bf16),
            pltpu.VMEM((4, own, width), bf16),
            pltpu.VMEM((3, own, width), bf16),
            pltpu.VMEM((3, own, width), bf16),
            *[pltpu.VMEM(operand.shape, f32) for operand in operands[4:11]],
            dma((7,)),
            dma((6, 16)), dma((6, 7)), dma((6, 8)),
            dma((chunks, 8)), dma((chunks, 7)),
            dma((chunks,)), dma((chunks,)), dma((chunks, 2)), dma((chunks, 2)),
        ],
        compiler_params=pltpu.CompilerParams(
            collective_id=0, has_side_effects=True, vmem_limit_bytes=63 * 2**20
        ),
    )(*operands)


def solution(mesh):
    n_fs, n_tp = mesh.shape["fs"], mesh.shape["tp"]
    share = math.gcd(math.gcd(HEADS // n_tp, n_fs), 4)
    if (n_fs, n_tp, share) == (16, 2, 4):
        body = fused_body
    else:
        body = make_body(n_fs, n_tp, share)
    in_specs = (
        P(("fs", "tp"), None),
        P(),
        P(),
        P(),
        P("fs", "tp"),
        P("tp"),
        P("fs", "tp"),
        P("tp"),
        P("tp", "fs"),
        P("fs"),
        P("fs", "tp"),
        P("tp"),
        P("fs", "tp"),
        P("tp"),
        P("fs", "tp"),
        P("tp"),
        P("tp", "fs"),
        P("fs"),
    )
    out_specs = P(("fs", "tp"), None)
    return jax.shard_map(body, mesh=mesh, in_specs=in_specs, out_specs=out_specs, check_vma=False)
```

```python
import functools
import math

import jax
import jax.numpy as jnp
import numpy as np
from jax import lax
from jax.experimental import pallas as pl
from jax.experimental.pallas import tpu as pltpu
from jax.sharding import PartitionSpec as P

HEADS = 8
HEAD_DIM = 256
BLOCK = 64


EPSILON = 1e-06
HEAD_FLOOR = 0.25
ROTARY_BASE = 10000.0
HIGHEST = lax.Precision.HIGHEST


def normalize(sequence_rows, gain_vector):
    values = sequence_rows.astype(jnp.float32)
    scaled = values * lax.rsqrt(jnp.mean(values * values, axis=-1, keepdims=True) + EPSILON)
    return (scaled * gain_vector).astype(jnp.bfloat16)


def head_rates(first_head, head_count, length):
    head_number = (first_head + jnp.arange(head_count)).astype(jnp.float32)
    return jnp.exp(jnp.log(1.0 / 16.0) + head_number / (HEADS - 1) * jnp.log(4.0 / length))


def rotate(values, positions):
    half_width = values.shape[-1] // 2
    frequency = ROTARY_BASE ** (-jnp.arange(half_width, dtype=jnp.float32) * 2.0 / values.shape[-1])
    angles = positions[:, None] * frequency[None, :]
    cosine = jnp.cos(angles)[:, None, :]
    sine_value = jnp.sin(angles)[:, None, :]
    front_half = values[..., :half_width]
    back_half = values[..., half_width:]
    return jnp.concatenate(
        [
            front_half * cosine - back_half * sine_value,
            back_half * cosine + front_half * sine_value,
        ],
        axis=-1,
    )


def retention(query_pre, key_pre, value_pre, decay_rates):
    length, head_count, head_width = query_pre.shape
    positions = jnp.arange(length, dtype=jnp.float32)
    query_rot = rotate(query_pre, positions).astype(jnp.bfloat16)
    key_rot = rotate(key_pre, positions).astype(jnp.bfloat16)
    value_low = value_pre.astype(jnp.bfloat16)
    blocks = length // BLOCK
    inside = jnp.arange(BLOCK, dtype=jnp.float32)
    distance = inside[:, None] - inside[None, :]
    within = jnp.where(
        distance >= 0, jnp.exp(-decay_rates[:, None, None] * jnp.maximum(distance, 0.0)), 0.0
    ) * head_width ** (-0.5)
    query_blocks = query_rot.reshape(blocks, BLOCK, head_count, head_width)
    key_blocks = key_rot.reshape(blocks, BLOCK, head_count, head_width)
    value_blocks = value_low.reshape(blocks, BLOCK, head_count, head_width)
    scores = jnp.einsum(
        "nihe,njhe->nhij", query_blocks, key_blocks, preferred_element_type=jnp.float32
    )
    weights = (scores * within[None]).astype(jnp.bfloat16)
    inner_part = jnp.einsum(
        "nhij,njhe->nihe", weights, value_blocks, preferred_element_type=jnp.float32
    )
    fading = jnp.exp(-decay_rates[None, :] * (BLOCK - 1.0 - inside[:, None])) * head_width ** (-0.5)
    key_faded = key_blocks.astype(jnp.float32) * fading[None, :, :, None]
    updates = jnp.einsum(
        "njhd,njhe->nhde", key_faded, value_blocks.astype(jnp.float32), precision=HIGHEST
    )
    block_decay = jnp.exp(-decay_rates * BLOCK)

    def advance(memory_state, update):
        return (memory_state * block_decay[:, None, None] + update, memory_state)

    _, before = lax.scan(
        advance, jnp.zeros((head_count, head_width, head_width), jnp.float32), updates
    )
    rising = jnp.exp(-decay_rates[None, :] * (inside[:, None] + 1.0))
    queried = query_blocks.astype(jnp.float32) * rising[None, :, :, None]
    carried_part = jnp.einsum("nihd,nhde->nihe", queried, before, precision=HIGHEST)
    combined = (inner_part + carried_part).reshape(length, head_count, head_width)
    normed = combined * lax.rsqrt(
        jnp.maximum(jnp.mean(combined * combined, axis=-1, keepdims=True), HEAD_FLOOR)
    )
    return normed.astype(jnp.bfloat16).reshape(length, head_count * head_width)


def split_three(values):
    high = values.astype(jnp.bfloat16)
    rest = values - high.astype(jnp.float32)
    middle_part = rest.astype(jnp.bfloat16)
    low = (rest - middle_part.astype(jnp.float32)).astype(jnp.bfloat16)
    return [high, middle_part, low]


def make_body(n_fs, n_tp, share):
    spread = n_fs // share
    STRIDED = False
    if STRIDED:
        teams = [[m * spread + r for m in range(share)] for r in range(spread)]
    else:
        teams = [[r * share + m for m in range(share)] for r in range(spread)]
    twins = [[team[m] for team in teams] for m in range(share)]
    row_teams = [[f * n_tp + t for f in team for t in range(n_tp)] for team in teams]

    def my_rank():
        position = lax.axis_index("fs")
        return position // spread if STRIDED else position % share

    def fetch(pieces):
        swapped = lax.all_to_all(
            pieces, "fs", split_axis=0, concat_axis=0, axis_index_groups=teams, tiled=True
        )
        return lax.all_gather(swapped, "fs", axis=0, axis_index_groups=twins, tiled=False)

    def order_features(rows):
        if not STRIDED:
            return rows
        count = rows.shape[0]
        return rows.reshape(count, share, spread, -1).swapaxes(1, 2).reshape(count, -1)

    def collect_rows(rows, gain_vector):
        return lax.all_gather(
            order_features(normalize(rows, gain_vector)),
            ("fs", "tp"),
            axis=0,
            axis_index_groups=row_teams,
            tiled=True,
        )

    def return_rows(inputs, weight, factor):
        term = jnp.dot(inputs, weight, preferred_element_type=jnp.float32) * factor
        return lax.psum_scatter(
            term.astype(jnp.bfloat16),
            ("fs", "tp"),
            scatter_dimension=0,
            axis_index_groups=row_teams,
            tiled=True,
        ).astype(jnp.float32)

    def columns_of(weight):
        low = weight.astype(jnp.bfloat16)
        return low.reshape(low.shape[0], share, -1).swapaxes(0, 1)

    def rows_of(weight):
        low = weight.astype(jnp.bfloat16)
        return low.reshape(share, -1, low.shape[1])

    def own(vector, rank):
        width = vector.shape[0] // share
        return lax.dynamic_slice_in_dim(vector, rank * width, width)

    def body(
        residual_in,
        gain_first,
        gain_mixer,
        gain_second,
        gate_weight,
        gate_scale,
        up_weight,
        up_scale,
        down_weight,
        down_scale,
        query_weight,
        query_scale,
        key_weight,
        key_scale,
        value_weight,
        value_scale,
        output_weight,
        output_scale,
    ):
        rank = my_rank()
        hidden_width = gate_weight.shape[1] // share
        mix_width = query_weight.shape[1] // share
        entry = fetch(jnp.concatenate([columns_of(gate_weight), columns_of(up_weight)], axis=2))
        factors = split_three(down_scale) + split_three(output_scale)
        factors = jnp.stack(factors + [jnp.zeros_like(factors[0])] * 10)
        leave_piece = jnp.concatenate(
            [
                rows_of(down_weight),
                rows_of(output_weight),
                jnp.broadcast_to(factors[None], (share,) + factors.shape),
            ],
            axis=1,
        )
        first_input = collect_rows(residual_in, gain_first)
        leave_piece, entry = lax.optimization_barrier((leave_piece, entry)) if False else (leave_piece, entry)
        leave = fetch(leave_piece)
        project_piece = jnp.concatenate(
            [columns_of(query_weight), columns_of(key_weight), columns_of(value_weight)], axis=2
        )
        project_piece, leave = lax.optimization_barrier((project_piece, leave)) if False else (project_piece, leave)
        project = fetch(project_piece)

        entry = entry.reshape(-1, 2 * hidden_width)
        project = project.reshape(-1, 3 * mix_width)
        if STRIDED:
            leave = leave.swapaxes(0, 1)
        leave = leave.transpose(2, 0, 1, 3).reshape(leave.shape[2], -1)
        down_full = leave[:hidden_width]
        output_full = leave[hidden_width : hidden_width + mix_width]
        parts = leave[hidden_width + mix_width :].astype(jnp.float32)
        down_factor = parts[0] + parts[1] + parts[2]
        output_factor = parts[3] + parts[4] + parts[5]
        gate_own, up_own = own(gate_scale, rank), own(up_scale, rank)

        def half_step(inputs):
            both = jnp.dot(inputs, entry, preferred_element_type=jnp.float32)
            gate_pre = both[:, :hidden_width] * gate_own
            up_pre = both[:, hidden_width:] * up_own
            hidden = (jax.nn.silu(gate_pre) * up_pre).astype(jnp.bfloat16)
            return return_rows(hidden, down_full, down_factor)

        mlp_first = half_step(first_input)
        middle = (residual_in.astype(jnp.float32) + 0.5 * mlp_first).astype(jnp.bfloat16)
        mixer_input = collect_rows(middle, gain_mixer)
        both = jnp.dot(mixer_input, project, preferred_element_type=jnp.float32)
        scale = jnp.concatenate([own(v, rank) for v in (query_scale, key_scale, value_scale)])
        length = residual_in.shape[0] * n_tp
        heads_own = mix_width // HEAD_DIM
        both = (both * scale).reshape(share, length, 3, heads_own, HEAD_DIM)
        first_head = (lax.axis_index("tp") * share + rank) * heads_own
        decay_rates = head_rates(first_head, heads_own, length)
        mixed = jax.vmap(lambda t: retention(t[:, 0], t[:, 1], t[:, 2], decay_rates))(both)
        mixer_out = return_rows(mixed.reshape(share * length, mix_width), output_full, output_factor)
        second = (middle.astype(jnp.float32) + mixer_out).astype(jnp.bfloat16)
        mlp_second = half_step(collect_rows(second, gain_second))
        return (second.astype(jnp.float32) + 0.5 * mlp_second).astype(jnp.bfloat16)

    return body


MESH = pl.DeviceIdType.MESH
GATE, UP, DN, QKV, OUT, SC = range(6)
PLANE = ((0, 0, 1), (0, 1, 0), (0, 1, 1), (1, 0, 0), (1, 1, 0), (1, 0, 1), (1, 1, 1))


EARLY = (
    (4, QKV, 0), (5, QKV, 1), (9, QKV, 2), (10, QKV, 3), (10, OUT, 0), (10, OUT, 1), (12, OUT, 2), (12, OUT, 3),
    (15, QKV, 4), (15, QKV, 5), (17, QKV, 6), (17, QKV, 7)
)


def fused_kernel(
    res_ref, g1_ref, g2_ref, g3_ref,
    gate_hbm, up_hbm, down_hbm, q_hbm, k_hbm, v_hbm, o_hbm,
    gs_ref, us_ref, qs_ref, ks_ref, vs_ref, ds_ref, os_ref, cos_ref, sin_ref,
    out_ref,
    rows_raw, rows_normed, w_gu, w_d, w_qkv, w_o, w_sc,
    st_gu, st_d, st_qkv, st_o, scales_ref, acc, power, hidden, mixed, part, part_twin, chip_part, far_part,
    gate_ref, up_ref, down_ref, q_ref, k_ref, v_ref, o_ref, in_sems,
    w_recv, w_send, w_fwd, ag_recv, ag_send, tw_recv, tw_send, rs_recv, rs_send,
):
    f32, bf16 = jnp.float32, jnp.bfloat16
    f, t = lax.axis_index("fs"), lax.axis_index("tp")
    x, y, z = f % 2, (f // 2) % 2, f // 4
    zl, zh = z % 2, z // 2
    me = zl * 2 + x
    own = res_ref.shape[0]
    width = res_ref.shape[1]
    seq = 2 * own
    ff = hidden.shape[1]
    hd = mixed.shape[1]
    piece = gate_ref.shape[0]
    chunk = 2 * piece
    chunks = width // chunk
    f_y = z * 4 + (1 - y) * 2 + x

    def plane_peer(dh, dl, dx):
        hh, ll, xx = (zh + dh) % 2, (zl + dl) % 2, (x + dx) % 2
        return (2 * hh + ll) * 4 + y * 2 + xx, ll * 2 + xx

    def remote(src, dst, send, recv, fs, tp):
        return pltpu.make_async_remote_copy(
            src_ref=src, dst_ref=dst, send_sem=send, recv_sem=recv, device_id=(fs, tp), device_id_type=MESH
        )

    sources = (gate_hbm, up_hbm, down_hbm, q_hbm, k_hbm, v_hbm, o_hbm)
    landed = (gate_ref, up_ref, down_ref, q_ref, k_ref, v_ref, o_ref)
    loads = [pltpu.make_async_copy(a, b, in_sems.at[i]) for i, (a, b) in enumerate(zip(sources, landed))]
    for load in loads:
        load.start()

    barrier = pltpu.get_barrier_semaphore()
    for dh, dl, dx in PLANE:
        peer, _ = plane_peer(dh, dl, dx)
        pl.semaphore_signal(barrier, inc=1, device_id=(peer, t), device_id_type=MESH)
    pl.semaphore_signal(barrier, inc=1, device_id=(f_y, t), device_id_type=MESH)
    pl.semaphore_signal(barrier, inc=1, device_id=(f, 1 - t), device_id_type=MESH)
    pl.semaphore_wait(barrier, 9)

    def slot(kind, s):
        if kind in (GATE, UP):
            return w_gu.at[pl.ds(pl.multiple_of(s * piece, piece), piece), pl.ds(kind * ff, ff)]
        if kind == DN:
            return w_d.at[:, pl.ds(pl.multiple_of(s * piece, piece), piece)]
        if kind == QKV:
            return w_qkv.at[pl.ds(pl.multiple_of(s * piece, piece), piece), :]
        if kind == OUT:
            return w_o.at[:, pl.ds(pl.multiple_of(s * piece, piece), piece)]
        return w_sc.at[pl.ds(pl.multiple_of(s * 8, 8), 8), :]

    def staged(kind, m):
        if kind == SC:
            return scales_ref
        if kind in (GATE, UP):
            return st_gu.at[m, :, pl.ds(kind * ff, ff)]
        return {DN: st_d, QKV: st_qkv, OUT: st_o}[kind].at[m]

    def send_across(kind):
        own_place = me if kind == DN else x
        remote(staged(kind, me), slot(kind, f), w_fwd.at[kind, own_place], w_recv.at[kind, f], f_y, t).start()

    def send_near(kind):
        send_some(kind, 0, 3)
        slot(kind, f)[...] = staged(kind, me)[...]

    def send_far(kind):
        send_some(kind, 3, 7)

    def send_some(kind, begin, end):
        for i in range(begin, end):
            peer, m = plane_peer(*PLANE[i])
            remote(staged(kind, m), slot(kind, f), w_send.at[kind, i], w_recv.at[kind, f], peer, t).start()

    def send_pieces(kind):
        send_across(kind)
        send_near(kind)
        send_far(kind)

    def pair_base(j):
        zz = 2 * ((zh + (j // 2) % 2) % 2) + j % 2
        return zz * 4 + ((y + j // 4) % 2) * 2

    def near_base(j):
        zz = 2 * ((zh + (j // 2) % 2) % 2) + (zl + j) % 2
        return zz * 4 + ((y + j // 4) % 2) * 2

    def take_pair(kind, j):
        base = pair_base(j) if kind == DN else near_base(j)
        for xx in (0, 1):
            s = base + xx

            @pl.when(s != f)
            def _():
                remote(slot(kind, s), slot(kind, s), w_fwd.at[kind, 0], w_recv.at[kind, s], f_y, t).wait_recv()

            @pl.when((s != f) & (j < 4))
            def _():
                remote(
                    slot(kind, s), slot(kind, s), w_fwd.at[kind, (j % 4) * 2 + xx], w_recv.at[kind, s], f_y, t
                ).start()

    def take_some(kind, begin, end):
        def step(j, _):
            take_pair(kind, j)
            return 0

        lax.fori_loop(begin, end, step, 0)

    def finish_sends(kind):
        for i, (dh, dl, dx) in enumerate(PLANE):
            peer, m = plane_peer(dh, dl, dx)
            remote(staged(kind, m), slot(kind, f), w_send.at[kind, i], w_recv.at[kind, f], peer, t).wait_send()
        for i in range(8):
            remote(slot(kind, f), slot(kind, f), w_fwd.at[kind, i], w_recv.at[kind, f], f_y, t).wait_send()

    def block_rows(m, core):
        return pl.ds(pl.multiple_of((m * 2 + core) * own, own), own)

    def column(j):
        return pl.multiple_of(pair_base(j) * piece, chunk)

    def ag_copy(j, i, src, m, core, fs, tp):
        dst = rows_raw.at[block_rows(m, core), pl.ds(column(j), chunk)]
        return remote(dst if src is None else src, dst, ag_send.at[j, i], ag_recv.at[j, m * 2 + core], fs, tp)

    def way(dl, dx):
        first, m_first = plane_peer(0, dl, dx)
        second, m_second = plane_peer(0, 1 - dl, 1 - dx)
        return first, second, m_first, m_second, plane_peer(0, 1, 1)[1]

    z_then_x, x_then_z, by_core = way(1, 0), way(0, 1), way(t, 1 - t)

    def ag_start(j, src, route):
        first, second, _, _, _ = route
        ag_copy(j, 0, src, me, t, first, t).start()
        ag_copy(j, 1, src, me, t, second, t).start()
        ag_copy(j, 2, src, me, t, f, 1 - t).start()

    def ag_relay(j, route):
        _, second, m_first, _, _ = route
        ag_copy(j, 3, None, m_first, t, second, t).wait_recv()
        ag_copy(j, 3, None, m_first, t, second, t).start()
        ag_copy(j, 4, None, m_first, t, f, 1 - t).start()

    def ag_pass(j, route):
        for i, m in enumerate(route[3:]):
            ag_copy(j, 5 + i, None, m, t, f, 1 - t).wait_recv()
            ag_copy(j, 5 + i, None, m, t, f, 1 - t).start()

    def ag_arrive(j):
        for m in range(4):
            ag_copy(j, 0, None, m, 1 - t, f, 1 - t).wait_recv()

    def ag_settle(j):
        for i in range(7):
            ag_copy(j, i, None, me, t, f, 1 - t).wait_send()

    def each_chunk(body):
        def step(j, _):
            body(j)
            return 0

        lax.fori_loop(0, chunks, step, 0)

    def norm_rows(gain_ref):
        def step(i, _):
            at = pl.ds(pl.multiple_of(i * 32, 32), 32)
            v = rows_raw[at, :].astype(f32)
            r = lax.rsqrt(jnp.mean(v * v, axis=-1, keepdims=True) + EPSILON)
            rows_normed[at, :] = (v * r * gain_ref[...]).astype(bf16)
            return 0

        lax.fori_loop(0, rows_raw.shape[0] // 32, step, 0)

    def row_tiles(size, body):
        def step(i, _):
            body(pl.ds(pl.multiple_of(i * size, size), size))
            return 0

        lax.fori_loop(0, rows_raw.shape[0] // size, step, 0)

    def absorber(gain_ref, weights):
        columns = weights.shape[1]

        def stage(j):
            at = pl.ds(column(j), chunk)

            @pl.when(j == 0)
            def _():
                def clear(r):
                    acc[r, :columns] = jnp.zeros((seq, columns), f32)
                    power[r, :] = jnp.zeros((seq, piece), f32)

                row_tiles(seq, clear)

            ag_arrive(j)

            def tile(r):
                v = rows_raw[r, at].astype(f32)
                square = v * v
                power[r, :] += square[:, :piece] + square[:, piece:]
                v = (v * gain_ref[:, at]).astype(bf16)
                acc[r, :columns] += jnp.dot(v, weights[at, :], preferred_element_type=f32)

            row_tiles(4 * seq, tile)

        return stage

    def row_factor(r):
        return lax.rsqrt(jnp.sum(power[r, :], axis=-1, keepdims=True) / width + EPSILON)

    def silu_mul(gate, up):
        gate = gate * gs_ref[:, pl.ds(pl.multiple_of(me * ff, ff), ff)]
        return (gate / (1.0 + jnp.exp(-gate)) * (up * us_ref[:, pl.ds(pl.multiple_of(me * ff, ff), ff)])).astype(bf16)

    def leave(inputs, weights, scale_row, factor, arriving, last, sums, rows, lags, absorb=None, during=None):
        def product(j):
            if arriving is not None:
                take_pair(arriving, j)
            base = pair_base(j)
            at = pl.ds(column(j), chunk)
            factors = jnp.concatenate(
                [w_sc[pl.ds((base + h) * 8 + scale_row, 1), :] for h in (0, 1)], axis=1
            )

            term = jnp.dot(inputs[...], weights[:, at], preferred_element_type=f32) * factors
            term = term.astype(bf16)
            for m in range(4):
                for core in range(2):
                    part[core, m, :, at] = term[(m * 2 + core) * own : (m * 2 + core + 1) * own]
            to_twin(j).start()

        def to_twin(j):
            at = pl.ds(column(j), chunk)
            return remote(part.at[1 - t, :, :, at], part_twin.at[:, :, at], tw_send.at[j], tw_recv.at[j], f, 1 - t)

        first, second, m_first, m_second, m_third = sums

        def to_first(j):
            at = pl.ds(column(j), chunk)
            pair = pl.ds(0, 2)
            return remote(
                chip_part.at[pair, :, at], far_part.at[pair, :, at], rs_send.at[j, 0], rs_recv.at[j, 0], first, t
            )

        def to_second(j):
            at = pl.ds(column(j), chunk)
            return remote(chip_part.at[2, :, at], far_part.at[2, :, at], rs_send.at[j, 1], rs_recv.at[j, 1], second, t)

        def chip_sum(m, at):
            return part[t, m, :, at].astype(f32) + part_twin[m, :, at].astype(f32)

        def reduce(j):
            at = pl.ds(column(j), chunk)
            to_twin(j).wait_recv()
            chip_part[0, :, at] = chip_sum(m_first, at).astype(bf16)
            chip_part[1, :, at] = chip_sum(m_third, at).astype(bf16)
            to_first(j).start()

        def relay(j):
            at = pl.ds(column(j), chunk)
            to_first(j).wait_recv()
            chip_part[2, :, at] = (chip_sum(m_second, at) + far_part[1, :, at].astype(f32)).astype(bf16)
            to_second(j).start()

        def finish(j):
            at = pl.ds(column(j), chunk)
            to_second(j).wait_recv()
            total = chip_sum(me, at) + far_part[0, :, at].astype(f32) + far_part[2, :, at].astype(f32)
            mine = block_rows(me, t)
            fresh = (rows_raw[mine, at].astype(f32) + factor * total).astype(bf16)
            if last:
                out_ref[:, at] = fresh
            else:
                rows_raw[mine, at] = fresh
                ag_start(j, None, rows)

        stages = [product, reduce, relay, finish]
        if not last:
            stages += [lambda j: ag_relay(j, rows), lambda j: ag_pass(j, rows), absorb]

        def step(i, _):
            for lag, stage in zip(lags, stages):
                pl.when((i >= lag) & (i < chunks + lag))(lambda stage=stage, lag=lag: stage(i - lag))
            if during is not None:
                during(i)
            return 0

        lax.fori_loop(0, chunks + lags[len(stages) - 1], step, 0)

        def drain(j, _):
            to_twin(j).wait_send()
            to_first(j).wait_send()
            to_second(j).wait_send()
            return 0

        lax.fori_loop(0, chunks, drain, 0)
        if not last:
            each_chunk(ag_settle)

    scales_ref[...] = jnp.zeros_like(scales_ref)
    scales_ref[0:1, :] = ds_ref[...]
    scales_ref[1:2, :] = os_ref[...]
    send_pieces(SC)

    loads[0].wait()
    for m in range(4):
        at = slice(m * ff, (m + 1) * ff)
        st_gu[m, :, :ff] = gate_ref[:, at].astype(bf16)
    send_pieces(GATE)
    each_chunk(lambda j: ag_start(j, res_ref.at[:, pl.ds(column(j), chunk)], z_then_x))
    rows_raw[block_rows(me, t), :] = res_ref[...]

    loads[1].wait()
    for m in range(4):
        st_gu[m, :, ff:] = up_ref[:, m * ff : (m + 1) * ff].astype(bf16)
    send_pieces(UP)
    for load in loads[2:]:
        load.wait()
    for m in range(4):
        at = slice(m * hd, (m + 1) * hd)
        st_d[m] = down_ref[m * ff : (m + 1) * ff, :].astype(bf16)
        st_qkv[m, :, :hd] = q_ref[:, at].astype(bf16)
        st_qkv[m, :, hd : 2 * hd] = k_ref[:, at].astype(bf16)
        st_qkv[m, :, 2 * hd :] = v_ref[:, at].astype(bf16)
        st_o[m] = o_ref[at, :].astype(bf16)

    for kind in (DN, QKV, OUT):
        send_across(kind)

    ahead = zl != zh
    take_some(SC, 0, 4)
    take_some(GATE, 0, 4)
    each_chunk(lambda j: ag_relay(j, z_then_x))
    send_near(DN)
    pl.when(ahead)(lambda: send_far(DN))
    send_near(QKV)
    send_near(OUT)
    take_some(UP, 0, 2)
    each_chunk(lambda j: ag_pass(j, z_then_x))
    each_chunk(ag_arrive)
    each_chunk(ag_settle)
    norm_rows(g1_ref)
    take_some(UP, 2, 3)
    take_some(GATE, 4, 8)

    def first_gate(r):
        acc[r, :ff] = jnp.dot(rows_normed[r, :], w_gu[:, :ff], preferred_element_type=f32)

    row_tiles(2 * seq, first_gate)
    take_some(UP, 3, 4)
    pl.when(ahead)(lambda: send_far(QKV))
    pl.when(jnp.logical_not(ahead))(lambda: send_far(DN))
    take_some(UP, 4, 8)
    take_some(SC, 4, 8)

    def first_hidden(r):
        up = jnp.dot(rows_normed[r, :], w_gu[:, ff:], preferred_element_type=f32)
        hidden[r, :] = silu_mul(acc[r, :ff], up)

    row_tiles(2 * seq, first_hidden)

    def take_early(i):
        pl.when((i == 3) & ahead)(lambda: send_far(OUT))
        pl.when((i == 3) & jnp.logical_not(ahead))(lambda: send_far(QKV))
        pl.when((i == 8) & jnp.logical_not(ahead))(lambda: send_far(OUT))
        for at, kind, j in EARLY:
            pl.when(i == at)(lambda kind=kind, j=j: take_pair(kind, j))

    leave(hidden, w_d, 0, 0.5, DN, False, x_then_z, by_core, (0, 1, 4, 7, 9, 11, 12), absorber(g2_ref, w_qkv), take_early)

    take_some(OUT, 4, 8)
    head = (t * 4 + me).astype(f32)
    ri = lax.broadcasted_iota(jnp.int32, (seq, seq), 0)
    ci = lax.broadcasted_iota(jnp.int32, (seq, seq), 1)
    rate = jnp.exp(math.log(1.0 / 16.0) + jnp.full((seq, seq), head, f32) / (HEADS - 1) * math.log(4.0 / seq))
    distance = jnp.maximum(ri - ci, 0).astype(f32)
    decay = jnp.where(ri >= ci, jnp.exp(-rate * distance), 0.0) * hd ** (-0.5)

    at_head = pl.ds(pl.multiple_of(me * hd, hd), hd)

    def turn(values):
        a, b = values[:, : hd // 2], values[:, hd // 2 :]
        c, s = cos_ref[...], sin_ref[...]
        return jnp.concatenate([a * c - b * s, b * c + a * s], axis=1).astype(bf16)

    def sequence(r):
        factor = row_factor(r)
        q = turn(acc[r, :hd] * factor * qs_ref[:, at_head])
        k = turn(acc[r, hd : 2 * hd] * factor * ks_ref[:, at_head])
        v = (acc[r, 2 * hd : 3 * hd] * factor * vs_ref[:, at_head]).astype(bf16)
        scores = lax.dot_general(q, k, (((1,), (1,)), ((), ())), preferred_element_type=f32)
        both = jnp.dot((scores * decay).astype(bf16), v, preferred_element_type=f32)
        level = jnp.maximum(jnp.mean(both * both, axis=-1, keepdims=True), HEAD_FLOOR)
        mixed[r, :] = (both * lax.rsqrt(level)).astype(bf16)

    row_tiles(seq, sequence)
    leave(mixed, w_o, 1, 1.0, None, False, by_core, by_core, (0, 1, 3, 6, 9, 12, 13), absorber(g3_ref, w_gu))

    def second_hidden(r):
        factor = row_factor(r)
        hidden[r, :] = silu_mul(acc[r, :ff] * factor, acc[r, ff : 2 * ff] * factor)

    row_tiles(own, second_hidden)
    leave(hidden, w_d, 0, 0.5, None, True, by_core, by_core, (0, 1, 4, 8))
    for kind in (SC, GATE, UP, DN, QKV, OUT):
        finish_sends(kind)


def fused_body(
    residual_in, gain_first, gain_mixer, gain_second,
    gate_weight, gate_scale, up_weight, up_scale, down_weight, down_scale,
    query_weight, query_scale, key_weight, key_scale, value_weight, value_scale,
    output_weight, output_scale,
):
    f32, bf16 = jnp.float32, jnp.bfloat16
    own, width = residual_in.shape
    rows, piece = 8 * own, gate_weight.shape[0]
    ff, hd = gate_weight.shape[1] // 4, query_weight.shape[1] // 4
    chunks = width // (2 * piece)

    def row(vector):
        return vector.reshape(1, -1)

    half = hd // 2
    frequency = np.float32(ROTARY_BASE) ** (-np.arange(half, dtype=np.float32) * np.float32(2.0) / np.float32(hd))
    angles = np.arange(2 * own, dtype=np.float32)[:, None] * frequency.astype(np.float32)[None]
    cosine, sine_value = np.cos(angles).astype(np.float32), np.sin(angles).astype(np.float32)
    operands = (
        residual_in, row(gain_first), row(gain_mixer), row(gain_second),
        gate_weight, up_weight, down_weight, query_weight, key_weight, value_weight, output_weight,
        row(gate_scale), row(up_scale), row(query_scale), row(key_scale), row(value_scale),
        row(down_scale), row(output_scale), jnp.asarray(cosine), jnp.asarray(sine_value),
    )
    dma = pltpu.SemaphoreType.DMA
    return pl.pallas_call(
        fused_kernel,
        out_shape=jax.ShapeDtypeStruct((own, width), bf16),
        in_specs=[pl.BlockSpec(memory_space=pl.ANY if 4 <= i < 11 else pltpu.VMEM) for i in range(len(operands))],
        out_specs=pl.BlockSpec(memory_space=pltpu.VMEM),
        scratch_shapes=[
            pltpu.VMEM((rows, width), bf16),
            pltpu.VMEM((rows, width), bf16),
            pltpu.VMEM((width, 2 * ff), bf16),
            pltpu.VMEM((ff, width), bf16),
            pltpu.VMEM((width, 3 * hd), bf16),
            pltpu.VMEM((hd, width), bf16),
            pltpu.VMEM((8 * (width // piece), piece), f32),
            pltpu.VMEM((4, piece, 2 * ff), bf16),
            pltpu.VMEM((4, ff, piece), bf16),
            pltpu.VMEM((4, piece, 3 * hd), bf16),
            pltpu.VMEM((4, hd, piece), bf16),
            pltpu.VMEM((8, piece), f32),
            pltpu.VMEM((rows, max(2 * ff, 3 * hd)), f32),
            pltpu.VMEM((rows, piece), f32),
            pltpu.VMEM((rows, ff), bf16),
            pltpu.VMEM((rows, hd), bf16),
            pltpu.VMEM((2, 4, own, width), bf16),
            pltpu.VMEM((4, own, width), bf16),
            pltpu.VMEM((3, own, width), bf16),
            pltpu.VMEM((3, own, width), bf16),
            *[pltpu.VMEM(operand.shape, f32) for operand in operands[4:11]],
            dma((7,)),
            dma((6, 16)), dma((6, 7)), dma((6, 8)),
            dma((chunks, 8)), dma((chunks, 7)),
            dma((chunks,)), dma((chunks,)), dma((chunks, 2)), dma((chunks, 2)),
        ],
        compiler_params=pltpu.CompilerParams(
            collective_id=0, has_side_effects=True, vmem_limit_bytes=63 * 2**20
        ),
    )(*operands)


def solution(mesh):
    n_fs, n_tp = mesh.shape["fs"], mesh.shape["tp"]
    share = math.gcd(math.gcd(HEADS // n_tp, n_fs), 4)
    if (n_fs, n_tp, share) == (16, 2, 4):
        body = fused_body
    else:
        body = make_body(n_fs, n_tp, share)
    in_specs = (
        P(("fs", "tp"), None),
        P(),
        P(),
        P(),
        P("fs", "tp"),
        P("tp"),
        P("fs", "tp"),
        P("tp"),
        P("tp", "fs"),
        P("fs"),
        P("fs", "tp"),
        P("tp"),
        P("fs", "tp"),
        P("tp"),
        P("fs", "tp"),
        P("tp"),
        P("tp", "fs"),
        P("fs"),
    )
    out_specs = P(("fs", "tp"), None)
    return jax.shard_map(body, mesh=mesh, in_specs=in_specs, out_specs=out_specs, check_vma=False)
```

```python
import functools
import math

import jax
import jax.numpy as jnp
import numpy as np
from jax import lax
from jax.experimental import pallas as pl
from jax.experimental.pallas import tpu as pltpu
from jax.sharding import PartitionSpec as P

HEADS = 8
HEAD_DIM = 256
BLOCK = 64


EPSILON = 1e-06
HEAD_FLOOR = 0.25
ROTARY_BASE = 10000.0
HIGHEST = lax.Precision.HIGHEST


def normalize(sequence_rows, gain_vector):
    values = sequence_rows.astype(jnp.float32)
    scaled = values * lax.rsqrt(jnp.mean(values * values, axis=-1, keepdims=True) + EPSILON)
    return (scaled * gain_vector).astype(jnp.bfloat16)


def head_rates(first_head, head_count, length):
    head_number = (first_head + jnp.arange(head_count)).astype(jnp.float32)
    return jnp.exp(jnp.log(1.0 / 16.0) + head_number / (HEADS - 1) * jnp.log(4.0 / length))


def rotate(values, positions):
    half_width = values.shape[-1] // 2
    frequency = ROTARY_BASE ** (-jnp.arange(half_width, dtype=jnp.float32) * 2.0 / values.shape[-1])
    angles = positions[:, None] * frequency[None, :]
    cosine = jnp.cos(angles)[:, None, :]
    sine_value = jnp.sin(angles)[:, None, :]
    front_half = values[..., :half_width]
    back_half = values[..., half_width:]
    return jnp.concatenate(
        [
            front_half * cosine - back_half * sine_value,
            back_half * cosine + front_half * sine_value,
        ],
        axis=-1,
    )


def retention(query_pre, key_pre, value_pre, decay_rates):
    length, head_count, head_width = query_pre.shape
    positions = jnp.arange(length, dtype=jnp.float32)
    query_rot = rotate(query_pre, positions).astype(jnp.bfloat16)
    key_rot = rotate(key_pre, positions).astype(jnp.bfloat16)
    value_low = value_pre.astype(jnp.bfloat16)
    blocks = length // BLOCK
    inside = jnp.arange(BLOCK, dtype=jnp.float32)
    distance = inside[:, None] - inside[None, :]
    within = jnp.where(
        distance >= 0, jnp.exp(-decay_rates[:, None, None] * jnp.maximum(distance, 0.0)), 0.0
    ) * head_width ** (-0.5)
    query_blocks = query_rot.reshape(blocks, BLOCK, head_count, head_width)
    key_blocks = key_rot.reshape(blocks, BLOCK, head_count, head_width)
    value_blocks = value_low.reshape(blocks, BLOCK, head_count, head_width)
    scores = jnp.einsum(
        "nihe,njhe->nhij", query_blocks, key_blocks, preferred_element_type=jnp.float32
    )
    weights = (scores * within[None]).astype(jnp.bfloat16)
    inner_part = jnp.einsum(
        "nhij,njhe->nihe", weights, value_blocks, preferred_element_type=jnp.float32
    )
    fading = jnp.exp(-decay_rates[None, :] * (BLOCK - 1.0 - inside[:, None])) * head_width ** (-0.5)
    key_faded = key_blocks.astype(jnp.float32) * fading[None, :, :, None]
    updates = jnp.einsum(
        "njhd,njhe->nhde", key_faded, value_blocks.astype(jnp.float32), precision=HIGHEST
    )
    block_decay = jnp.exp(-decay_rates * BLOCK)

    def advance(memory_state, update):
        return (memory_state * block_decay[:, None, None] + update, memory_state)

    _, before = lax.scan(
        advance, jnp.zeros((head_count, head_width, head_width), jnp.float32), updates
    )
    rising = jnp.exp(-decay_rates[None, :] * (inside[:, None] + 1.0))
    queried = query_blocks.astype(jnp.float32) * rising[None, :, :, None]
    carried_part = jnp.einsum("nihd,nhde->nihe", queried, before, precision=HIGHEST)
    combined = (inner_part + carried_part).reshape(length, head_count, head_width)
    normed = combined * lax.rsqrt(
        jnp.maximum(jnp.mean(combined * combined, axis=-1, keepdims=True), HEAD_FLOOR)
    )
    return normed.astype(jnp.bfloat16).reshape(length, head_count * head_width)


def split_three(values):
    high = values.astype(jnp.bfloat16)
    rest = values - high.astype(jnp.float32)
    middle_part = rest.astype(jnp.bfloat16)
    low = (rest - middle_part.astype(jnp.float32)).astype(jnp.bfloat16)
    return [high, middle_part, low]


def make_body(n_fs, n_tp, share):
    spread = n_fs // share
    STRIDED = False
    if STRIDED:
        teams = [[m * spread + r for m in range(share)] for r in range(spread)]
    else:
        teams = [[r * share + m for m in range(share)] for r in range(spread)]
    twins = [[team[m] for team in teams] for m in range(share)]
    row_teams = [[f * n_tp + t for f in team for t in range(n_tp)] for team in teams]

    def my_rank():
        position = lax.axis_index("fs")
        return position // spread if STRIDED else position % share

    def fetch(pieces):
        swapped = lax.all_to_all(
            pieces, "fs", split_axis=0, concat_axis=0, axis_index_groups=teams, tiled=True
        )
        return lax.all_gather(swapped, "fs", axis=0, axis_index_groups=twins, tiled=False)

    def order_features(rows):
        if not STRIDED:
            return rows
        count = rows.shape[0]
        return rows.reshape(count, share, spread, -1).swapaxes(1, 2).reshape(count, -1)

    def collect_rows(rows, gain_vector):
        return lax.all_gather(
            order_features(normalize(rows, gain_vector)),
            ("fs", "tp"),
            axis=0,
            axis_index_groups=row_teams,
            tiled=True,
        )

    def return_rows(inputs, weight, factor):
        term = jnp.dot(inputs, weight, preferred_element_type=jnp.float32) * factor
        return lax.psum_scatter(
            term.astype(jnp.bfloat16),
            ("fs", "tp"),
            scatter_dimension=0,
            axis_index_groups=row_teams,
            tiled=True,
        ).astype(jnp.float32)

    def columns_of(weight):
        low = weight.astype(jnp.bfloat16)
        return low.reshape(low.shape[0], share, -1).swapaxes(0, 1)

    def rows_of(weight):
        low = weight.astype(jnp.bfloat16)
        return low.reshape(share, -1, low.shape[1])

    def own(vector, rank):
        width = vector.shape[0] // share
        return lax.dynamic_slice_in_dim(vector, rank * width, width)

    def body(
        residual_in,
        gain_first,
        gain_mixer,
        gain_second,
        gate_weight,
        gate_scale,
        up_weight,
        up_scale,
        down_weight,
        down_scale,
        query_weight,
        query_scale,
        key_weight,
        key_scale,
        value_weight,
        value_scale,
        output_weight,
        output_scale,
    ):
        rank = my_rank()
        hidden_width = gate_weight.shape[1] // share
        mix_width = query_weight.shape[1] // share
        entry = fetch(jnp.concatenate([columns_of(gate_weight), columns_of(up_weight)], axis=2))
        factors = split_three(down_scale) + split_three(output_scale)
        factors = jnp.stack(factors + [jnp.zeros_like(factors[0])] * 10)
        leave_piece = jnp.concatenate(
            [
                rows_of(down_weight),
                rows_of(output_weight),
                jnp.broadcast_to(factors[None], (share,) + factors.shape),
            ],
            axis=1,
        )
        first_input = collect_rows(residual_in, gain_first)
        leave_piece, entry = lax.optimization_barrier((leave_piece, entry)) if False else (leave_piece, entry)
        leave = fetch(leave_piece)
        project_piece = jnp.concatenate(
            [columns_of(query_weight), columns_of(key_weight), columns_of(value_weight)], axis=2
        )
        project_piece, leave = lax.optimization_barrier((project_piece, leave)) if False else (project_piece, leave)
        project = fetch(project_piece)

        entry = entry.reshape(-1, 2 * hidden_width)
        project = project.reshape(-1, 3 * mix_width)
        if STRIDED:
            leave = leave.swapaxes(0, 1)
        leave = leave.transpose(2, 0, 1, 3).reshape(leave.shape[2], -1)
        down_full = leave[:hidden_width]
        output_full = leave[hidden_width : hidden_width + mix_width]
        parts = leave[hidden_width + mix_width :].astype(jnp.float32)
        down_factor = parts[0] + parts[1] + parts[2]
        output_factor = parts[3] + parts[4] + parts[5]
        gate_own, up_own = own(gate_scale, rank), own(up_scale, rank)

        def half_step(inputs):
            both = jnp.dot(inputs, entry, preferred_element_type=jnp.float32)
            gate_pre = both[:, :hidden_width] * gate_own
            up_pre = both[:, hidden_width:] * up_own
            hidden = (jax.nn.silu(gate_pre) * up_pre).astype(jnp.bfloat16)
            return return_rows(hidden, down_full, down_factor)

        mlp_first = half_step(first_input)
        middle = (residual_in.astype(jnp.float32) + 0.5 * mlp_first).astype(jnp.bfloat16)
        mixer_input = collect_rows(middle, gain_mixer)
        both = jnp.dot(mixer_input, project, preferred_element_type=jnp.float32)
        scale = jnp.concatenate([own(v, rank) for v in (query_scale, key_scale, value_scale)])
        length = residual_in.shape[0] * n_tp
        heads_own = mix_width // HEAD_DIM
        both = (both * scale).reshape(share, length, 3, heads_own, HEAD_DIM)
        first_head = (lax.axis_index("tp") * share + rank) * heads_own
        decay_rates = head_rates(first_head, heads_own, length)
        mixed = jax.vmap(lambda t: retention(t[:, 0], t[:, 1], t[:, 2], decay_rates))(both)
        mixer_out = return_rows(mixed.reshape(share * length, mix_width), output_full, output_factor)
        second = (middle.astype(jnp.float32) + mixer_out).astype(jnp.bfloat16)
        mlp_second = half_step(collect_rows(second, gain_second))
        return (second.astype(jnp.float32) + 0.5 * mlp_second).astype(jnp.bfloat16)

    return body


MESH = pl.DeviceIdType.MESH
GATE, UP, DN, QKV, OUT, SC = range(6)
PLANE = ((0, 0, 1), (0, 1, 0), (0, 1, 1), (1, 0, 0), (1, 1, 0), (1, 0, 1), (1, 1, 1))


EARLY = (
    (4, QKV, 0), (5, QKV, 1), (9, QKV, 2), (10, QKV, 3), (10, OUT, 0), (10, OUT, 1), (12, OUT, 2), (12, OUT, 3),
    (15, QKV, 4), (15, QKV, 5), (17, QKV, 6), (17, QKV, 7)
)


def fused_kernel(
    res_ref, g1_ref, g2_ref, g3_ref,
    gate_hbm, up_hbm, down_hbm, q_hbm, k_hbm, v_hbm, o_hbm,
    gs_ref, us_ref, qs_ref, ks_ref, vs_ref, ds_ref, os_ref, cos_ref, sin_ref,
    out_ref,
    rows_raw, rows_normed, w_gu, w_d, w_qkv, w_o, w_sc,
    st_gu, st_d, st_qkv, st_o, scales_ref, acc, power, hidden, mixed, part, part_twin, chip_part, far_part,
    gate_ref, up_ref, down_ref, q_ref, k_ref, v_ref, o_ref, in_sems,
    w_recv, w_send, w_fwd, ag_recv, ag_send, tw_recv, tw_send, rs_recv, rs_send,
):
    f32, bf16 = jnp.float32, jnp.bfloat16
    f, t = lax.axis_index("fs"), lax.axis_index("tp")
    x, y, z = f % 2, (f // 2) % 2, f // 4
    zl, zh = z % 2, z // 2
    me = zl * 2 + x
    own = res_ref.shape[0]
    width = res_ref.shape[1]
    seq = 2 * own
    ff = hidden.shape[1]
    hd = mixed.shape[1]
    piece = gate_ref.shape[0]
    chunk = 2 * piece
    chunks = width // chunk
    f_y = z * 4 + (1 - y) * 2 + x

    def plane_peer(dh, dl, dx):
        hh, ll, xx = (zh + dh) % 2, (zl + dl) % 2, (x + dx) % 2
        return (2 * hh + ll) * 4 + y * 2 + xx, ll * 2 + xx

    def remote(src, dst, send, recv, fs, tp):
        return pltpu.make_async_remote_copy(
            src_ref=src, dst_ref=dst, send_sem=send, recv_sem=recv, device_id=(fs, tp), device_id_type=MESH
        )

    sources = (gate_hbm, up_hbm, down_hbm, q_hbm, k_hbm, v_hbm, o_hbm)
    landed = (gate_ref, up_ref, down_ref, q_ref, k_ref, v_ref, o_ref)
    loads = [pltpu.make_async_copy(a, b, in_sems.at[i]) for i, (a, b) in enumerate(zip(sources, landed))]
    for load in loads:
        load.start()

    barrier = pltpu.get_barrier_semaphore()
    for dh, dl, dx in PLANE:
        peer, _ = plane_peer(dh, dl, dx)
        pl.semaphore_signal(barrier, inc=1, device_id=(peer, t), device_id_type=MESH)
    pl.semaphore_signal(barrier, inc=1, device_id=(f_y, t), device_id_type=MESH)
    pl.semaphore_signal(barrier, inc=1, device_id=(f, 1 - t), device_id_type=MESH)
    pl.semaphore_wait(barrier, 9)

    def slot(kind, s):
        if kind in (GATE, UP):
            return w_gu.at[pl.ds(pl.multiple_of(s * piece, piece), piece), pl.ds(kind * ff, ff)]
        if kind == DN:
            return w_d.at[:, pl.ds(pl.multiple_of(s * piece, piece), piece)]
        if kind == QKV:
            return w_qkv.at[pl.ds(pl.multiple_of(s * piece, piece), piece), :]
        if kind == OUT:
            return w_o.at[:, pl.ds(pl.multiple_of(s * piece, piece), piece)]
        return w_sc.at[pl.ds(pl.multiple_of(s * 8, 8), 8), :]

    def staged(kind, m):
        if kind == SC:
            return scales_ref
        if kind in (GATE, UP):
            return st_gu.at[m, :, pl.ds(kind * ff, ff)]
        return {DN: st_d, QKV: st_qkv, OUT: st_o}[kind].at[m]

    def send_across(kind):
        own_place = me if kind == DN else x
        remote(staged(kind, me), slot(kind, f), w_fwd.at[kind, own_place], w_recv.at[kind, f], f_y, t).start()

    def send_near(kind):
        send_some(kind, 0, 3)
        slot(kind, f)[...] = staged(kind, me)[...]

    def send_far(kind):
        send_some(kind, 3, 7)

    def send_some(kind, begin, end):
        for i in range(begin, end):
            peer, m = plane_peer(*PLANE[i])
            remote(staged(kind, m), slot(kind, f), w_send.at[kind, i], w_recv.at[kind, f], peer, t).start()

    def send_pieces(kind):
        send_across(kind)
        send_near(kind)
        send_far(kind)

    def pair_base(j):
        zz = 2 * ((zh + (j // 2) % 2) % 2) + j % 2
        return zz * 4 + ((y + j // 4) % 2) * 2

    def near_base(j):
        zz = 2 * ((zh + (j // 2) % 2) % 2) + (zl + j) % 2
        return zz * 4 + ((y + j // 4) % 2) * 2

    def take_pair(kind, j):
        base = pair_base(j) if kind == DN else near_base(j)
        for xx in (0, 1):
            s = base + xx

            @pl.when(s != f)
            def _():
                remote(slot(kind, s), slot(kind, s), w_fwd.at[kind, 0], w_recv.at[kind, s], f_y, t).wait_recv()

            @pl.when((s != f) & (j < 4))
            def _():
                remote(
                    slot(kind, s), slot(kind, s), w_fwd.at[kind, (j % 4) * 2 + xx], w_recv.at[kind, s], f_y, t
                ).start()

    def take_some(kind, begin, end):
        def step(j, _):
            take_pair(kind, j)
            return 0

        lax.fori_loop(begin, end, step, 0)

    def finish_sends(kind):
        for i, (dh, dl, dx) in enumerate(PLANE):
            peer, m = plane_peer(dh, dl, dx)
            remote(staged(kind, m), slot(kind, f), w_send.at[kind, i], w_recv.at[kind, f], peer, t).wait_send()
        for i in range(8):
            remote(slot(kind, f), slot(kind, f), w_fwd.at[kind, i], w_recv.at[kind, f], f_y, t).wait_send()

    def block_rows(m, core):
        return pl.ds(pl.multiple_of((m * 2 + core) * own, own), own)

    def column(j):
        return pl.multiple_of(pair_base(j) * piece, chunk)

    def ag_copy(j, i, src, m, core, fs, tp):
        dst = rows_raw.at[block_rows(m, core), pl.ds(column(j), chunk)]
        return remote(dst if src is None else src, dst, ag_send.at[j, i], ag_recv.at[j, m * 2 + core], fs, tp)

    def way(dl, dx):
        first, m_first = plane_peer(0, dl, dx)
        second, m_second = plane_peer(0, 1 - dl, 1 - dx)
        return first, second, m_first, m_second, plane_peer(0, 1, 1)[1]

    z_then_x, x_then_z, by_core = way(1, 0), way(0, 1), way(t, 1 - t)

    def ag_start(j, src, route):
        first, second, _, _, _ = route
        ag_copy(j, 0, src, me, t, first, t).start()
        ag_copy(j, 1, src, me, t, second, t).start()
        ag_copy(j, 2, src, me, t, f, 1 - t).start()

    def ag_relay(j, route):
        _, second, m_first, _, _ = route
        ag_copy(j, 3, None, m_first, t, second, t).wait_recv()
        ag_copy(j, 3, None, m_first, t, second, t).start()
        ag_copy(j, 4, None, m_first, t, f, 1 - t).start()

    def ag_pass(j, route):
        for i, m in enumerate(route[3:]):
            ag_copy(j, 5 + i, None, m, t, f, 1 - t).wait_recv()
            ag_copy(j, 5 + i, None, m, t, f, 1 - t).start()

    def ag_arrive(j):
        for m in range(4):
            ag_copy(j, 0, None, m, 1 - t, f, 1 - t).wait_recv()

    def ag_settle(j):
        for i in range(7):
            ag_copy(j, i, None, me, t, f, 1 - t).wait_send()

    def each_chunk(body):
        def step(j, _):
            body(j)
            return 0

        lax.fori_loop(0, chunks, step, 0)

    def norm_rows(gain_ref):
        def step(i, _):
            at = pl.ds(pl.multiple_of(i * 32, 32), 32)
            v = rows_raw[at, :].astype(f32)
            r = lax.rsqrt(jnp.mean(v * v, axis=-1, keepdims=True) + EPSILON)
            rows_normed[at, :] = (v * r * gain_ref[...]).astype(bf16)
            return 0

        lax.fori_loop(0, rows_raw.shape[0] // 32, step, 0)

    def row_tiles(size, body):
        def step(i, _):
            body(pl.ds(pl.multiple_of(i * size, size), size))
            return 0

        lax.fori_loop(0, rows_raw.shape[0] // size, step, 0)

    def absorber(gain_ref, weights):
        columns = weights.shape[1]

        def clear(r):
            acc[r, :columns] = jnp.zeros((seq, columns), f32)
            power[r, :] = jnp.zeros((seq, piece), f32)

        def stage(j):
            at = pl.ds(column(j), chunk)

            ag_arrive(j)

            def tile(r):
                v = rows_raw[r, at].astype(f32)
                square = v * v
                power[r, :] += square[:, :piece] + square[:, piece:]
                v = (v * gain_ref[:, at]).astype(bf16)
                acc[r, :columns] += jnp.dot(v, weights[at, :], preferred_element_type=f32)

            row_tiles(4 * seq, tile)

        return stage, lambda: row_tiles(seq, clear)

    def row_factor(r):
        return lax.rsqrt(jnp.sum(power[r, :], axis=-1, keepdims=True) / width + EPSILON)

    def silu_mul(gate, up):
        gate = gate * gs_ref[:, pl.ds(pl.multiple_of(me * ff, ff), ff)]
        return (gate / (1.0 + jnp.exp(-gate)) * (up * us_ref[:, pl.ds(pl.multiple_of(me * ff, ff), ff)])).astype(bf16)

    def leave(inputs, weights, scale_row, factor, arriving, last, sums, rows, lags, absorb=None, during=None):
        def product(j):
            if arriving is not None:
                take_pair(arriving, j)
            base = pair_base(j)
            at = pl.ds(column(j), chunk)
            factors = jnp.concatenate(
                [w_sc[pl.ds((base + h) * 8 + scale_row, 1), :] for h in (0, 1)], axis=1
            )

            term = jnp.dot(inputs[...], weights[:, at], preferred_element_type=f32) * factors
            term = term.astype(bf16)
            for m in range(4):
                for core in range(2):
                    part[core, m, :, at] = term[(m * 2 + core) * own : (m * 2 + core + 1) * own]
            to_twin(j).start()

        def to_twin(j):
            at = pl.ds(column(j), chunk)
            return remote(part.at[1 - t, :, :, at], part_twin.at[:, :, at], tw_send.at[j], tw_recv.at[j], f, 1 - t)

        first, second, m_first, m_second, m_third = sums

        def to_first(j):
            at = pl.ds(column(j), chunk)
            pair = pl.ds(0, 2)
            return remote(
                chip_part.at[pair, :, at], far_part.at[pair, :, at], rs_send.at[j, 0], rs_recv.at[j, 0], first, t
            )

        def to_second(j):
            at = pl.ds(column(j), chunk)
            return remote(chip_part.at[2, :, at], far_part.at[2, :, at], rs_send.at[j, 1], rs_recv.at[j, 1], second, t)

        def chip_sum(m, at):
            return part[t, m, :, at].astype(f32) + part_twin[m, :, at].astype(f32)

        def reduce(j):
            at = pl.ds(column(j), chunk)
            to_twin(j).wait_recv()
            chip_part[0, :, at] = chip_sum(m_first, at).astype(bf16)
            chip_part[1, :, at] = chip_sum(m_third, at).astype(bf16)
            to_first(j).start()

        def relay(j):
            at = pl.ds(column(j), chunk)
            to_first(j).wait_recv()
            chip_part[2, :, at] = (chip_sum(m_second, at) + far_part[1, :, at].astype(f32)).astype(bf16)
            to_second(j).start()

        def finish(j):
            at = pl.ds(column(j), chunk)
            to_second(j).wait_recv()
            total = chip_sum(me, at) + far_part[0, :, at].astype(f32) + far_part[2, :, at].astype(f32)
            mine = block_rows(me, t)
            fresh = (rows_raw[mine, at].astype(f32) + factor * total).astype(bf16)
            if last:
                out_ref[:, at] = fresh
            else:
                rows_raw[mine, at] = fresh
                ag_start(j, None, rows)

        stages = [product, reduce, relay, finish]
        if not last:
            stages += [lambda j: ag_relay(j, rows), lambda j: ag_pass(j, rows), absorb[0]]

        def step(i, _):
            for lag, stage in zip(lags, stages):
                pl.when((i >= lag) & (i < chunks + lag))(lambda stage=stage, lag=lag: stage(i - lag))
            if absorb is not None:
                pl.when(i == 2)(absorb[1])
            if during is not None:
                during(i)
            return 0

        lax.fori_loop(0, chunks + lags[len(stages) - 1], step, 0)

        def drain(j, _):
            to_twin(j).wait_send()
            to_first(j).wait_send()
            to_second(j).wait_send()
            return 0

        lax.fori_loop(0, chunks, drain, 0)
        if not last:
            each_chunk(ag_settle)

    scales_ref[...] = jnp.zeros_like(scales_ref)
    scales_ref[0:1, :] = ds_ref[...]
    scales_ref[1:2, :] = os_ref[...]
    send_pieces(SC)

    loads[0].wait()
    for m in range(4):
        at = slice(m * ff, (m + 1) * ff)
        st_gu[m, :, :ff] = gate_ref[:, at].astype(bf16)
    send_pieces(GATE)
    each_chunk(lambda j: ag_start(j, res_ref.at[:, pl.ds(column(j), chunk)], z_then_x))
    rows_raw[block_rows(me, t), :] = res_ref[...]

    loads[1].wait()
    for m in range(4):
        st_gu[m, :, ff:] = up_ref[:, m * ff : (m + 1) * ff].astype(bf16)
    send_pieces(UP)
    for load in loads[2:]:
        load.wait()
    for m in range(4):
        at = slice(m * hd, (m + 1) * hd)
        st_d[m] = down_ref[m * ff : (m + 1) * ff, :].astype(bf16)
        st_qkv[m, :, :hd] = q_ref[:, at].astype(bf16)
        st_qkv[m, :, hd : 2 * hd] = k_ref[:, at].astype(bf16)
        st_qkv[m, :, 2 * hd :] = v_ref[:, at].astype(bf16)
        st_o[m] = o_ref[at, :].astype(bf16)

    for kind in (DN, QKV, OUT):
        send_across(kind)

    ahead = zl != zh
    take_some(SC, 0, 4)
    take_some(GATE, 0, 4)
    each_chunk(lambda j: ag_relay(j, z_then_x))
    send_near(DN)
    pl.when(ahead)(lambda: send_far(DN))
    send_near(QKV)
    send_near(OUT)
    take_some(UP, 0, 2)
    each_chunk(lambda j: ag_pass(j, z_then_x))
    each_chunk(ag_arrive)
    each_chunk(ag_settle)
    norm_rows(g1_ref)
    take_some(UP, 2, 3)
    take_some(GATE, 4, 8)

    def first_gate(r):
        acc[r, :ff] = jnp.dot(rows_normed[r, :], w_gu[:, :ff], preferred_element_type=f32)

    row_tiles(2 * seq, first_gate)
    take_some(UP, 3, 4)
    pl.when(ahead)(lambda: send_far(QKV))
    pl.when(jnp.logical_not(ahead))(lambda: send_far(DN))
    take_some(UP, 4, 8)
    take_some(SC, 4, 8)

    def first_hidden(r):
        up = jnp.dot(rows_normed[r, :], w_gu[:, ff:], preferred_element_type=f32)
        hidden[r, :] = silu_mul(acc[r, :ff], up)

    row_tiles(2 * seq, first_hidden)

    def take_early(i):
        pl.when((i == 3) & ahead)(lambda: send_far(OUT))
        pl.when((i == 3) & jnp.logical_not(ahead))(lambda: send_far(QKV))
        pl.when((i == 8) & jnp.logical_not(ahead))(lambda: send_far(OUT))
        for at, kind, j in EARLY:
            pl.when(i == at)(lambda kind=kind, j=j: take_pair(kind, j))

    leave(hidden, w_d, 0, 0.5, DN, False, x_then_z, by_core, (0, 1, 4, 6, 9, 11, 12), absorber(g2_ref, w_qkv), take_early)

    take_some(OUT, 4, 8)
    head = (t * 4 + me).astype(f32)
    ri = lax.broadcasted_iota(jnp.int32, (seq, seq), 0)
    ci = lax.broadcasted_iota(jnp.int32, (seq, seq), 1)
    rate = jnp.exp(math.log(1.0 / 16.0) + jnp.full((seq, seq), head, f32) / (HEADS - 1) * math.log(4.0 / seq))
    distance = jnp.maximum(ri - ci, 0).astype(f32)
    decay = jnp.where(ri >= ci, jnp.exp(-rate * distance), 0.0) * hd ** (-0.5)

    at_head = pl.ds(pl.multiple_of(me * hd, hd), hd)

    def turn(values):
        a, b = values[:, : hd // 2], values[:, hd // 2 :]
        c, s = cos_ref[...], sin_ref[...]
        return jnp.concatenate([a * c - b * s, b * c + a * s], axis=1).astype(bf16)

    def sequence(r):
        factor = row_factor(r)
        q = turn(acc[r, :hd] * factor * qs_ref[:, at_head])
        k = turn(acc[r, hd : 2 * hd] * factor * ks_ref[:, at_head])
        v = (acc[r, 2 * hd : 3 * hd] * factor * vs_ref[:, at_head]).astype(bf16)
        scores = lax.dot_general(q, k, (((1,), (1,)), ((), ())), preferred_element_type=f32)
        both = jnp.dot((scores * decay).astype(bf16), v, preferred_element_type=f32)
        level = jnp.maximum(jnp.mean(both * both, axis=-1, keepdims=True), HEAD_FLOOR)
        mixed[r, :] = (both * lax.rsqrt(level)).astype(bf16)

    row_tiles(seq, sequence)
    leave(mixed, w_o, 1, 1.0, None, False, by_core, by_core, (0, 1, 3, 6, 9, 12, 13), absorber(g3_ref, w_gu))

    def second_hidden(r):
        factor = row_factor(r)
        hidden[r, :] = silu_mul(acc[r, :ff] * factor, acc[r, ff : 2 * ff] * factor)

    row_tiles(own, second_hidden)
    leave(hidden, w_d, 0, 0.5, None, True, by_core, by_core, (0, 1, 3, 7))
    for kind in (SC, GATE, UP, DN, QKV, OUT):
        finish_sends(kind)


def fused_body(
    residual_in, gain_first, gain_mixer, gain_second,
    gate_weight, gate_scale, up_weight, up_scale, down_weight, down_scale,
    query_weight, query_scale, key_weight, key_scale, value_weight, value_scale,
    output_weight, output_scale,
):
    f32, bf16 = jnp.float32, jnp.bfloat16
    own, width = residual_in.shape
    rows, piece = 8 * own, gate_weight.shape[0]
    ff, hd = gate_weight.shape[1] // 4, query_weight.shape[1] // 4
    chunks = width // (2 * piece)

    def row(vector):
        return vector.reshape(1, -1)

    half = hd // 2
    frequency = np.float32(ROTARY_BASE) ** (-np.arange(half, dtype=np.float32) * np.float32(2.0) / np.float32(hd))
    angles = np.arange(2 * own, dtype=np.float32)[:, None] * frequency.astype(np.float32)[None]
    cosine, sine_value = np.cos(angles).astype(np.float32), np.sin(angles).astype(np.float32)
    operands = (
        residual_in, row(gain_first), row(gain_mixer), row(gain_second),
        gate_weight, up_weight, down_weight, query_weight, key_weight, value_weight, output_weight,
        row(gate_scale), row(up_scale), row(query_scale), row(key_scale), row(value_scale),
        row(down_scale), row(output_scale), jnp.asarray(cosine), jnp.asarray(sine_value),
    )
    dma = pltpu.SemaphoreType.DMA
    return pl.pallas_call(
        fused_kernel,
        out_shape=jax.ShapeDtypeStruct((own, width), bf16),
        in_specs=[pl.BlockSpec(memory_space=pl.ANY if 4 <= i < 11 else pltpu.VMEM) for i in range(len(operands))],
        out_specs=pl.BlockSpec(memory_space=pltpu.VMEM),
        scratch_shapes=[
            pltpu.VMEM((rows, width), bf16),
            pltpu.VMEM((rows, width), bf16),
            pltpu.VMEM((width, 2 * ff), bf16),
            pltpu.VMEM((ff, width), bf16),
            pltpu.VMEM((width, 3 * hd), bf16),
            pltpu.VMEM((hd, width), bf16),
            pltpu.VMEM((8 * (width // piece), piece), f32),
            pltpu.VMEM((4, piece, 2 * ff), bf16),
            pltpu.VMEM((4, ff, piece), bf16),
            pltpu.VMEM((4, piece, 3 * hd), bf16),
            pltpu.VMEM((4, hd, piece), bf16),
            pltpu.VMEM((8, piece), f32),
            pltpu.VMEM((rows, max(2 * ff, 3 * hd)), f32),
            pltpu.VMEM((rows, piece), f32),
            pltpu.VMEM((rows, ff), bf16),
            pltpu.VMEM((rows, hd), bf16),
            pltpu.VMEM((2, 4, own, width), bf16),
            pltpu.VMEM((4, own, width), bf16),
            pltpu.VMEM((3, own, width), bf16),
            pltpu.VMEM((3, own, width), bf16),
            *[pltpu.VMEM(operand.shape, f32) for operand in operands[4:11]],
            dma((7,)),
            dma((6, 16)), dma((6, 7)), dma((6, 8)),
            dma((chunks, 8)), dma((chunks, 7)),
            dma((chunks,)), dma((chunks,)), dma((chunks, 2)), dma((chunks, 2)),
        ],
        compiler_params=pltpu.CompilerParams(
            collective_id=0, has_side_effects=True, vmem_limit_bytes=63 * 2**20
        ),
    )(*operands)


def solution(mesh):
    n_fs, n_tp = mesh.shape["fs"], mesh.shape["tp"]
    share = math.gcd(math.gcd(HEADS // n_tp, n_fs), 4)
    if (n_fs, n_tp, share) == (16, 2, 4):
        body = fused_body
    else:
        body = make_body(n_fs, n_tp, share)
    in_specs = (
        P(("fs", "tp"), None),
        P(),
        P(),
        P(),
        P("fs", "tp"),
        P("tp"),
        P("fs", "tp"),
        P("tp"),
        P("tp", "fs"),
        P("fs"),
        P("fs", "tp"),
        P("tp"),
        P("fs", "tp"),
        P("tp"),
        P("fs", "tp"),
        P("tp"),
        P("tp", "fs"),
        P("fs"),
    )
    out_specs = P(("fs", "tp"), None)
    return jax.shard_map(body, mesh=mesh, in_specs=in_specs, out_specs=out_specs, check_vma=False)
```
